512 devices in a mesh: fs: 64 (over z, y), tp: 8 (over x, core).
Axes of the slice: x: 4, y: 8, z: 8, core: 2. Of those that a mesh axis runs over, the one named last changes fastest.
Arguments:
- tokens: bfloat16 [8, 256, 2048], P('tp'), may hold values from -6 to 6
- gain_first: float32 [2048], P('fs'), may hold values from 0.1 to 1.9
- gate_first: float32 [2048, 5632], P('fs', 'tp'), may hold values from -0.125 to 0.125
- up_first: float32 [2048, 5632], P('fs', 'tp'), may hold values from -0.125 to 0.125
- down_first: float32 [2048, 5632], P('fs', 'tp'), may hold values from -0.3125 to 0.3125
- gain_second: float32 [2048], P('fs'), may hold values from 0.1 to 1.9
- gate_second: float32 [2048, 5632], P('fs', 'tp'), may hold values from -0.125 to 0.125
- up_second: float32 [2048, 5632], P('fs', 'tp'), may hold values from -0.125 to 0.125
- down_second: float32 [2048, 5632], P('fs', 'tp'), may hold values from -0.3125 to 0.3125
Outputs:
- mixed: bfloat16 [8, 256, 2048], P('tp', 'fs')
- served_gate_first: bfloat16 [8, 704, 2048], P(None, 'fs')
- served_up_first: bfloat16 [8, 704, 2048], P(None, 'fs')
- served_down_first: bfloat16 [8, 704, 2048], P(None, 'fs')
- served_gate_second: bfloat16 [8, 704, 2048], P(None, 'fs')
- served_up_second: bfloat16 [8, 704, 2048], P(None, 'fs')
- served_down_second: bfloat16 [8, 704, 2048], P(None, 'fs')
The draws below stay inside these ranges and needn't reach their ends.
All inputs are finite; a program needn't handle non-finite values.
Results may differ from the reference program's by a relative error of at most 0.013.
Values may be sent and summed in bfloat16 or wider, within the bound.
A program may use at most 64 MiB of HBM per device.

```python
import jax
import jax.numpy as jnp
from jax import lax

D = 2048
FF = 5632
PLEN = 256
PROMPTS = 8
N_TP = 8


def steps_of(key, dims, pieces, smallest, largest):
    loudness = 1.0
    for position, blocks in pieces:
        draws = jax.random.uniform(jax.random.fold_in(jax.random.fold_in(key, 6), position), (blocks,), jnp.float32, smallest / len(pieces), largest / len(pieces))
        loudness = loudness * jnp.repeat(jnp.exp(draws), dims[position] // blocks).reshape((-1,) + (1,) * (len(dims) - 1 - position))
    return loudness


def bell_draw(rng, dims, width, reach, split=(), kind=jnp.bfloat16):
    values = jax.random.normal(rng, dims, jnp.float32) * width
    if len(split) > 0:
        values = steps_of(rng, dims, split, -0.22, 0.18) * values
    return jnp.clip(values, min=-reach, max=reach).astype(kind)


def setup_inputs(seed: int = 0) -> dict:
    keys = jax.random.split(jax.random.key(seed), 10)
    tokens = bell_draw(keys[0], (PROMPTS, PLEN, D), 1.0, 6.0, ((0, 8),))
    gain_first = jnp.clip(1.0 + 0.18 * jax.random.normal(keys[1], (D,), jnp.float32), 0.1, 1.9)
    gate_first = bell_draw(keys[2], (D, FF), D ** -0.5, 0.125, ((0, 64), (1, 8)), jnp.float32)
    up_first = bell_draw(keys[3], (D, FF), D ** -0.5, 0.125, ((0, 64), (1, 8)), jnp.float32)
    down_first = bell_draw(keys[4], (D, FF), (FF // 16) ** -0.5, 0.3125, ((0, 64), (1, 8)), jnp.float32)
    gain_second = jnp.clip(1.0 + 0.18 * jax.random.normal(keys[5], (D,), jnp.float32), 0.1, 1.9)
    gate_second = bell_draw(keys[6], (D, FF), D ** -0.5, 0.125, ((0, 64), (1, 8)), jnp.float32)
    up_second = bell_draw(keys[7], (D, FF), D ** -0.5, 0.125, ((0, 64), (1, 8)), jnp.float32)
    down_second = bell_draw(keys[8], (D, FF), (FF // 16) ** -0.5, 0.3125, ((0, 64), (1, 8)), jnp.float32)
    return {"tokens": tokens, "gain_first": gain_first, "gate_first": gate_first, "up_first": up_first, "down_first": down_first, "gain_second": gain_second, "gate_second": gate_second, "up_second": up_second, "down_second": down_second}


def normalize(values):
    wide = values.astype(jnp.float32)
    scale = lax.rsqrt(lax.optimization_barrier(jnp.mean(wide * wide, axis=-1, keepdims=True)) + 1e-06)
    return (wide * scale).astype(jnp.bfloat16)

def gated_branch(values, gate_cast, up_cast, down_cast):
    normed = normalize(values)
    gate_act = jnp.dot(normed, gate_cast, preferred_element_type=jnp.float32)
    up_act = jnp.dot(normed, up_cast, preferred_element_type=jnp.float32)
    hidden = (jax.nn.silu(gate_act) * up_act).astype(jnp.bfloat16)
    return jnp.dot(hidden, down_cast.T, preferred_element_type=jnp.float32)

def served(cast):
    return cast.T.reshape(N_TP, FF // N_TP, D)

def reference(tokens, gain_first, gate_first, up_first, down_first, gain_second, gate_second, up_second, down_second):
    gate_one = (gate_first * gain_first[:, None]).astype(jnp.bfloat16)
    up_one = (up_first * gain_first[:, None]).astype(jnp.bfloat16)
    down_one = down_first.astype(jnp.bfloat16)
    gate_two = (gate_second * gain_second[:, None]).astype(jnp.bfloat16)
    up_two = (up_second * gain_second[:, None]).astype(jnp.bfloat16)
    down_two = down_second.astype(jnp.bfloat16)
    rows = tokens.reshape(-1, D)
    branch_first = gated_branch(rows, gate_one, up_one, down_one)
    middle = (rows.astype(jnp.float32) + 0.5 * branch_first).astype(jnp.bfloat16)
    branch_second = gated_branch(middle, gate_two, up_two, down_two)
    mixed = (middle.astype(jnp.float32) + 0.5 * branch_second).astype(jnp.bfloat16)
    return (mixed.reshape(tokens.shape), served(gate_one), served(up_one), served(down_one), served(gate_two), served(up_two), served(down_two))
```

```python
import functools

import jax
import jax.numpy as jnp
from jax import lax
from jax.experimental import pallas as pl
from jax.experimental.pallas import tpu as pltpu
from jax.sharding import PartitionSpec as P

MESH = pl.DeviceIdType.MESH
F32, BF16 = jnp.float32, jnp.bfloat16
ROWS = 16
OWN = 4


def rsqrt_norm(wide):
    scale = lax.rsqrt(jnp.mean(wide * wide, axis=-1, keepdims=True) + 1e-06)
    return (wide * scale).astype(BF16)


def kernel(
    n, n_tp, hu, fd,
    tokens, gain_one, gate_one, up_one, down_one, gain_two, gate_two, up_two, down_two,
    mixed, served,
    stack, turned, outgoing, incoming, weights, hidden, normed, part, landed, group, owner,
    small, gathered, middle,
    w_send, w_recv, x_send, x_recv, r_send, ra_recv, rb_recv, q_send, q_recv,
    s_send, s_recv, g_send, ga_recv, gb_recv, out_sem,
):
    fs = n * n
    d = fs * fd
    half = OWN * fs // 2
    block = half // n
    groups = n // 2
    f, t = lax.axis_index("fs"), lax.axis_index("tp")
    z, y = f // n, lax.rem(f, n)
    x, c = t // 2, lax.rem(t, 2)
    nx = n_tp // 2
    even = lax.rem(z + y, 2) == 0

    def at(zz, yy):
        return (zz * n + yy, t)

    def remote(src, dst, send, recv, device):
        return pltpu.make_async_remote_copy(
            src_ref=src, dst_ref=dst, send_sem=send, recv_sem=recv, device_id=device, device_id_type=MESH
        )

    def drain(ref, sem):
        pltpu.make_async_copy(ref, ref, sem).wait()

    barrier = pltpu.get_barrier_semaphore()

    @pl.loop(1, fs)
    def _(k):
        pl.semaphore_signal(barrier, inc=1, device_id=(lax.rem(f + k, fs), t), device_id_type=MESH)

    for k in range(1, nx):
        pl.semaphore_signal(
            barrier, inc=1, device_id=(f, lax.rem(x + k, nx) * 2 + c), device_id_type=MESH
        )
    partner = (f, x * 2 + 1 - c)
    pl.semaphore_signal(barrier, inc=1, device_id=partner, device_id_type=MESH)

    hidden_units = gate_one.shape[1]
    for b, (gain, gate, up, down) in enumerate(
        ((gain_one, gate_one, up_one, down_one), (gain_two, gate_two, up_two, down_two))
    ):
        stack[...] = jnp.zeros_like(stack)
        stack[0:fd, 0:hidden_units] = gate[...]
        stack[fd : 2 * fd, 0:hidden_units] = up[...]
        stack[2 * fd : 3 * fd, 0:hidden_units] = down[...]
        ones = jnp.ones((1, fd), F32)
        scale = jnp.concatenate([gain[...], gain[...], ones, ones], axis=1)
        turned[...] = stack[...].T * scale
        live = lax.broadcasted_iota(jnp.int32, (ROWS, 128), 0) < hu
        for k in range(fs):
            rows = turned[k * hu : k * hu + ROWS, :]
            outgoing[b, k] = jnp.where(live, rows, 0.0).astype(BF16)

    pl.semaphore_wait(barrier, fs - 1 + nx - 1 + 1)

    for b in range(2):

        @pl.loop(1, fs)
        def _(k):
            peer = lax.rem(f + k, fs)
            remote(
                outgoing.at[b, peer],
                incoming.at[b, lax.rem(f, 4), f // 4],
                w_send.at[b],
                w_recv.at[b],
                (peer, t),
            ).start()

        pltpu.make_async_copy(
            outgoing.at[b, f], incoming.at[b, lax.rem(f, 4), f // 4], w_recv.at[b]
        ).start()

    wide = tokens[...].astype(F32)
    normed_rows = rsqrt_norm(wide)
    spot = lax.broadcasted_iota(jnp.int32, (2 * half, 2 * half), 0)
    source = lax.broadcasted_iota(jnp.int32, (2 * half, 2 * half), 1)
    in_first = spot < half
    inside = jnp.where(in_first, spot, spot - half)
    major = inside // block
    minor = (inside % block) // OWN
    row = inside % OWN
    first_home = major * n + 2 * minor + major % 2
    second_home = (2 * minor + (major + 1) % 2) * n + major
    home = jnp.where(in_first, first_home, second_home) * OWN + row
    shuffle = jnp.where(home == source, 1.0, 0.0).astype(BF16)
    normed[...] = jnp.dot(shuffle, normed_rows, preferred_element_type=F32).astype(BF16)
    pick_row = lax.broadcasted_iota(jnp.int32, (8, 2 * half), 0)
    pick_source = lax.broadcasted_iota(jnp.int32, (8, 2 * half), 1)
    pick = jnp.where((pick_row < OWN) & (pick_source == pick_row + f * OWN), 1.0, 0.0).astype(BF16)
    mine = jnp.dot(pick, tokens[...], preferred_element_type=F32)[0:OWN]

    lanes = 3 * 128
    m = lax.broadcasted_iota(jnp.int32, (128, lanes), 0)
    l = lax.broadcasted_iota(jnp.int32, (128, lanes), 1)
    inner = l % 128

    def exchange(b):
        drain(incoming.at[b], w_recv.at[b])
        total = jnp.zeros((fs // 4 * ROWS, lanes), F32)
        for i in range(4):
            chosen = (inner // 32 == i) & (m == l // 128 * 32 + inner % 32)
            spread = jnp.where(chosen, 1.0, 0.0).astype(BF16)
            piece = incoming[b, i].reshape(fs // 4 * ROWS, 128)
            total = total + jnp.dot(piece, spread, preferred_element_type=F32)
        merged = total.astype(BF16)
        for j in range(fs // 4):
            for w in range(3):
                weights[b, t, w, :, j * 128 : (j + 1) * 128] = merged[
                    j * ROWS : (j + 1) * ROWS, w * 128 : (w + 1) * 128
                ]
        for k in range(1, nx):
            remote(
                weights.at[b, t], weights.at[b, t], x_send.at[b, k - 1], x_recv.at[b, t],
                (f, lax.rem(x + k, nx) * 2 + c),
            ).start()
        remote(weights.at[b, t], weights.at[b, t], x_send.at[b, nx - 1], x_recv.at[b, t], partner).start()

    def hand_over(b):
        for k in range(1, nx):
            slot = lax.rem(x + nx - k, nx) * 2 + c
            drain(weights.at[b, slot], x_recv.at[b, slot])
            remote(
                weights.at[b, slot], weights.at[b, slot], x_send.at[b, nx - 1 + k], x_recv.at[b, slot], partner
            ).start()

    def collected(b):
        for k in range(nx):
            slot = lax.rem(x + k, nx) * 2 + 1 - c
            drain(weights.at[b, slot], x_recv.at[b, slot])
        for k in range(2 * nx - 1):
            drain(weights.at[b, t], x_send.at[b, k])

    def publish(b):
        return pltpu.make_async_copy(weights.at[b], served.at[b], out_sem.at[b])

    def feed(b, side):
        rows = normed[side * half : (side + 1) * half, :]
        contract = (((1,), (1,)), ((), ()))
        gate = weights[b, :, 0].reshape(n_tp * ROWS, d)
        up = weights[b, :, 1].reshape(n_tp * ROWS, d)
        down = weights[b, :, 2].reshape(n_tp * ROWS, d)
        gate_act = lax.dot_general(rows, gate, contract, preferred_element_type=F32)
        up_act = lax.dot_general(rows, up, contract, preferred_element_type=F32)
        act = (gate_act / (1.0 + jnp.exp(-gate_act)) * up_act).astype(BF16)
        branch = jnp.dot(act, down, preferred_element_type=F32).astype(BF16)
        part[b, side * n : (side + 1) * n] = branch.reshape(n, block, d)

    def send_blocks(b, side):
        me = z if side == 0 else y
        recv = ra_recv if side == 0 else rb_recv

        @pl.loop(1, n)
        def _(k):
            peer = lax.rem(me + k, n)
            remote(
                part.at[b, side * n + peer],
                landed.at[b, side, me],
                r_send.at[b],
                recv.at[b],
                at(peer, y) if side == 0 else at(z, peer),
            ).start()

        pltpu.make_async_copy(part.at[b, side * n + me], landed.at[b, side, me], recv.at[b]).start()

    def reduce_blocks(b, side):
        recv = ra_recv if side == 0 else rb_recv
        drain(landed.at[b, side], recv.at[b])
        total = landed[b, side, 0].astype(F32)
        for k in range(1, n):
            total = total + landed[b, side, k].astype(F32)
        for k in range(groups):
            group[b, side, k] = total[k * OWN : (k + 1) * OWN].astype(BF16)
        me = y if side == 0 else z
        for k in range(groups):
            peer = 2 * k + (lax.rem(z, 2) if side == 0 else lax.rem(y + 1, 2))

            @pl.when(peer != me)
            def _():
                remote(
                    group.at[b, side, k],
                    owner.at[b, me],
                    q_send.at[b],
                    q_recv.at[b],
                    at(z, peer) if side == 0 else at(peer, y),
                ).start()

            @pl.when(peer == me)
            def _():
                pltpu.make_async_copy(group.at[b, side, k], owner.at[b, me], q_recv.at[b]).start()

    def summed(b):
        drain(owner.at[b], q_recv.at[b])
        total = owner[b, 0].astype(F32)
        for k in range(1, n):
            total = total + owner[b, k].astype(F32)
        return total

    exchange(0)
    hand_over(0)
    exchange(1)
    collected(0)
    publish(0).start()
    for side in range(2):
        feed(0, side)
        send_blocks(0, side)
    hand_over(1)
    for side in range(2):
        reduce_blocks(0, side)
    middle[...] = (mine + 0.5 * summed(0)).astype(BF16)
    mid = middle[...].astype(F32)
    own_slot = jnp.where(even, y // 2, groups + z // 2)
    small[own_slot] = rsqrt_norm(mid)

    @pl.loop(1, n)
    def _(k):
        peer = jnp.where(even, z * n + lax.rem(y + k, n), lax.rem(z + k, n) * n + y)
        remote(small.at[own_slot], small.at[own_slot], s_send, s_recv, (peer, t)).start()

    drain(small.at[pl.ds(0, n - 1)], s_recv)
    for side in range(2):
        me = z if side == 0 else y
        recv = ga_recv if side == 0 else gb_recv
        rows = jnp.concatenate(
            [small[side * groups + k].astype(F32) for k in range(groups)], axis=0
        )
        gathered[side, me] = rows.astype(BF16)

        @pl.loop(1, n)
        def _(k):
            peer = lax.rem(me + k, n)
            remote(
                gathered.at[side, me],
                gathered.at[side, me],
                g_send,
                recv,
                at(peer, y) if side == 0 else at(z, peer),
            ).start()

    collected(1)
    publish(1).start()
    for side in range(2):
        recv = ga_recv if side == 0 else gb_recv
        drain(gathered.at[side, pl.ds(0, n - 1)], recv)
        normed[side * half : (side + 1) * half, :] = gathered[side].reshape(half, d)
        feed(1, side)
        send_blocks(1, side)
    for side in range(2):
        reduce_blocks(1, side)
    mixed[...] = (mid + 0.5 * summed(1)).astype(BF16)

    drain(small.at[pl.ds(0, n - 1)], s_send)
    drain(part.at[0, pl.ds(0, 2 * n - 2)], g_send)
    for b in range(2):
        drain(outgoing.at[b, pl.ds(0, fs - 1)], w_send.at[b])
        drain(part.at[b, pl.ds(0, 2 * n - 2)], r_send.at[b])
        drain(owner.at[b, pl.ds(0, n - 1)], q_send.at[b])
        publish(b).wait()


def shards(
    tokens, gain_first, gate_first, up_first, down_first, gain_second, gate_second, up_second, down_second
):
    fs, n_tp = lax.axis_size("fs"), lax.axis_size("tp")
    n = int(round(fs**0.5))
    fd, local = gate_first.shape
    hu = local // fs
    d = fs * fd
    rows = tokens.shape[1]
    block = rows // 2 // n
    wide = -(-(local + ROWS) // 128) * 128
    vmem = pl.BlockSpec(memory_space=pltpu.VMEM)
    dma, one = pltpu.SemaphoreType.DMA, (2,)
    mixed, served = pl.pallas_call(
        functools.partial(kernel, n, n_tp, hu, fd),
        out_shape=(
            jax.ShapeDtypeStruct((OWN, d), BF16),
            jax.ShapeDtypeStruct((2, n_tp, 3, ROWS, d), BF16),
        ),
        in_specs=[vmem] * 9,
        out_specs=(vmem, pl.BlockSpec(memory_space=pl.ANY)),
        scratch_shapes=[
            pltpu.VMEM((4 * fd, wide), F32),
            pltpu.VMEM((wide, 4 * fd), F32),
            pltpu.VMEM((2, fs, ROWS, 128), BF16),
            pltpu.VMEM((2, 4, fs // 4, ROWS, 128), BF16),
            pltpu.VMEM((2, n_tp, 3, ROWS, d), BF16),
            pltpu.VMEM((8, 128), BF16),
            pltpu.VMEM((rows, d), BF16),
            pltpu.VMEM((2, 2 * n, block, d), BF16),
            pltpu.VMEM((2, 2, n, block, d), BF16),
            pltpu.VMEM((2, 2, n // 2, OWN, d), BF16),
            pltpu.VMEM((2, n, OWN, d), BF16),
            pltpu.VMEM((n, OWN, d), BF16),
            pltpu.VMEM((2, n, block, d), BF16),
            pltpu.VMEM((OWN, d), BF16),
            dma(one), dma(one), dma((2, n_tp - 1)), dma((2, n_tp)),
            dma(one), dma(one), dma(one), dma(one), dma(one),
            dma(()), dma(()), dma(()), dma(()), dma(()), dma(one),
        ],
        compiler_params=pltpu.CompilerParams(
            collective_id=0, has_side_effects=True, vmem_limit_bytes=60 * 1024 * 1024
        ),
    )(
        tokens[0],
        gain_first[None], gate_first, up_first, down_first,
        gain_second[None], gate_second, up_second, down_second,
    )
    return (mixed[None],) + tuple(served[b, :, w, :hu, :] for b in range(2) for w in range(3))


def solution(mesh):
    weight = P("fs", "tp")
    cut = P(None, "fs", None)
    return jax.shard_map(
        shards,
        mesh=mesh,
        in_specs=(P("tp", None, None), P("fs"), weight, weight, weight, P("fs"), weight, weight, weight),
        out_specs=(P("tp", "fs", None),) + (cut,) * 6,
        check_vma=False,
    )
```

```python
import functools

import jax
import jax.numpy as jnp
from jax import lax
from jax.experimental import pallas as pl
from jax.experimental.pallas import tpu as pltpu
from jax.sharding import PartitionSpec as P

MESH = pl.DeviceIdType.MESH
F32, BF16 = jnp.float32, jnp.bfloat16
ROWS = 16
OWN = 4


def rsqrt_norm(wide):
    scale = lax.rsqrt(jnp.mean(wide * wide, axis=-1, keepdims=True) + 1e-06)
    return (wide * scale).astype(BF16)


def kernel(
    n, n_tp, hu, fd,
    tokens_hbm, gain_one, gate_one, up_one, down_one, gain_two, gate_two, up_two, down_two,
    mixed, out_0, out_1, out_2, out_3, out_4, out_5,
    tokens, gains, trained, stack, turned, outgoing, incoming, weights, hidden, normed, part, landed, group, owner,
    small, gathered, middle, staged,
    w_send, w_recv, x_send, x_recv, r_send, ra_recv, rb_recv, q_send, q_recv,
    s_send, s_recv, g_send, ga_recv, gb_recv, in_sem, out_sem,
):
    served = (out_0, out_1, out_2, out_3, out_4, out_5)
    fs = n * n
    d = fs * fd
    half = OWN * fs // 2
    block = half // n
    groups = n // 2
    f, t = lax.axis_index("fs"), lax.axis_index("tp")
    z, y = f // n, lax.rem(f, n)
    x, c = t // 2, lax.rem(t, 2)
    nx = n_tp // 2
    even = lax.rem(z + y, 2) == 0

    def at(zz, yy):
        return (zz * n + yy, t)

    def remote(src, dst, send, recv, device):
        return pltpu.make_async_remote_copy(
            src_ref=src, dst_ref=dst, send_sem=send, recv_sem=recv, device_id=device, device_id_type=MESH
        )

    def drain(ref, sem):
        pltpu.make_async_copy(ref, ref, sem).wait()

    given = ((gain_one, gate_one, up_one, down_one), (gain_two, gate_two, up_two, down_two))
    loads = []
    for b, (gain, *each) in enumerate(given):
        loads.append(pltpu.make_async_copy(gain, gains.at[b], in_sem.at[b, 3]))
        for w in range(3):
            loads.append(pltpu.make_async_copy(each[w], trained.at[b, w], in_sem.at[b, w]))
    loads.append(pltpu.make_async_copy(tokens_hbm, tokens, in_sem.at[0, 4]))
    for load in loads:
        load.start()

    barrier = pltpu.get_barrier_semaphore()

    @pl.loop(1, fs)
    def _(k):
        pl.semaphore_signal(barrier, inc=1, device_id=(lax.rem(f + k, fs), t), device_id_type=MESH)

    for k in range(1, nx):
        pl.semaphore_signal(
            barrier, inc=1, device_id=(f, lax.rem(x + k, nx) * 2 + c), device_id_type=MESH
        )
    partner = (f, x * 2 + 1 - c)
    pl.semaphore_signal(barrier, inc=1, device_id=partner, device_id_type=MESH)

    hidden_units = gate_one.shape[1]
    stack[...] = jnp.zeros_like(stack)
    for b in range(2):
        for load in loads[4 * b : 4 * b + 4]:
            load.wait()
        for w in range(3):
            stack[w * fd : (w + 1) * fd, 0:hidden_units] = trained[b, w]
        ones = jnp.ones((1, fd), F32)
        scale = jnp.concatenate([gains[b], gains[b], ones, ones], axis=1)
        turned[...] = stack[...].T * scale
        live = lax.broadcasted_iota(jnp.int32, (ROWS, 128), 0) < hu
        for k in range(fs):
            rows = turned[k * hu : k * hu + ROWS, :]
            outgoing[b, k] = jnp.where(live, rows, 0.0).astype(BF16)

    pl.semaphore_wait(barrier, fs - 1 + nx - 1 + 1)

    for b in range(2):

        @pl.loop(1, fs)
        def _(k):
            peer = lax.rem(f + k, fs)
            remote(
                outgoing.at[b, peer],
                incoming.at[b, lax.rem(f, 4), f // 4],
                w_send.at[b],
                w_recv.at[b],
                (peer, t),
            ).start()

        pltpu.make_async_copy(
            outgoing.at[b, f], incoming.at[b, lax.rem(f, 4), f // 4], w_recv.at[b]
        ).start()

    loads[8].wait()
    wide = tokens[...].astype(F32)
    normed_rows = rsqrt_norm(wide)
    spot = lax.broadcasted_iota(jnp.int32, (2 * half, 2 * half), 0)
    source = lax.broadcasted_iota(jnp.int32, (2 * half, 2 * half), 1)
    in_first = spot < half
    inside = jnp.where(in_first, spot, spot - half)
    major = inside // block
    minor = (inside % block) // OWN
    row = inside % OWN
    first_home = major * n + 2 * minor + major % 2
    second_home = (2 * minor + (major + 1) % 2) * n + major
    home = jnp.where(in_first, first_home, second_home) * OWN + row
    shuffle = jnp.where(home == source, 1.0, 0.0).astype(BF16)
    normed[...] = jnp.dot(shuffle, normed_rows, preferred_element_type=F32).astype(BF16)
    pick_row = lax.broadcasted_iota(jnp.int32, (8, 2 * half), 0)
    pick_source = lax.broadcasted_iota(jnp.int32, (8, 2 * half), 1)
    pick = jnp.where((pick_row < OWN) & (pick_source == pick_row + f * OWN), 1.0, 0.0).astype(BF16)
    mine = jnp.dot(pick, tokens[...], preferred_element_type=F32)[0:OWN]

    lanes = 3 * 128
    m = lax.broadcasted_iota(jnp.int32, (128, lanes), 0)
    l = lax.broadcasted_iota(jnp.int32, (128, lanes), 1)
    inner = l % 128

    def exchange(b):
        drain(incoming.at[b], w_recv.at[b])
        total = jnp.zeros((fs // 4 * ROWS, lanes), F32)
        for i in range(4):
            chosen = (inner // 32 == i) & (m == l // 128 * 32 + inner % 32)
            spread = jnp.where(chosen, 1.0, 0.0).astype(BF16)
            piece = incoming[b, i].reshape(fs // 4 * ROWS, 128)
            total = total + jnp.dot(piece, spread, preferred_element_type=F32)
        merged = total.astype(BF16)
        for j in range(fs // 4):
            for w in range(3):
                weights[b, t, w, :, j * 128 : (j + 1) * 128] = merged[
                    j * ROWS : (j + 1) * ROWS, w * 128 : (w + 1) * 128
                ]
        for k in range(1, nx):
            remote(
                weights.at[b, t], weights.at[b, t], x_send.at[b, k - 1], x_recv.at[b, t],
                (f, lax.rem(x + k, nx) * 2 + c),
            ).start()
        remote(weights.at[b, t], weights.at[b, t], x_send.at[b, nx - 1], x_recv.at[b, t], partner).start()

    def hand_over(b):
        for k in range(1, nx):
            slot = lax.rem(x + nx - k, nx) * 2 + c
            drain(weights.at[b, slot], x_recv.at[b, slot])
            remote(
                weights.at[b, slot], weights.at[b, slot], x_send.at[b, nx - 1 + k], x_recv.at[b, slot], partner
            ).start()

    def collected(b):
        for k in range(nx):
            slot = lax.rem(x + k, nx) * 2 + 1 - c
            drain(weights.at[b, slot], x_recv.at[b, slot])
        for k in range(2 * nx - 1):
            drain(weights.at[b, t], x_send.at[b, k])

    def shipped(b, w):
        return pltpu.make_async_copy(staged.at[3 * b + w], served[3 * b + w], out_sem.at[b, w])

    def publish(b):
        width = hu * n_tp
        spot = lax.broadcasted_iota(jnp.int32, (width, n_tp * ROWS), 0)
        source = lax.broadcasted_iota(jnp.int32, (width, n_tp * ROWS), 1)
        swap = jnp.where(source == spot % n_tp * ROWS + spot // n_tp, 1.0, 0.0).astype(BF16)
        for w in range(3):
            held = weights[b, :, w].reshape(n_tp * ROWS, d)
            rows = jnp.dot(swap, held, preferred_element_type=F32)
            for r in range(hu):
                staged[3 * b + w, r] = rows[r * n_tp : (r + 1) * n_tp].astype(BF16)
            shipped(b, w).start()

    def feed(b, side):
        rows = normed[side * half : (side + 1) * half, :]
        contract = (((1,), (1,)), ((), ()))
        gate = weights[b, :, 0].reshape(n_tp * ROWS, d)
        up = weights[b, :, 1].reshape(n_tp * ROWS, d)
        down = weights[b, :, 2].reshape(n_tp * ROWS, d)
        gate_act = lax.dot_general(rows, gate, contract, preferred_element_type=F32)
        up_act = lax.dot_general(rows, up, contract, preferred_element_type=F32)
        act = (gate_act / (1.0 + jnp.exp(-gate_act)) * up_act).astype(BF16)
        branch = jnp.dot(act, down, preferred_element_type=F32).astype(BF16)
        part[b, side * n : (side + 1) * n] = branch.reshape(n, block, d)

    def send_blocks(b, side):
        me = z if side == 0 else y
        recv = ra_recv if side == 0 else rb_recv

        @pl.loop(1, n)
        def _(k):
            peer = lax.rem(me + k, n)
            remote(
                part.at[b, side * n + peer],
                landed.at[b, side, me],
                r_send.at[b],
                recv.at[b],
                at(peer, y) if side == 0 else at(z, peer),
            ).start()

        pltpu.make_async_copy(part.at[b, side * n + me], landed.at[b, side, me], recv.at[b]).start()

    def reduce_blocks(b, side):
        recv = ra_recv if side == 0 else rb_recv
        drain(landed.at[b, side], recv.at[b])
        total = landed[b, side, 0].astype(F32)
        for k in range(1, n):
            total = total + landed[b, side, k].astype(F32)
        for k in range(groups):
            group[b, side, k] = total[k * OWN : (k + 1) * OWN].astype(BF16)
        me = y if side == 0 else z
        for k in range(groups):
            peer = 2 * k + (lax.rem(z, 2) if side == 0 else lax.rem(y + 1, 2))

            @pl.when(peer != me)
            def _():
                remote(
                    group.at[b, side, k],
                    owner.at[b, me],
                    q_send.at[b],
                    q_recv.at[b],
                    at(z, peer) if side == 0 else at(peer, y),
                ).start()

            @pl.when(peer == me)
            def _():
                pltpu.make_async_copy(group.at[b, side, k], owner.at[b, me], q_recv.at[b]).start()

    def summed(b):
        drain(owner.at[b], q_recv.at[b])
        total = owner[b, 0].astype(F32)
        for k in range(1, n):
            total = total + owner[b, k].astype(F32)
        return total

    exchange(0)
    hand_over(0)
    collected(0)
    for side in range(2):
        feed(0, side)
        send_blocks(0, side)
    exchange(1)
    publish(0)
    hand_over(1)
    for side in range(2):
        reduce_blocks(0, side)
    middle[...] = (mine + 0.5 * summed(0)).astype(BF16)
    mid = middle[...].astype(F32)
    own_slot = jnp.where(even, y // 2, groups + z // 2)
    small[own_slot] = rsqrt_norm(mid)

    @pl.loop(1, n)
    def _(k):
        peer = jnp.where(even, z * n + lax.rem(y + k, n), lax.rem(z + k, n) * n + y)
        remote(small.at[own_slot], small.at[own_slot], s_send, s_recv, (peer, t)).start()

    drain(small.at[pl.ds(0, n - 1)], s_recv)
    for side in range(2):
        me = z if side == 0 else y
        recv = ga_recv if side == 0 else gb_recv
        rows = jnp.concatenate(
            [small[side * groups + k].astype(F32) for k in range(groups)], axis=0
        )
        gathered[side, me] = rows.astype(BF16)

        @pl.loop(1, n)
        def _(k):
            peer = lax.rem(me + k, n)
            remote(
                gathered.at[side, me],
                gathered.at[side, me],
                g_send,
                recv,
                at(peer, y) if side == 0 else at(z, peer),
            ).start()

    collected(1)
    for side in range(2):
        recv = ga_recv if side == 0 else gb_recv
        drain(gathered.at[side, pl.ds(0, n - 1)], recv)
        normed[side * half : (side + 1) * half, :] = gathered[side].reshape(half, d)
        feed(1, side)
        send_blocks(1, side)
    publish(1)
    for side in range(2):
        reduce_blocks(1, side)
    mixed[...] = (mid + 0.5 * summed(1)).astype(BF16)

    drain(small.at[pl.ds(0, n - 1)], s_send)
    drain(part.at[0, pl.ds(0, 2 * n - 2)], g_send)
    for b in range(2):
        drain(outgoing.at[b, pl.ds(0, fs - 1)], w_send.at[b])
        drain(part.at[b, pl.ds(0, 2 * n - 2)], r_send.at[b])
        drain(owner.at[b, pl.ds(0, n - 1)], q_send.at[b])
        for w in range(3):
            shipped(b, w).wait()


def deliver(count, *refs):
    sources, targets, held = refs[:count], refs[count : 2 * count], refs[2 * count : 3 * count]
    in_sem, out_sem = refs[3 * count :]
    taken = [pltpu.make_async_copy(sources[k], held[k], in_sem.at[k]) for k in range(count)]
    given = [pltpu.make_async_copy(held[k], targets[k], out_sem.at[k]) for k in range(count)]
    for copy in taken:
        copy.start()
    for k in range(count):
        taken[k].wait()
        given[k].start()
    for copy in given:
        copy.wait()


def shards(
    tokens, gain_first, gate_first, up_first, down_first, gain_second, gate_second, up_second, down_second
):
    fs, n_tp = lax.axis_size("fs"), lax.axis_size("tp")
    n = int(round(fs**0.5))
    fd, local = gate_first.shape
    hu = local // fs
    d = fs * fd
    rows = tokens.shape[1]
    block = rows // 2 // n
    wide = -(-(local + ROWS) // 128) * 128
    vmem = pl.BlockSpec(memory_space=pltpu.VMEM)
    hbm = pl.BlockSpec(memory_space=pltpu.HBM)
    dma, one = pltpu.SemaphoreType.DMA, (2,)
    results = pl.pallas_call(
        functools.partial(kernel, n, n_tp, hu, fd),
        out_shape=(
            jax.ShapeDtypeStruct((OWN, d), BF16),
        )
        + (jax.ShapeDtypeStruct((hu, n_tp, d), BF16),) * 6,
        in_specs=[hbm] * 9,
        out_specs=(vmem,) + (hbm,) * 6,
        scratch_shapes=[
            pltpu.VMEM((rows, d), BF16),
            pltpu.VMEM((2, 1, fd), F32),
            pltpu.VMEM((2, 3, fd, local), F32),
            pltpu.VMEM((4 * fd, wide), F32),
            pltpu.VMEM((wide, 4 * fd), F32),
            pltpu.VMEM((2, fs, ROWS, 128), BF16),
            pltpu.VMEM((2, 4, fs // 4, ROWS, 128), BF16),
            pltpu.VMEM((2, n_tp, 3, ROWS, d), BF16),
            pltpu.VMEM((8, 128), BF16),
            pltpu.VMEM((rows, d), BF16),
            pltpu.VMEM((2, 2 * n, block, d), BF16),
            pltpu.VMEM((2, 2, n, block, d), BF16),
            pltpu.VMEM((2, 2, n // 2, OWN, d), BF16),
            pltpu.VMEM((2, n, OWN, d), BF16),
            pltpu.VMEM((n, OWN, d), BF16),
            pltpu.VMEM((2, n, block, d), BF16),
            pltpu.VMEM((OWN, d), BF16),
            pltpu.VMEM((6, hu, n_tp, d), BF16),
            dma(one), dma(one), dma((2, n_tp - 1)), dma((2, n_tp)),
            dma(one), dma(one), dma(one), dma(one), dma(one),
            dma(()), dma(()), dma(()), dma(()), dma(()), dma((2, 5)), dma((2, 3)),
        ],
        compiler_params=pltpu.CompilerParams(
            collective_id=0, has_side_effects=True, vmem_limit_bytes=67043328
        ),
    )(
        tokens[0],
        gain_first[None], gate_first, up_first, down_first,
        gain_second[None], gate_second, up_second, down_second,
    )
    mixed, *served = pl.pallas_call(
        functools.partial(deliver, 7),
        out_shape=tuple(jax.ShapeDtypeStruct(r.shape, r.dtype) for r in results),
        in_specs=[hbm] * 7,
        out_specs=(hbm,) * 7,
        scratch_shapes=[pltpu.VMEM(r.shape, r.dtype) for r in results] + [dma((7,)), dma((7,))],
    )(*results)
    return (mixed[None],) + tuple(jnp.swapaxes(r, 0, 1) for r in served)


def solution(mesh):
    weight = P("fs", "tp")
    cut = P(None, "fs", None)
    return jax.shard_map(
        shards,
        mesh=mesh,
        in_specs=(P("tp", None, None), P("fs"), weight, weight, weight, P("fs"), weight, weight, weight),
        out_specs=(P("tp", "fs", None),) + (cut,) * 6,
        check_vma=False,
    )
```

```python
import functools

import jax
import jax.numpy as jnp
from jax import lax
from jax.experimental import pallas as pl
from jax.experimental.pallas import tpu as pltpu
from jax.sharding import PartitionSpec as P

MESH = pl.DeviceIdType.MESH
F32, BF16 = jnp.float32, jnp.bfloat16
ROWS = 16
OWN = 4


def rsqrt_norm(wide):
    scale = lax.rsqrt(jnp.mean(wide * wide, axis=-1, keepdims=True) + 1e-06)
    return (wide * scale).astype(BF16)


def kernel(
    n, n_tp, hu, fd,
    tokens_hbm, gain_one, gate_one, up_one, down_one, gain_two, gate_two, up_two, down_two,
    mixed, out_0, out_1, out_2, out_3, out_4, out_5,
    tokens, gains, trained, stack, turned, outgoing, incoming, weights, normed,
    part, landed, group, owner, small, gathered_a, gathered_b, part_a, part_b, landed_a, landed_b,
    group_a, group_b, owner_two, middle, staged,
    w_send, w_recv, x_send, x_recv, half_recv, pair_send, pair_recv, r_send, ra_recv, rb_recv,
    q_send, q_recv, s_send, s_recv, g_send, ga_recv, gb_recv, in_sem, out_sem,
):
    served = (out_0, out_1, out_2, out_3, out_4, out_5)
    fs = n * n
    d = fs * fd
    half = OWN * fs // 2
    block = half // n
    groups = n // 2
    m = n // 2
    f, t = lax.axis_index("fs"), lax.axis_index("tp")
    z, y = f // n, lax.rem(f, n)
    e, q = lax.rem(y, 2), y // 2
    x, c = t // 2, lax.rem(t, 2)
    nx = n_tp // 2
    even = lax.rem(z + y, 2) == 0
    even_two = lax.rem(z + q, 2) == 0
    partner = (f, x * 2 + 1 - c)

    def at(zz, yy):
        return (zz * n + yy, t)

    def at_two(zz, qq):
        return (zz * n + 2 * qq + e, t)

    def along(step):
        return (f, lax.rem(x + nx + step, nx) * 2 + c)

    def slot_of(step, core):
        return lax.rem(x + nx + step, nx) * 2 + core

    def remote(src, dst, send, recv, device):
        return pltpu.make_async_remote_copy(
            src_ref=src, dst_ref=dst, send_sem=send, recv_sem=recv, device_id=device, device_id_type=MESH
        )

    def drain(ref, sem):
        pltpu.make_async_copy(ref, ref, sem).wait()

    given = ((gain_one, gate_one, up_one, down_one), (gain_two, gate_two, up_two, down_two))
    loads = []
    for b, (gain, *each) in enumerate(given):
        loads.append(pltpu.make_async_copy(gain, gains.at[b], in_sem.at[b, 3]))
        for w in range(3):
            loads.append(pltpu.make_async_copy(each[w], trained.at[b, w], in_sem.at[b, w]))
    loads.append(pltpu.make_async_copy(tokens_hbm, tokens, in_sem.at[0, 4]))
    for load in loads:
        load.start()
    owner_two[...] = jnp.zeros_like(owner_two)

    barrier = pltpu.get_barrier_semaphore()

    @pl.loop(1, fs)
    def _(k):
        pl.semaphore_signal(barrier, inc=1, device_id=(lax.rem(f + k, fs), t), device_id_type=MESH)

    around = {1: (), 2: (1,), 4: (1, -1)}[nx]
    for step in around:
        pl.semaphore_signal(barrier, inc=1, device_id=along(step), device_id_type=MESH)
    pl.semaphore_signal(barrier, inc=1, device_id=partner, device_id_type=MESH)

    hidden_units = gate_one.shape[1]
    stack[...] = jnp.zeros_like(stack)
    for b in range(2):
        for load in loads[4 * b : 4 * b + 4]:
            load.wait()
        for w in range(3):
            stack[w * fd : (w + 1) * fd, 0:hidden_units] = trained[b, w]
        ones = jnp.ones((1, fd), F32)
        scale = jnp.concatenate([gains[b], gains[b], ones, ones], axis=1)
        turned[...] = stack[...].T * scale
        live = lax.broadcasted_iota(jnp.int32, (ROWS, 128), 0) < hu
        for k in range(fs):
            rows = turned[k * hu : k * hu + ROWS, :]
            outgoing[b, k] = jnp.where(live, rows, 0.0).astype(BF16)

    pl.semaphore_wait(barrier, fs - 1 + len(around) + 1)

    for b in range(2):

        @pl.loop(1, fs)
        def _(k):
            peer = lax.rem(f + k, fs)
            remote(
                outgoing.at[b, peer],
                incoming.at[b, lax.rem(f, 4), f // 4],
                w_send.at[b],
                w_recv.at[b],
                (peer, t),
            ).start()

        pltpu.make_async_copy(
            outgoing.at[b, f], incoming.at[b, lax.rem(f, 4), f // 4], w_recv.at[b]
        ).start()

    loads[8].wait()
    wide = tokens[...].astype(F32)
    normed_rows = rsqrt_norm(wide)
    spot = lax.broadcasted_iota(jnp.int32, (2 * half, 2 * half), 0)
    source = lax.broadcasted_iota(jnp.int32, (2 * half, 2 * half), 1)
    in_first = spot < half
    inside = jnp.where(in_first, spot, spot - half)
    major = inside // block
    minor = (inside % block) // OWN
    row = inside % OWN
    first_home = major * n + 2 * minor + major % 2
    second_home = (2 * minor + (major + 1) % 2) * n + major
    home = jnp.where(in_first, first_home, second_home) * OWN + row
    shuffle = jnp.where(home == source, 1.0, 0.0).astype(BF16)
    normed[...] = jnp.dot(shuffle, normed_rows, preferred_element_type=F32).astype(BF16)
    pick_row = lax.broadcasted_iota(jnp.int32, (8, 2 * half), 0)
    pick_source = lax.broadcasted_iota(jnp.int32, (8, 2 * half), 1)
    pick = jnp.where((pick_row < OWN) & (pick_source == pick_row + f * OWN), 1.0, 0.0).astype(BF16)
    mine = jnp.dot(pick, tokens[...], preferred_element_type=F32)[0:OWN]

    lanes = 3 * 128
    lane_in = lax.broadcasted_iota(jnp.int32, (128, lanes), 0)
    lane_out = lax.broadcasted_iota(jnp.int32, (128, lanes), 1)
    inner = lane_out % 128

    def merge(b):
        drain(incoming.at[b], w_recv.at[b])
        total = jnp.zeros((fs // 4 * ROWS, lanes), F32)
        for i in range(4):
            chosen = (inner // 32 == i) & (lane_in == lane_out // 128 * 32 + inner % 32)
            spread_out = jnp.where(chosen, 1.0, 0.0).astype(BF16)
            piece = incoming[b, i].reshape(fs // 4 * ROWS, 128)
            total = total + jnp.dot(piece, spread_out, preferred_element_type=F32)
        merged = total.astype(BF16)
        for j in range(fs // 4):
            for w in range(3):
                weights[b, t, w, :, j * 128 : (j + 1) * 128] = merged[
                    j * ROWS : (j + 1) * ROWS, w * 128 : (w + 1) * 128
                ]

    def part_of(s, slot, h):
        return weights.at[s, slot, :, :, h * (d // 2) : (h + 1) * (d // 2)]

    def spread(s):
        for step in around:
            remote(weights.at[s, t], weights.at[s, t], x_send.at[s], x_recv.at[s, t], along(step)).start()
        remote(weights.at[s, t], weights.at[s, t], x_send.at[s], x_recv.at[s, t], partner).start()

    def relay(s):
        for h, step in enumerate(around):
            slot = slot_of(-step, c)
            drain(weights.at[s, slot], x_recv.at[s, slot])
            if nx == 4:
                remote(
                    part_of(s, slot, h), part_of(s, slot, h), x_send.at[s], half_recv.at[s, h], along(step)
                ).start()
            remote(
                weights.at[s, slot], weights.at[s, slot], x_send.at[s], x_recv.at[s, slot], partner
            ).start()

    def finish(s):
        if nx == 4:
            slot = slot_of(2, c)
            for h in range(2):
                drain(part_of(s, slot, h), half_recv.at[s, h])
                remote(
                    part_of(s, slot, h), part_of(s, slot, h), x_send.at[s], x_recv.at[s, slot], partner
                ).start()

    def collected(s):
        for k in range(nx):
            slot = slot_of(k, 1 - c)
            drain(weights.at[s, slot], x_recv.at[s, slot])

    def shipped(b, w):
        return pltpu.make_async_copy(staged.at[3 * b + w], served[3 * b + w], out_sem.at[b, w])

    def publish(b):
        width = hu * n_tp
        spot = lax.broadcasted_iota(jnp.int32, (width, n_tp * ROWS), 0)
        source = lax.broadcasted_iota(jnp.int32, (width, n_tp * ROWS), 1)
        swap = jnp.where(source == spot % n_tp * ROWS + spot // n_tp, 1.0, 0.0).astype(BF16)
        for w in range(3):
            held = weights[b, :, w].reshape(n_tp * ROWS, d)
            rows = jnp.dot(swap, held, preferred_element_type=F32)
            for r in range(hu):
                staged[3 * b + w, r] = rows[r * n_tp : (r + 1) * n_tp].astype(BF16)
            shipped(b, w).start()

    contract = (((1,), (1,)), ((), ()))

    def branch_of(rows, sets):
        gate, up, down = [
            jnp.concatenate([weights[s, :, w].reshape(n_tp * ROWS, d) for s in sets], axis=0)
            for w in range(3)
        ]
        gate_act = lax.dot_general(rows, gate, contract, preferred_element_type=F32)
        up_act = lax.dot_general(rows, up, contract, preferred_element_type=F32)
        act = (gate_act / (1.0 + jnp.exp(-gate_act)) * up_act).astype(BF16)
        return jnp.dot(act, down, preferred_element_type=F32).astype(BF16)

    def send_blocks(source, target, me, count, send, recv, device):
        @pl.loop(1, count)
        def _(k):
            peer = lax.rem(me + k, count)
            remote(source.at[peer], target.at[me], send, recv, device(peer)).start()

        pltpu.make_async_copy(source.at[me], target.at[me], recv).start()

    def reduced(target, count, recv):
        drain(target, recv)
        total = target[0].astype(F32)
        for k in range(1, count):
            total = total + target[k].astype(F32)
        return total

    def hand_groups(total, held, targets, me, own, send, recv, device):
        for k, peer in enumerate(targets):
            held[k] = total[k * OWN : (k + 1) * OWN].astype(BF16)

            @pl.when(peer != me)
            def _():
                remote(held.at[k], own.at[me], send, recv, device(peer)).start()

            @pl.when(peer == me)
            def _():
                pltpu.make_async_copy(held.at[k], own.at[me], recv).start()

    def added(own):
        total = own[0].astype(F32)
        for k in range(1, n):
            total = total + own[k].astype(F32)
        return total

    merge(0)
    spread(0)
    relay(0)
    finish(0)
    collected(0)
    for side in range(2):
        rows = normed[side * half : (side + 1) * half, :]
        part[side * n : (side + 1) * n] = branch_of(rows, (0,)).reshape(n, block, d)
        send_blocks(
            part.at[pl.ds(side * n, n)],
            landed.at[side],
            z if side == 0 else y,
            n,
            r_send.at[0],
            (ra_recv if side == 0 else rb_recv).at[0],
            (lambda peer: at(peer, y)) if side == 0 else (lambda peer: at(z, peer)),
        )
    merge(1)
    spread(1)
    twin = (z * n + y + 1 - 2 * e, t)
    remote(weights.at[1, t], weights.at[2, t], pair_send, pair_recv, twin).start()
    publish(0)
    drain(weights.at[2, t], pair_recv)
    spread(2)
    total = reduced(landed.at[0], n, ra_recv.at[0])
    hand_groups(
        total, group.at[0], [2 * k + lax.rem(z, 2) for k in range(groups)], y,
        owner, q_send.at[0], q_recv.at[0], lambda peer: at(z, peer),
    )
    total = reduced(landed.at[1], n, rb_recv.at[0])
    hand_groups(
        total, group.at[1], [2 * k + lax.rem(y + 1, 2) for k in range(groups)], z,
        owner, q_send.at[0], q_recv.at[0], lambda peer: at(peer, y),
    )
    relay(1)
    drain(owner, q_recv.at[0])
    middle[...] = (mine + 0.5 * added(owner)).astype(BF16)
    mid = middle[...].astype(F32)
    own_slot = jnp.where(even_two, q // 2, m // 2 + z // 2)
    small[own_slot] = rsqrt_norm(mid)
    for k in range(1, n):
        peer = jnp.where(even_two, z * n + 2 * lax.rem(q + k, m) + e, lax.rem(z + k, n) * n + y)

        def tell():
            remote(small.at[own_slot], small.at[own_slot], s_send, s_recv, (peer, t)).start()

        if k < m:
            tell()
        else:
            pl.when(jnp.logical_not(even_two))(tell)
    finish(1)
    drain(small.at[pl.ds(0, m // 2 + groups - 1)], s_recv)
    rows = jnp.concatenate([small[k].astype(F32) for k in range(m // 2)], axis=0)
    gathered_a[z] = rows.astype(BF16)
    rows = jnp.concatenate([small[m // 2 + k].astype(F32) for k in range(groups)], axis=0)
    gathered_b[q] = rows.astype(BF16)

    @pl.loop(1, n)
    def _(k):
        remote(
            gathered_a.at[z], gathered_a.at[z], g_send.at[0], ga_recv, at_two(lax.rem(z + k, n), q)
        ).start()

    @pl.loop(1, m)
    def _(k):
        remote(
            gathered_b.at[q], gathered_b.at[q], g_send.at[1], gb_recv, at_two(z, lax.rem(q + k, m))
        ).start()

    relay(2)
    finish(2)
    collected(1)
    collected(2)
    drain(gathered_a.at[pl.ds(0, n - 1)], ga_recv)
    drain(gathered_b.at[pl.ds(0, m - 1)], gb_recv)
    quarter = half // 2
    rows = jnp.concatenate(
        [gathered_a[...].reshape(quarter, d), gathered_b[...].reshape(quarter, d)], axis=0
    )
    branch = branch_of(rows, (1, 2))
    part_a[...] = branch[0:quarter].reshape(part_a.shape)
    part_b[...] = branch[quarter:].reshape(part_b.shape)
    send_blocks(part_a, landed_a, z, n, r_send.at[1], ra_recv.at[1], lambda peer: at_two(peer, q))
    send_blocks(part_b, landed_b, q, m, r_send.at[2], rb_recv.at[1], lambda peer: at_two(z, peer))
    publish(1)
    total = reduced(landed_a, n, ra_recv.at[1])
    hand_groups(
        total, group_a, [2 * k + lax.rem(z, 2) for k in range(m // 2)], q,
        owner_two, q_send.at[1], q_recv.at[1], lambda peer: at_two(z, peer),
    )
    total = reduced(landed_b, m, rb_recv.at[1])
    hand_groups(
        total, group_b, [2 * k + lax.rem(q + 1, 2) for k in range(groups)], z,
        owner_two, q_send.at[1], q_recv.at[1], lambda peer: at_two(peer, q),
    )

    @pl.when(even_two)
    def _():
        drain(owner_two.at[pl.ds(0, m)], q_recv.at[1])
        drain(small.at[pl.ds(0, m - 1)], s_send)

    @pl.when(jnp.logical_not(even_two))
    def _():
        drain(owner_two, q_recv.at[1])
        drain(owner.at[pl.ds(0, n - 1)], s_send)

    mixed[...] = (mid + 0.5 * added(owner_two)).astype(BF16)

    drain(weights.at[2, t], pair_send)
    for s in range(3):
        drain(weights.at[s, pl.ds(0, n_tp - 1)], x_send.at[s])
    drain(gathered_a.at[pl.ds(0, n - 1)], g_send.at[0])
    drain(gathered_b.at[pl.ds(0, m - 1)], g_send.at[1])
    drain(part.at[pl.ds(0, 2 * n - 2)], r_send.at[0])
    drain(part_a.at[pl.ds(0, n - 1)], r_send.at[1])
    drain(part_b.at[pl.ds(0, m - 1)], r_send.at[2])
    drain(owner.at[pl.ds(0, n - 1)], q_send.at[0])
    drain(owner_two.at[pl.ds(0, m // 2 + groups - 1)], q_send.at[1])
    for b in range(2):
        drain(outgoing.at[b, pl.ds(0, fs - 1)], w_send.at[b])
        for w in range(3):
            shipped(b, w).wait()


def deliver(count, *refs):
    sources, targets, held = refs[:count], refs[count : 2 * count], refs[2 * count : 3 * count]
    in_sem, out_sem = refs[3 * count :]
    taken = [pltpu.make_async_copy(sources[k], held[k], in_sem.at[k]) for k in range(count)]
    given = [pltpu.make_async_copy(held[k], targets[k], out_sem.at[k]) for k in range(count)]
    for copy in taken:
        copy.start()
    for k in range(count):
        taken[k].wait()
        given[k].start()
    for copy in given:
        copy.wait()


def shards(
    tokens, gain_first, gate_first, up_first, down_first, gain_second, gate_second, up_second, down_second
):
    fs, n_tp = lax.axis_size("fs"), lax.axis_size("tp")
    n = int(round(fs**0.5))
    fd, local = gate_first.shape
    hu = local // fs
    d = fs * fd
    rows = tokens.shape[1]
    block = rows // 2 // n
    wide = -(-(local + ROWS) // 128) * 128
    vmem = pl.BlockSpec(memory_space=pltpu.VMEM)
    hbm = pl.BlockSpec(memory_space=pltpu.HBM)
    dma = pltpu.SemaphoreType.DMA
    m = n // 2
    shape_a = (n, OWN * m // 2, d)
    shape_b = (m, OWN * n // 2, d)
    results = pl.pallas_call(
        functools.partial(kernel, n, n_tp, hu, fd),
        out_shape=(
            jax.ShapeDtypeStruct((OWN, d), BF16),
        )
        + (jax.ShapeDtypeStruct((hu, n_tp, d), BF16),) * 6,
        in_specs=[hbm] * 9,
        out_specs=(vmem,) + (hbm,) * 6,
        scratch_shapes=[
            pltpu.VMEM((rows, d), BF16),
            pltpu.VMEM((2, 1, fd), F32),
            pltpu.VMEM((2, 3, fd, local), F32),
            pltpu.VMEM((4 * fd, wide), F32),
            pltpu.VMEM((wide, 4 * fd), F32),
            pltpu.VMEM((2, fs, ROWS, 128), BF16),
            pltpu.VMEM((2, 4, fs // 4, ROWS, 128), BF16),
            pltpu.VMEM((3, n_tp, 3, ROWS, d), BF16),
            pltpu.VMEM((rows, d), BF16),
            pltpu.VMEM((2 * n, block, d), BF16),
            pltpu.VMEM((2, n, block, d), BF16),
            pltpu.VMEM((2, m, OWN, d), BF16),
            pltpu.VMEM((n, OWN, d), BF16),
            pltpu.VMEM((m // 2 + m, OWN, d), BF16),
            pltpu.VMEM(shape_a, BF16),
            pltpu.VMEM(shape_b, BF16),
            pltpu.VMEM(shape_a, BF16),
            pltpu.VMEM(shape_b, BF16),
            pltpu.VMEM(shape_a, BF16),
            pltpu.VMEM(shape_b, BF16),
            pltpu.VMEM((m // 2, OWN, d), BF16),
            pltpu.VMEM((m, OWN, d), BF16),
            pltpu.VMEM((n, OWN, d), BF16),
            pltpu.VMEM((OWN, d), BF16),
            pltpu.VMEM((6, hu, n_tp, d), BF16),
            dma((2,)), dma((2,)), dma((3,)), dma((3, n_tp)), dma((3, 2)), dma(()), dma(()),
            dma((3,)), dma((2,)), dma((2,)), dma((2,)), dma((2,)), dma(()), dma(()),
            dma((2,)), dma(()), dma(()), dma((2, 5)), dma((2, 3)),
        ],
        compiler_params=pltpu.CompilerParams(
            collective_id=0, has_side_effects=True, vmem_limit_bytes=67043328
        ),
    )(
        tokens[0],
        gain_first[None], gate_first, up_first, down_first,
        gain_second[None], gate_second, up_second, down_second,
    )
    mixed, *served = pl.pallas_call(
        functools.partial(deliver, 7),
        out_shape=tuple(jax.ShapeDtypeStruct(r.shape, r.dtype) for r in results),
        in_specs=[hbm] * 7,
        out_specs=(hbm,) * 7,
        scratch_shapes=[pltpu.VMEM(r.shape, r.dtype) for r in results] + [dma((7,)), dma((7,))],
    )(*results)
    return (mixed[None],) + tuple(jnp.swapaxes(r, 0, 1) for r in served)


def solution(mesh):
    weight = P("fs", "tp")
    cut = P(None, "fs", None)
    return jax.shard_map(
        shards,
        mesh=mesh,
        in_specs=(P("tp", None, None), P("fs"), weight, weight, weight, P("fs"), weight, weight, weight),
        out_specs=(P("tp", "fs", None),) + (cut,) * 6,
        check_vma=False,
    )
```

```python
import functools

import jax
import jax.numpy as jnp
from jax import lax
from jax.experimental import pallas as pl
from jax.experimental.pallas import tpu as pltpu
from jax.sharding import PartitionSpec as P

MESH = pl.DeviceIdType.MESH
F32, BF16 = jnp.float32, jnp.bfloat16
ROWS = 16
OWN = 4


def far_first(count):
    return sorted(range(1, count), key=lambda k: (-min(k, count - k), k))


def rsqrt_norm(wide):
    scale = lax.rsqrt(jnp.mean(wide * wide, axis=-1, keepdims=True) + 1e-06)
    return (wide * scale).astype(BF16)


def kernel(
    n, n_tp, hu, fd,
    tokens_hbm, gain_one, gate_one, up_one, down_one, gain_two, gate_two, up_two, down_two,
    mixed, out_0, out_1, out_2, out_3, out_4, out_5,
    tokens, gains, trained, stack, turned, outgoing, incoming, weights, normed,
    part, landed, group, owner, small, gathered_a, gathered_b, part_a, part_b, landed_a, landed_b,
    group_a, group_b, owner_two, middle, staged,
    w_send, w_recv, x_send, x_recv, half_recv, pair_send, pair_recv, r_send, ra_recv, rb_recv,
    q_send, q_recv, s_send, s_recv, g_send, ga_recv, gb_recv, in_sem, out_sem,
):
    served = (out_0, out_1, out_2, out_3, out_4, out_5)
    fs = n * n
    d = fs * fd
    half = OWN * fs // 2
    block = half // n
    groups = n // 2
    m = n // 2
    f, t = lax.axis_index("fs"), lax.axis_index("tp")
    z, y = f // n, lax.rem(f, n)
    e, q = lax.rem(y, 2), y // 2
    x, c = t // 2, lax.rem(t, 2)
    nx = n_tp // 2
    even = lax.rem(z + y, 2) == 0
    even_two = lax.rem(z + q, 2) == 0
    partner = (f, x * 2 + 1 - c)

    def at(zz, yy):
        return (zz * n + yy, t)

    def at_two(zz, qq):
        return (zz * n + 2 * qq + e, t)

    def along(step):
        return (f, lax.rem(x + nx + step, nx) * 2 + c)

    def slot_of(step, core):
        return lax.rem(x + nx + step, nx) * 2 + core

    def remote(src, dst, send, recv, device):
        return pltpu.make_async_remote_copy(
            src_ref=src, dst_ref=dst, send_sem=send, recv_sem=recv, device_id=device, device_id_type=MESH
        )

    def drain(ref, sem):
        pltpu.make_async_copy(ref, ref, sem).wait()

    given = ((gain_one, gate_one, up_one, down_one), (gain_two, gate_two, up_two, down_two))
    loads = []
    for b, (gain, *each) in enumerate(given):
        loads.append(pltpu.make_async_copy(gain, gains.at[b], in_sem.at[b, 3]))
        for w in range(3):
            loads.append(pltpu.make_async_copy(each[w], trained.at[b, w], in_sem.at[b, w]))
    loads.append(pltpu.make_async_copy(tokens_hbm, tokens, in_sem.at[0, 4]))
    for load in loads:
        load.start()
    owner_two[...] = jnp.zeros_like(owner_two)

    barrier = pltpu.get_barrier_semaphore()

    @pl.loop(1, fs)
    def _(k):
        pl.semaphore_signal(barrier, inc=1, device_id=(lax.rem(f + k, fs), t), device_id_type=MESH)

    around = {1: (), 2: (1,), 4: (1, -1)}[nx]
    for step in around:
        pl.semaphore_signal(barrier, inc=1, device_id=along(step), device_id_type=MESH)
    pl.semaphore_signal(barrier, inc=1, device_id=partner, device_id_type=MESH)

    hidden_units = gate_one.shape[1]
    stack[...] = jnp.zeros_like(stack)
    for b in range(2):
        for load in loads[4 * b : 4 * b + 4]:
            load.wait()
        for w in range(3):
            stack[w * fd : (w + 1) * fd, 0:hidden_units] = trained[b, w]
        ones = jnp.ones((1, fd), F32)
        scale = jnp.concatenate([gains[b], gains[b], ones, ones], axis=1)
        turned[...] = stack[...].T * scale
        live = lax.broadcasted_iota(jnp.int32, (ROWS, 128), 0) < hu
        for k in range(fs):
            rows = turned[k * hu : k * hu + ROWS, :]
            outgoing[b, k] = jnp.where(live, rows, 0.0).astype(BF16)

    pl.semaphore_wait(barrier, fs - 1 + len(around) + 1)

    offsets = [(dz, dy) for dz in range(n) for dy in range(n) if dz or dy]
    offsets.sort(key=lambda o: -(min(o[0], n - o[0]) + min(o[1], n - o[1])))
    for b in range(2):
        for dz, dy in offsets:
            peer = lax.rem(z + dz, n) * n + lax.rem(y + dy, n)
            remote(
                outgoing.at[b, peer],
                incoming.at[b, lax.rem(f, 4), f // 4],
                w_send.at[b],
                w_recv.at[b],
                (peer, t),
            ).start()

        pltpu.make_async_copy(
            outgoing.at[b, f], incoming.at[b, lax.rem(f, 4), f // 4], w_recv.at[b]
        ).start()

    loads[8].wait()
    wide = tokens[...].astype(F32)
    normed_rows = rsqrt_norm(wide)
    spot = lax.broadcasted_iota(jnp.int32, (2 * half, 2 * half), 0)
    source = lax.broadcasted_iota(jnp.int32, (2 * half, 2 * half), 1)
    in_first = spot < half
    inside = jnp.where(in_first, spot, spot - half)
    major = inside // block
    minor = (inside % block) // OWN
    row = inside % OWN
    first_home = major * n + 2 * minor + major % 2
    second_home = (2 * minor + (major + 1) % 2) * n + major
    home = jnp.where(in_first, first_home, second_home) * OWN + row
    shuffle = jnp.where(home == source, 1.0, 0.0).astype(BF16)
    normed[...] = jnp.dot(shuffle, normed_rows, preferred_element_type=F32).astype(BF16)
    pick_row = lax.broadcasted_iota(jnp.int32, (8, 2 * half), 0)
    pick_source = lax.broadcasted_iota(jnp.int32, (8, 2 * half), 1)
    pick = jnp.where((pick_row < OWN) & (pick_source == pick_row + f * OWN), 1.0, 0.0).astype(BF16)
    mine = jnp.dot(pick, tokens[...], preferred_element_type=F32)[0:OWN]

    lanes = 3 * 128
    lane_in = lax.broadcasted_iota(jnp.int32, (128, lanes), 0)
    lane_out = lax.broadcasted_iota(jnp.int32, (128, lanes), 1)
    inner = lane_out % 128

    def merge(b):
        drain(incoming.at[b], w_recv.at[b])
        total = jnp.zeros((fs // 4 * ROWS, lanes), F32)
        for i in range(4):
            chosen = (inner // 32 == i) & (lane_in == lane_out // 128 * 32 + inner % 32)
            spread_out = jnp.where(chosen, 1.0, 0.0).astype(BF16)
            piece = incoming[b, i].reshape(fs // 4 * ROWS, 128)
            total = total + jnp.dot(piece, spread_out, preferred_element_type=F32)
        merged = total.astype(BF16)
        for j in range(fs // 4):
            for w in range(3):
                weights[b, t, w, :, j * 128 : (j + 1) * 128] = merged[
                    j * ROWS : (j + 1) * ROWS, w * 128 : (w + 1) * 128
                ]

    def part_of(s, slot, h):
        return weights.at[s, slot, :, :, h * (d // 2) : (h + 1) * (d // 2)]

    def spread(s):
        for step in around:
            remote(weights.at[s, t], weights.at[s, t], x_send.at[s], x_recv.at[s, t], along(step)).start()
        remote(weights.at[s, t], weights.at[s, t], x_send.at[s], x_recv.at[s, t], partner).start()

    def relay(s):
        for h, step in enumerate(around):
            slot = slot_of(-step, c)
            drain(weights.at[s, slot], x_recv.at[s, slot])
            if nx == 4:
                remote(
                    part_of(s, slot, h), part_of(s, slot, h), x_send.at[s], half_recv.at[s, h], along(step)
                ).start()
            remote(
                weights.at[s, slot], weights.at[s, slot], x_send.at[s], x_recv.at[s, slot], partner
            ).start()

    def finish(s):
        if nx == 4:
            slot = slot_of(2, c)
            for h in range(2):
                drain(part_of(s, slot, h), half_recv.at[s, h])
                remote(
                    part_of(s, slot, h), part_of(s, slot, h), x_send.at[s], x_recv.at[s, slot], partner
                ).start()

    def collected(s):
        for k in range(nx):
            slot = slot_of(k, 1 - c)
            drain(weights.at[s, slot], x_recv.at[s, slot])

    def shipped(b, w):
        return pltpu.make_async_copy(staged.at[3 * b + w], served[3 * b + w], out_sem.at[b, w])

    def publish(b):
        width = hu * n_tp
        spot = lax.broadcasted_iota(jnp.int32, (width, n_tp * ROWS), 0)
        source = lax.broadcasted_iota(jnp.int32, (width, n_tp * ROWS), 1)
        swap = jnp.where(source == spot % n_tp * ROWS + spot // n_tp, 1.0, 0.0).astype(BF16)
        for w in range(3):
            held = weights[b, :, w].reshape(n_tp * ROWS, d)
            rows = jnp.dot(swap, held, preferred_element_type=F32)
            for r in range(hu):
                staged[3 * b + w, r] = rows[r * n_tp : (r + 1) * n_tp].astype(BF16)
            shipped(b, w).start()

    contract = (((1,), (1,)), ((), ()))

    def branch_of(rows, sets):
        gate, up, down = [
            jnp.concatenate([weights[s, :, w].reshape(n_tp * ROWS, d) for s in sets], axis=0)
            for w in range(3)
        ]
        gate_act = lax.dot_general(rows, gate, contract, preferred_element_type=F32)
        up_act = lax.dot_general(rows, up, contract, preferred_element_type=F32)
        act = (gate_act / (1.0 + jnp.exp(-gate_act)) * up_act).astype(BF16)
        return jnp.dot(act, down, preferred_element_type=F32).astype(BF16)

    def send_blocks(source, target, me, count, send, recv, device):
        for k in far_first(count):
            peer = lax.rem(me + k, count)
            remote(source.at[peer], target.at[me], send, recv, device(peer)).start()

        pltpu.make_async_copy(source.at[me], target.at[me], recv).start()

    def reduced(target, count, recv):
        drain(target, recv)
        total = target[0].astype(F32)
        for k in range(1, count):
            total = total + target[k].astype(F32)
        return total

    def hand_groups(total, held, targets, me, own, send, recv, device):
        for k, peer in enumerate(targets):
            held[k] = total[k * OWN : (k + 1) * OWN].astype(BF16)

            @pl.when(peer != me)
            def _():
                remote(held.at[k], own.at[me], send, recv, device(peer)).start()

            @pl.when(peer == me)
            def _():
                pltpu.make_async_copy(held.at[k], own.at[me], recv).start()

    def added(own):
        total = own[0].astype(F32)
        for k in range(1, n):
            total = total + own[k].astype(F32)
        return total

    merge(0)
    spread(0)
    relay(0)
    merge(1)
    twin = (z * n + y + 1 - 2 * e, t)
    remote(weights.at[1, t], weights.at[2, t], pair_send, pair_recv, twin).start()
    finish(0)
    collected(0)
    for side in range(2):
        rows = normed[side * half : (side + 1) * half, :]
        part[side * n : (side + 1) * n] = branch_of(rows, (0,)).reshape(n, block, d)
        send_blocks(
            part.at[pl.ds(side * n, n)],
            landed.at[side],
            z if side == 0 else y,
            n,
            r_send.at[0],
            (ra_recv if side == 0 else rb_recv).at[0],
            (lambda peer: at(peer, y)) if side == 0 else (lambda peer: at(z, peer)),
        )
    spread(1)
    drain(weights.at[2, t], pair_recv)
    spread(2)
    publish(0)
    relay(1)
    total = reduced(landed.at[0], n, ra_recv.at[0])
    hand_groups(
        total, group.at[0], [2 * k + lax.rem(z, 2) for k in range(groups)], y,
        owner, q_send.at[0], q_recv.at[0], lambda peer: at(z, peer),
    )
    total = reduced(landed.at[1], n, rb_recv.at[0])
    hand_groups(
        total, group.at[1], [2 * k + lax.rem(y + 1, 2) for k in range(groups)], z,
        owner, q_send.at[0], q_recv.at[0], lambda peer: at(peer, y),
    )
    relay(2)
    drain(owner, q_recv.at[0])
    middle[...] = (mine + 0.5 * added(owner)).astype(BF16)
    mid = middle[...].astype(F32)
    own_slot = jnp.where(even_two, q // 2, m // 2 + z // 2)
    small[own_slot] = rsqrt_norm(mid)
    for k in range(1, n):
        peer = jnp.where(even_two, z * n + 2 * lax.rem(q + k, m) + e, lax.rem(z + k, n) * n + y)

        def tell():
            remote(small.at[own_slot], small.at[own_slot], s_send, s_recv, (peer, t)).start()

        if k < m:
            tell()
        else:
            pl.when(jnp.logical_not(even_two))(tell)
    drain(small.at[pl.ds(0, m // 2 + groups - 1)], s_recv)
    rows = jnp.concatenate([small[k].astype(F32) for k in range(m // 2)], axis=0)
    gathered_a[z] = rows.astype(BF16)
    rows = jnp.concatenate([small[m // 2 + k].astype(F32) for k in range(groups)], axis=0)
    gathered_b[q] = rows.astype(BF16)

    for k in far_first(n):
        remote(
            gathered_a.at[z], gathered_a.at[z], g_send.at[0], ga_recv, at_two(lax.rem(z + k, n), q)
        ).start()
    for k in far_first(m):
        remote(
            gathered_b.at[q], gathered_b.at[q], g_send.at[1], gb_recv, at_two(z, lax.rem(q + k, m))
        ).start()
    finish(1)
    finish(2)
    collected(1)
    collected(2)
    drain(gathered_a.at[pl.ds(0, n - 1)], ga_recv)
    drain(gathered_b.at[pl.ds(0, m - 1)], gb_recv)
    quarter = half // 2
    rows = jnp.concatenate(
        [gathered_a[...].reshape(quarter, d), gathered_b[...].reshape(quarter, d)], axis=0
    )
    branch = branch_of(rows, (1, 2))
    part_a[...] = branch[0:quarter].reshape(part_a.shape)
    part_b[...] = branch[quarter:].reshape(part_b.shape)
    send_blocks(part_a, landed_a, z, n, r_send.at[1], ra_recv.at[1], lambda peer: at_two(peer, q))
    send_blocks(part_b, landed_b, q, m, r_send.at[2], rb_recv.at[1], lambda peer: at_two(z, peer))
    publish(1)
    total = reduced(landed_a, n, ra_recv.at[1])
    hand_groups(
        total, group_a, [2 * k + lax.rem(z, 2) for k in range(m // 2)], q,
        owner_two, q_send.at[1], q_recv.at[1], lambda peer: at_two(z, peer),
    )
    total = reduced(landed_b, m, rb_recv.at[1])
    hand_groups(
        total, group_b, [2 * k + lax.rem(q + 1, 2) for k in range(groups)], z,
        owner_two, q_send.at[1], q_recv.at[1], lambda peer: at_two(peer, q),
    )

    @pl.when(even_two)
    def _():
        drain(owner_two.at[pl.ds(0, m)], q_recv.at[1])
        drain(small.at[pl.ds(0, m - 1)], s_send)

    @pl.when(jnp.logical_not(even_two))
    def _():
        drain(owner_two, q_recv.at[1])
        drain(owner.at[pl.ds(0, n - 1)], s_send)

    mixed[...] = (mid + 0.5 * added(owner_two)).astype(BF16)

    drain(weights.at[2, t], pair_send)
    for s in range(3):
        drain(weights.at[s, pl.ds(0, n_tp - 1)], x_send.at[s])
    drain(gathered_a.at[pl.ds(0, n - 1)], g_send.at[0])
    drain(gathered_b.at[pl.ds(0, m - 1)], g_send.at[1])
    drain(part.at[pl.ds(0, 2 * n - 2)], r_send.at[0])
    drain(part_a.at[pl.ds(0, n - 1)], r_send.at[1])
    drain(part_b.at[pl.ds(0, m - 1)], r_send.at[2])
    drain(owner.at[pl.ds(0, n - 1)], q_send.at[0])
    drain(owner_two.at[pl.ds(0, m // 2 + groups - 1)], q_send.at[1])
    for b in range(2):
        drain(outgoing.at[b, pl.ds(0, fs - 1)], w_send.at[b])
        for w in range(3):
            shipped(b, w).wait()


def deliver(count, *refs):
    sources, targets, held = refs[:count], refs[count : 2 * count], refs[2 * count : 3 * count]
    in_sem, out_sem = refs[3 * count :]
    taken = [pltpu.make_async_copy(sources[k], held[k], in_sem.at[k]) for k in range(count)]
    given = [pltpu.make_async_copy(held[k], targets[k], out_sem.at[k]) for k in range(count)]
    for copy in taken:
        copy.start()
    for k in range(count):
        taken[k].wait()
        given[k].start()
    for copy in given:
        copy.wait()


def shards(
    tokens, gain_first, gate_first, up_first, down_first, gain_second, gate_second, up_second, down_second
):
    fs, n_tp = lax.axis_size("fs"), lax.axis_size("tp")
    n = int(round(fs**0.5))
    fd, local = gate_first.shape
    hu = local // fs
    d = fs * fd
    rows = tokens.shape[1]
    block = rows // 2 // n
    wide = -(-(local + ROWS) // 128) * 128
    vmem = pl.BlockSpec(memory_space=pltpu.VMEM)
    hbm = pl.BlockSpec(memory_space=pltpu.HBM)
    dma = pltpu.SemaphoreType.DMA
    m = n // 2
    shape_a = (n, OWN * m // 2, d)
    shape_b = (m, OWN * n // 2, d)
    results = pl.pallas_call(
        functools.partial(kernel, n, n_tp, hu, fd),
        out_shape=(
            jax.ShapeDtypeStruct((OWN, d), BF16),
        )
        + (jax.ShapeDtypeStruct((hu, n_tp, d), BF16),) * 6,
        in_specs=[hbm] * 9,
        out_specs=(vmem,) + (hbm,) * 6,
        scratch_shapes=[
            pltpu.VMEM((rows, d), BF16),
            pltpu.VMEM((2, 1, fd), F32),
            pltpu.VMEM((2, 3, fd, local), F32),
            pltpu.VMEM((4 * fd, wide), F32),
            pltpu.VMEM((wide, 4 * fd), F32),
            pltpu.VMEM((2, fs, ROWS, 128), BF16),
            pltpu.VMEM((2, 4, fs // 4, ROWS, 128), BF16),
            pltpu.VMEM((3, n_tp, 3, ROWS, d), BF16),
            pltpu.VMEM((rows, d), BF16),
            pltpu.VMEM((2 * n, block, d), BF16),
            pltpu.VMEM((2, n, block, d), BF16),
            pltpu.VMEM((2, m, OWN, d), BF16),
            pltpu.VMEM((n, OWN, d), BF16),
            pltpu.VMEM((m // 2 + m, OWN, d), BF16),
            pltpu.VMEM(shape_a, BF16),
            pltpu.VMEM(shape_b, BF16),
            pltpu.VMEM(shape_a, BF16),
            pltpu.VMEM(shape_b, BF16),
            pltpu.VMEM(shape_a, BF16),
            pltpu.VMEM(shape_b, BF16),
            pltpu.VMEM((m // 2, OWN, d), BF16),
            pltpu.VMEM((m, OWN, d), BF16),
            pltpu.VMEM((n, OWN, d), BF16),
            pltpu.VMEM((OWN, d), BF16),
            pltpu.VMEM((6, hu, n_tp, d), BF16),
            dma((2,)), dma((2,)), dma((3,)), dma((3, n_tp)), dma((3, 2)), dma(()), dma(()),
            dma((3,)), dma((2,)), dma((2,)), dma((2,)), dma((2,)), dma(()), dma(()),
            dma((2,)), dma(()), dma(()), dma((2, 5)), dma((2, 3)),
        ],
        compiler_params=pltpu.CompilerParams(
            collective_id=0, has_side_effects=True, vmem_limit_bytes=67043328
        ),
    )(
        tokens[0],
        gain_first[None], gate_first, up_first, down_first,
        gain_second[None], gate_second, up_second, down_second,
    )
    mixed, *served = pl.pallas_call(
        functools.partial(deliver, 7),
        out_shape=tuple(jax.ShapeDtypeStruct(r.shape, r.dtype) for r in results),
        in_specs=[hbm] * 7,
        out_specs=(hbm,) * 7,
        scratch_shapes=[pltpu.VMEM(r.shape, r.dtype) for r in results] + [dma((7,)), dma((7,))],
    )(*results)
    return (mixed[None],) + tuple(jnp.swapaxes(r, 0, 1) for r in served)


def solution(mesh):
    weight = P("fs", "tp")
    cut = P(None, "fs", None)
    return jax.shard_map(
        shards,
        mesh=mesh,
        in_specs=(P("tp", None, None), P("fs"), weight, weight, weight, P("fs"), weight, weight, weight),
        out_specs=(P("tp", "fs", None),) + (cut,) * 6,
        check_vma=False,
    )
```

```python
import functools

import jax
import jax.numpy as jnp
from jax import lax
from jax.experimental import pallas as pl
from jax.experimental.pallas import tpu as pltpu
from jax.sharding import PartitionSpec as P

MESH = pl.DeviceIdType.MESH
F32, BF16 = jnp.float32, jnp.bfloat16
ROWS = 16
OWN = 4


def far_first(count):
    return sorted(range(1, count), key=lambda k: (-min(k, count - k), k))


def rsqrt_norm(wide):
    scale = lax.rsqrt(jnp.mean(wide * wide, axis=-1, keepdims=True) + 1e-06)
    return (wide * scale).astype(BF16)


def kernel(
    n, n_tp, hu, fd,
    tokens_hbm, gain_one, gate_one, up_one, down_one, gain_two, gate_two, up_two, down_two,
    mixed, out_0, out_1, out_2, out_3, out_4, out_5,
    tokens, gains, trained, stack, turned, outgoing, incoming, weights_8, weights_4, ready, normed,
    part, landed, group, owner, small, gathered, part_two, landed_two, group_two, owner_two, middle,
    staged,
    w_send, w_recv, x_send, near_recv, half_recv, die_recv, quad_send, quad_recv, r_send, r_recv,
    q_send, q_recv, s_send, s_recv, g_send, g_recv, in_sem, out_sem,
):
    served = (out_0, out_1, out_2, out_3, out_4, out_5)
    fs = n * n
    d = fs * fd
    half = OWN * fs // 2
    block = half // n
    groups = n // 2
    m = n // 2
    f, t = lax.axis_index("fs"), lax.axis_index("tp")
    z, y = f // n, lax.rem(f, n)
    ez, ey, p, q = lax.rem(z, 2), lax.rem(y, 2), z // 2, y // 2
    x, c = t // 2, lax.rem(t, 2)
    nx = n_tp // 2
    even = lax.rem(p + q, 2) == 0
    partner = (f, x * 2 + 1 - c)

    def at(zz, yy):
        return (zz * n + yy, t)

    def at_two(pp, qq):
        return ((2 * pp + ez) * n + 2 * qq + ey, t)

    def along(step):
        return (f, lax.rem(x + nx + step, nx) * 2 + c)

    def slot_of(step, core):
        return lax.rem(x + nx + step, nx) * 2 + core

    def remote(src, dst, send, recv, device):
        return pltpu.make_async_remote_copy(
            src_ref=src, dst_ref=dst, send_sem=send, recv_sem=recv, device_id=device, device_id_type=MESH
        )

    def drain(ref, sem):
        pltpu.make_async_copy(ref, ref, sem).wait()

    given = ((gain_one, gate_one, up_one, down_one), (gain_two, gate_two, up_two, down_two))
    for b, (gain, *each) in enumerate(given):
        pltpu.make_async_copy(gain, gains.at[b], in_sem.at[3]).start()
        for w in range(3):
            pltpu.make_async_copy(each[w], trained.at[b, w], in_sem.at[b]).start()
    pltpu.make_async_copy(tokens_hbm, tokens, in_sem.at[2]).start()

    barrier = pltpu.get_barrier_semaphore()

    @pl.loop(1, fs)
    def _(k):
        pl.semaphore_signal(barrier, inc=1, device_id=(lax.rem(f + k, fs), t), device_id_type=MESH)

    around = {1: (), 2: (1,), 4: (1, -1)}[nx]
    for step in around:
        pl.semaphore_signal(barrier, inc=1, device_id=along(step), device_id_type=MESH)
    pl.semaphore_signal(barrier, inc=1, device_id=partner, device_id_type=MESH)

    hidden_units = gate_one.shape[1]
    stack[...] = jnp.zeros_like(stack)
    drain(gains, in_sem.at[3])
    for b in range(2):
        drain(trained.at[b], in_sem.at[b])
        for w in range(3):
            stack[w * fd : (w + 1) * fd, 0:hidden_units] = trained[b, w]
        ones = jnp.ones((1, fd), F32)
        scale = jnp.concatenate([gains[b], gains[b], ones, ones], axis=1)
        turned[...] = stack[...].T * scale
        live = lax.broadcasted_iota(jnp.int32, (ROWS, 128), 0) < hu
        for k in range(fs):
            rows = turned[k * hu : k * hu + ROWS, :]
            outgoing[b, k] = jnp.where(live, rows, 0.0).astype(BF16)

    pl.semaphore_wait(barrier, fs - 1 + len(around) + 1)

    offsets = [(dz, dy) for dz in range(n) for dy in range(n) if dz or dy]
    offsets.sort(key=lambda o: -(min(o[0], n - o[0]) + min(o[1], n - o[1])))
    for b in range(2):
        for dz, dy in offsets:
            peer = lax.rem(z + dz, n) * n + lax.rem(y + dy, n)
            remote(
                outgoing.at[b, peer],
                incoming.at[b, lax.rem(f, 4), f // 4],
                w_send.at[b],
                w_recv.at[b],
                (peer, t),
            ).start()

        pltpu.make_async_copy(
            outgoing.at[b, f], incoming.at[b, lax.rem(f, 4), f // 4], w_recv.at[b]
        ).start()

    drain(tokens, in_sem.at[2])
    wide = tokens[...].astype(F32)
    normed_rows = rsqrt_norm(wide)
    spot = lax.broadcasted_iota(jnp.int32, (2 * half, 2 * half), 0)
    source = lax.broadcasted_iota(jnp.int32, (2 * half, 2 * half), 1)
    in_first = spot < half
    inside = jnp.where(in_first, spot, spot - half)
    major = inside // block
    minor = (inside % block) // OWN
    row = inside % OWN
    first_home = major * n + 2 * minor + major % 2
    second_home = (2 * minor + (major + 1) % 2) * n + major
    home = jnp.where(in_first, first_home, second_home) * OWN + row
    shuffle = jnp.where(home == source, 1.0, 0.0).astype(BF16)
    normed[...] = jnp.dot(shuffle, normed_rows, preferred_element_type=F32).astype(BF16)
    pick_row = lax.broadcasted_iota(jnp.int32, (8, 2 * half), 0)
    pick_source = lax.broadcasted_iota(jnp.int32, (8, 2 * half), 1)
    pick = jnp.where((pick_row < OWN) & (pick_source == pick_row + f * OWN), 1.0, 0.0).astype(BF16)
    mine = jnp.dot(pick, tokens[...], preferred_element_type=F32)[0:OWN]

    lanes = 3 * 128
    lane_in = lax.broadcasted_iota(jnp.int32, (128, lanes), 0)
    lane_out = lax.broadcasted_iota(jnp.int32, (128, lanes), 1)
    inner = lane_out % 128

    def merge(b):
        drain(incoming.at[b], w_recv.at[b])
        total = jnp.zeros((fs // 4 * ROWS, lanes), F32)
        for i in range(4):
            chosen = (inner // 32 == i) & (lane_in == lane_out // 128 * 32 + inner % 32)
            spread_out = jnp.where(chosen, 1.0, 0.0).astype(BF16)
            piece = incoming[b, i].reshape(fs // 4 * ROWS, 128)
            total = total + jnp.dot(piece, spread_out, preferred_element_type=F32)
        for j in range(fs // 4):
            for w in range(3):
                there = slice(j * 128, (j + 1) * 128)
                cut = total[j * ROWS : (j + 1) * ROWS, w * 128 : (w + 1) * 128]
                weights_8[b, t, w, :, there] = cut[0:8].astype(BF16)
                weights_4[b, t, w, :, there] = cut[8:12].astype(BF16)

    def chunks(s):
        return ((0, 1), (1, 1), (2, 1)) if s == 0 else ((0, 3),)

    def send_piece(s, slot, chunk, send, recv, device, columns=pl.ds(0, d)):
        for held in (weights_8, weights_4):
            source = held.at[s, slot, pl.ds(*chunk), :, columns]
            remote(source, source, send, recv, device).start()

    def taken(sem, rows, columns=d):
        drain(weights_4.at[pl.ds(0, rows), 0, :, :, pl.ds(0, columns)], sem)

    def taken_sets(sem, count):
        drain(weights_4.at[pl.ds(0, 3), pl.ds(0, count)], sem)

    def index(s, i):
        return i if s == 0 else 2 + s

    def spread(s):
        for i, chunk in enumerate(chunks(s)):
            for h, step in enumerate(around):
                send_piece(s, t, chunk, x_send.at[s], near_recv.at[index(s, i), h], along(step))
            send_piece(s, t, chunk, x_send.at[s], die_recv.at[s], partner)

    def relay(s):
        for i, chunk in enumerate(chunks(s)):
            for h, step in enumerate(around):
                slot = slot_of(-step, c)
                taken(near_recv.at[index(s, i), h], chunk[1])
                if nx == 4:
                    send_piece(
                        s, slot, chunk, x_send.at[s], half_recv.at[index(s, i), h], along(step),
                        pl.ds(h * (d // 2), d // 2),
                    )
                send_piece(s, slot, chunk, x_send.at[s], die_recv.at[s], partner)

    def finish(s):
        if nx == 4:
            for i, chunk in enumerate(chunks(s)):
                for h in range(2):
                    taken(half_recv.at[index(s, i), h], chunk[1], d // 2)
                    send_piece(
                        s, slot_of(2, c), chunk, x_send.at[s], die_recv.at[s], partner,
                        pl.ds(h * (d // 2), d // 2),
                    )

    def collected(s):
        taken_sets(die_recv.at[s], nx)

    def units(s, w):
        tail = jnp.concatenate([weights_4[s, j, w].astype(F32) for j in range(n_tp)], axis=0)
        return jnp.concatenate([weights_8[s, :, w].reshape(n_tp * 8, d), tail.astype(BF16)], axis=0)

    def publish(b):
        width = hu * n_tp
        spot = lax.broadcasted_iota(jnp.int32, (width, n_tp * 12), 0)
        source = lax.broadcasted_iota(jnp.int32, (width, n_tp * 12), 1)
        owner_of, unit = spot % n_tp, spot // n_tp
        from_spot = jnp.where(unit < 8, owner_of * 8 + unit, n_tp * 8 + owner_of * 4 + unit - 8)
        swap = jnp.where(source == from_spot, 1.0, 0.0).astype(BF16)
        for w in range(3):
            rows = jnp.dot(swap, units(b, w), preferred_element_type=F32)
            for r in range(hu):
                staged[3 * b + w, r] = rows[r * n_tp : (r + 1) * n_tp].astype(BF16)
            pltpu.make_async_copy(staged.at[3 * b + w], served[3 * b + w], out_sem.at[b]).start()

    contract = (((1,), (1,)), ((), ()))

    def branch_of(rows, gate, up, down):
        gate_act = lax.dot_general(rows, gate, contract, preferred_element_type=F32)
        up_act = lax.dot_general(rows, up, contract, preferred_element_type=F32)
        act = (gate_act / (1.0 + jnp.exp(-gate_act)) * up_act).astype(BF16)
        return jnp.dot(act, down, preferred_element_type=F32).astype(BF16)

    def send_blocks(source, target, me, count, send, recv, device):
        for k in far_first(count):
            peer = lax.rem(me + k, count)
            remote(source.at[peer], target.at[me], send, recv, device(peer)).start()

        pltpu.make_async_copy(source.at[me], target.at[me], recv).start()

    def reduced(target, count, recv):
        drain(target, recv)
        total = target[0].astype(F32)
        for k in range(1, count):
            total = total + target[k].astype(F32)
        return total

    def hand_groups(total, held, targets, me, own, send, recv, device):
        for k, peer in enumerate(targets):
            held[k] = total[k * OWN : (k + 1) * OWN].astype(BF16)

            @pl.when(peer != me)
            def _():
                remote(held.at[k], own.at[me], send, recv, device(peer)).start()

            @pl.when(peer == me)
            def _():
                pltpu.make_async_copy(held.at[k], own.at[me], recv).start()

    def added(own, count):
        total = own[0].astype(F32)
        for k in range(1, count):
            total = total + own[k].astype(F32)
        return total

    merge(0)
    spread(0)
    relay(0)
    merge(1)
    quad = [((z + 1 - 2 * ez) * n + y, t), (z * n + y + 1 - 2 * ey, t)]
    quad.append(((z + 1 - 2 * ez) * n + y + 1 - 2 * ey, t))
    for k, device in enumerate(quad):
        for held in (weights_8, weights_4):
            remote(held.at[1, t], held.at[2 + k, t], quad_send.at[k], quad_recv.at[k], device).start()
    finish(0)
    collected(0)
    block_one = [units(0, w) for w in range(3)]
    for side in range(2):
        rows = normed[side * half : (side + 1) * half, :]
        part[side * n : (side + 1) * n] = branch_of(rows, *block_one).reshape(n, block, d)
        send_blocks(
            part.at[pl.ds(side * n, n)],
            landed.at[side],
            z if side == 0 else y,
            n,
            r_send.at[0],
            r_recv.at[side],
            (lambda peer: at(peer, y)) if side == 0 else (lambda peer: at(z, peer)),
        )
    spread(1)
    publish(0)
    for k in range(3):
        taken(quad_recv.at[k], 3)
        spread(2 + k)
    relay(1)
    relay(2)
    total = reduced(landed.at[0], n, r_recv.at[0])
    hand_groups(
        total, group.at[0], [2 * k + lax.rem(z, 2) for k in range(groups)], y,
        owner, q_send.at[0], q_recv.at[0], lambda peer: at(z, peer),
    )
    total = reduced(landed.at[1], n, r_recv.at[1])
    hand_groups(
        total, group.at[1], [2 * k + lax.rem(y + 1, 2) for k in range(groups)], z,
        owner, q_send.at[0], q_recv.at[0], lambda peer: at(peer, y),
    )
    finish(1)
    relay(3)
    drain(owner, q_recv.at[0])
    middle[...] = (mine + 0.5 * added(owner, n)).astype(BF16)
    mid = middle[...].astype(F32)
    own_slot = jnp.where(even, q // 2, m // 2 + p // 2)
    small[own_slot] = rsqrt_norm(mid)
    for k in far_first(m):
        near, far = at_two(p, lax.rem(q + k, m)), at_two(lax.rem(p + k, m), q)
        peer = jnp.where(even, near[0], far[0])
        remote(small.at[own_slot], small.at[own_slot], s_send, s_recv, (peer, t)).start()
    finish(2)
    relay(4)
    drain(small.at[pl.ds(0, m - 1)], s_recv)
    for side in range(2):
        rows = jnp.concatenate(
            [small[side * (m // 2) + k].astype(F32) for k in range(m // 2)], axis=0
        )
        me = p if side == 0 else q
        gathered[side, me] = rows.astype(BF16)
        for k in far_first(m):
            peer = lax.rem(me + k, m)
            remote(
                gathered.at[side, me], gathered.at[side, me], g_send.at[side], g_recv.at[side],
                at_two(peer, q) if side == 0 else at_two(p, peer),
            ).start()
    finish(3)
    finish(4)
    for s in range(1, 5):
        collected(s)
        for w in range(3):
            ready[w, (s - 1) * 12 * n_tp : s * 12 * n_tp, :] = units(s, w)
    quarter = OWN * m * m // 2
    for side in range(2):
        drain(gathered.at[side, pl.ds(0, m - 1)], g_recv.at[side])
    branch = branch_of(gathered[...].reshape(2 * quarter, d), ready[0], ready[1], ready[2])
    part_two[...] = branch.reshape(part_two.shape)
    for side in range(2):
        send_blocks(
            part_two.at[side], landed_two.at[side], p if side == 0 else q, m, r_send.at[1 + side],
            r_recv.at[2 + side],
            (lambda peer: at_two(peer, q)) if side == 0 else (lambda peer: at_two(p, peer)),
        )
    publish(1)
    total = reduced(landed_two.at[0], m, r_recv.at[2])
    hand_groups(
        total, group_two.at[0], [2 * k + lax.rem(p, 2) for k in range(m // 2)], q,
        owner_two, q_send.at[1], q_recv.at[1], lambda peer: at_two(p, peer),
    )
    total = reduced(landed_two.at[1], m, r_recv.at[3])
    hand_groups(
        total, group_two.at[1], [2 * k + lax.rem(q + 1, 2) for k in range(m // 2)], p,
        owner_two, q_send.at[1], q_recv.at[1], lambda peer: at_two(peer, q),
    )
    for k in range(3):
        taken(quad_send.at[k], 3)
    for s in range(5):
        taken_sets(x_send.at[s], 2 * nx - 1)
    drain(small.at[pl.ds(0, m - 1)], s_send)
    drain(part_two.at[0].at[pl.ds(0, m - 1)], g_send.at[0])
    drain(part_two.at[0].at[pl.ds(0, m - 1)], g_send.at[1])
    drain(part.at[pl.ds(0, 2 * n - 2)], r_send.at[0])
    drain(owner.at[pl.ds(0, n - 1)], q_send.at[0])
    for b in range(2):
        drain(outgoing.at[b, pl.ds(0, fs - 1)], w_send.at[b])
        drain(staged.at[pl.ds(3 * b, 3)], out_sem.at[b])
        drain(part_two.at[0].at[pl.ds(0, m - 1)], r_send.at[1 + b])
    drain(owner_two.at[pl.ds(0, m - 1)], q_send.at[1])
    drain(owner_two, q_recv.at[1])
    mixed[...] = (mid + 0.5 * added(owner_two, m)).astype(BF16)


def deliver(count, *refs):
    sources, targets, held = refs[:count], refs[count : 2 * count], refs[2 * count : 3 * count]
    in_sem, out_sem = refs[3 * count :]
    taken = [pltpu.make_async_copy(sources[k], held[k], in_sem.at[k]) for k in range(count)]
    given = [pltpu.make_async_copy(held[k], targets[k], out_sem.at[k]) for k in range(count)]
    for copy in taken:
        copy.start()
    for k in range(count):
        taken[k].wait()
        given[k].start()
    for copy in given:
        copy.wait()


def shards(
    tokens, gain_first, gate_first, up_first, down_first, gain_second, gate_second, up_second, down_second
):
    fs, n_tp = lax.axis_size("fs"), lax.axis_size("tp")
    n = int(round(fs**0.5))
    fd, local = gate_first.shape
    hu = local // fs
    d = fs * fd
    rows = tokens.shape[1]
    block = rows // 2 // n
    wide = -(-(local + ROWS) // 128) * 128
    vmem = pl.BlockSpec(memory_space=pltpu.VMEM)
    hbm = pl.BlockSpec(memory_space=pltpu.HBM)
    dma = pltpu.SemaphoreType.DMA
    m = n // 2
    two = (2, m, OWN * m // 2, d)
    results = pl.pallas_call(
        functools.partial(kernel, n, n_tp, hu, fd),
        out_shape=(
            jax.ShapeDtypeStruct((OWN, d), BF16),
        )
        + (jax.ShapeDtypeStruct((hu, n_tp, d), BF16),) * 6,
        in_specs=[hbm] * 9,
        out_specs=(vmem,) + (hbm,) * 6,
        scratch_shapes=[
            pltpu.VMEM((rows, d), BF16),
            pltpu.VMEM((2, 1, fd), F32),
            pltpu.VMEM((2, 3, fd, local), F32),
            pltpu.VMEM((4 * fd, wide), F32),
            pltpu.VMEM((wide, 4 * fd), F32),
            pltpu.VMEM((2, fs, ROWS, 128), BF16),
            pltpu.VMEM((2, 4, fs // 4, ROWS, 128), BF16),
            pltpu.VMEM((5, n_tp, 3, 8, d), BF16),
            pltpu.VMEM((5, n_tp, 3, 4, d), BF16),
            pltpu.VMEM((3, 4 * 12 * n_tp, d), BF16),
            pltpu.VMEM((rows, d), BF16),
            pltpu.VMEM((2 * n, block, d), BF16),
            pltpu.VMEM((2, n, block, d), BF16),
            pltpu.VMEM((2, m, OWN, d), BF16),
            pltpu.VMEM((n, OWN, d), BF16),
            pltpu.VMEM((m, OWN, d), BF16),
            pltpu.VMEM(two, BF16),
            pltpu.VMEM(two, BF16),
            pltpu.VMEM(two, BF16),
            pltpu.VMEM((2, m // 2, OWN, d), BF16),
            pltpu.VMEM((m, OWN, d), BF16),
            pltpu.VMEM((OWN, d), BF16),
            pltpu.VMEM((6, hu, n_tp, d), BF16),
            dma((2,)), dma((2,)), dma((5,)), dma((7, 2)), dma((7, 2)), dma((5,)), dma((3,)), dma((3,)),
            dma((3,)), dma((4,)), dma((2,)), dma((2,)), dma(()), dma(()), dma((2,)), dma((2,)),
            dma((4,)), dma((2,)),
        ],
        compiler_params=pltpu.CompilerParams(
            collective_id=0, has_side_effects=True, vmem_limit_bytes=67043328
        ),
    )(
        tokens[0],
        gain_first[None], gate_first, up_first, down_first,
        gain_second[None], gate_second, up_second, down_second,
    )
    mixed, *served = pl.pallas_call(
        functools.partial(deliver, 7),
        out_shape=tuple(jax.ShapeDtypeStruct(r.shape, r.dtype) for r in results),
        in_specs=[hbm] * 7,
        out_specs=(hbm,) * 7,
        scratch_shapes=[pltpu.VMEM(r.shape, r.dtype) for r in results] + [dma((7,)), dma((7,))],
    )(*results)
    return (mixed[None],) + tuple(jnp.swapaxes(r, 0, 1) for r in served)


def solution(mesh):
    weight = P("fs", "tp")
    cut = P(None, "fs", None)
    return jax.shard_map(
        shards,
        mesh=mesh,
        in_specs=(P("tp", None, None), P("fs"), weight, weight, weight, P("fs"), weight, weight, weight),
        out_specs=(P("tp", "fs", None),) + (cut,) * 6,
        check_vma=False,
    )
```

```python
import functools

import jax
import jax.numpy as jnp
from jax import lax
from jax.experimental import pallas as pl
from jax.experimental.pallas import tpu as pltpu
from jax.sharding import PartitionSpec as P

MESH = pl.DeviceIdType.MESH
F32, BF16 = jnp.float32, jnp.bfloat16
SENT = 12
OWN = 4


def far_first(count):
    return sorted(range(1, count), key=lambda k: (-min(k, count - k), k))


def rsqrt_norm(wide):
    scale = lax.rsqrt(jnp.mean(wide * wide, axis=-1, keepdims=True) + 1e-06)
    return (wide * scale).astype(BF16)


def kernel(
    n, n_tp, hu, fd,
    tokens_hbm, gain_one, gate_one, up_one, down_one, gain_two, gate_two, up_two, down_two,
    mixed, out_0, out_1, out_2, out_3, out_4, out_5,
    tokens, gains, trained, stack, turned, outgoing, incoming, placing, weights_8, weights_4, ready, normed,
    part, landed, group, line, gathered, part_two, landed_two, group_two, owner_two, middle, residual, staged,
    w_send, w_recv, x_send, near_recv, half_recv, die_recv, quad_send, quad_recv, r_send, r_recv,
    l_send, l_recv, two_send, two_recv, q_send, q_recv, g_send, g_recv, in_sem, out_sem,
):
    served = (out_0, out_1, out_2, out_3, out_4, out_5)
    fs = n * n
    d = fs * fd
    half = OWN * fs // 2
    block = half // n
    m = n // 2
    share = OWN * m // 2
    f, t = lax.axis_index("fs"), lax.axis_index("tp")
    z, y = f // n, lax.rem(f, n)
    ez, ey, p, q = lax.rem(z, 2), lax.rem(y, 2), z // 2, y // 2
    x, c = t // 2, lax.rem(t, 2)
    nx = n_tp // 2
    even = lax.rem(p + q, 2) == 0
    partner = (f, x * 2 + 1 - c)

    def at(zz, yy):
        return (zz * n + yy, t)

    def at_two(pp, qq):
        return ((2 * pp + ez) * n + 2 * qq + ey, t)

    def along(step):
        return (f, lax.rem(x + nx + step, nx) * 2 + c)

    def slot_of(step, core):
        return lax.rem(x + nx + step, nx) * 2 + core

    def remote(src, dst, send, recv, device):
        return pltpu.make_async_remote_copy(
            src_ref=src, dst_ref=dst, send_sem=send, recv_sem=recv, device_id=device, device_id_type=MESH
        )

    def drain(ref, sem):
        pltpu.make_async_copy(ref, ref, sem).wait()

    given = ((gain_one, gate_one, up_one, down_one), (gain_two, gate_two, up_two, down_two))
    for b, (gain, *each) in enumerate(given):
        pltpu.make_async_copy(gain, gains.at[b], in_sem.at[3]).start()
        for w in range(3):
            pltpu.make_async_copy(each[w], trained.at[b, w], in_sem.at[b]).start()
    pltpu.make_async_copy(tokens_hbm, tokens, in_sem.at[2]).start()

    barrier = pltpu.get_barrier_semaphore()

    @pl.loop(1, fs)
    def _(k):
        pl.semaphore_signal(barrier, inc=1, device_id=(lax.rem(f + k, fs), t), device_id_type=MESH)

    around = {1: (), 2: (1,), 4: (1, -1)}[nx]
    for step in around:
        pl.semaphore_signal(barrier, inc=1, device_id=along(step), device_id_type=MESH)
    pl.semaphore_signal(barrier, inc=1, device_id=partner, device_id_type=MESH)

    hidden_units = gate_one.shape[1]
    stack[...] = jnp.zeros_like(stack)
    drain(gains, in_sem.at[3])
    for b in range(2):
        drain(trained.at[b], in_sem.at[b])
        for w in range(3):
            stack[w * fd : (w + 1) * fd, 0:hidden_units] = trained[b, w]
        ones = jnp.ones((1, fd), F32)
        scale = jnp.concatenate([gains[b], gains[b], ones, ones], axis=1)
        turned[...] = stack[...].T * scale
        live = lax.broadcasted_iota(jnp.int32, (SENT, 128), 0) < hu
        for k in range(fs):
            rows = jnp.where(live, turned[k * hu : k * hu + SENT, :], 0.0)
            for g in range(SENT // 4):
                outgoing[b, k, g] = rows[4 * g : 4 * g + 4].astype(BF16)

    lanes = 3 * 128
    lane_in = lax.broadcasted_iota(jnp.int32, (128, lanes), 0)
    lane_out = lax.broadcasted_iota(jnp.int32, (128, lanes), 1)
    inner = lane_out % 128
    for i in range(4):
        chosen = (inner // 32 == i) & (lane_in == lane_out // 128 * 32 + inner % 32)
        placing[i] = jnp.where(chosen, 1.0, 0.0).astype(BF16)

    pl.semaphore_wait(barrier, fs - 1 + len(around) + 1)

    offsets = [(dz, dy) for dz in range(n) for dy in range(n) if dz or dy]
    offsets.sort(key=lambda o: (min(o[0], n - o[0]), -min(o[1], n - o[1])))
    for b in range(2):
        for dz, dy in offsets:
            peer = lax.rem(z + dz, n) * n + lax.rem(y + dy, n)
            remote(
                outgoing.at[b, peer],
                incoming.at[b, lax.rem(f, 4), f // 4],
                w_send.at[b],
                w_recv.at[z if b == 0 else n],
                (peer, t),
            ).start()

        pltpu.make_async_copy(
            outgoing.at[b, f], incoming.at[b, lax.rem(f, 4), f // 4], w_recv.at[z if b == 0 else n]
        ).start()

    drain(tokens, in_sem.at[2])
    wide = tokens[...].astype(F32)
    normed_rows = rsqrt_norm(wide)
    spot = lax.broadcasted_iota(jnp.int32, (2 * half, 2 * half), 0)
    source = lax.broadcasted_iota(jnp.int32, (2 * half, 2 * half), 1)
    in_first = spot < half
    inside = jnp.where(in_first, spot, spot - half)
    major = inside // block
    side_e = inside % block // share
    minor = inside % share // OWN
    row = inside % OWN
    first_home = major * n + 2 * (2 * minor + major // 2 % 2) + side_e
    second_home = (2 * (2 * minor + (major // 2 + 1) % 2) + side_e) * n + major
    home = jnp.where(in_first, first_home, second_home) * OWN + row
    shuffle = jnp.where(home == source, 1.0, 0.0).astype(BF16)
    normed[...] = jnp.dot(shuffle, normed_rows, preferred_element_type=F32).astype(BF16)
    pick_row = lax.broadcasted_iota(jnp.int32, (2 * share, 2 * half), 0)
    pick_source = lax.broadcasted_iota(jnp.int32, (2 * share, 2 * half), 1)
    inside = pick_row % share
    row_home = jnp.where(
        pick_row < share,
        z * n + 2 * (2 * (inside // OWN) + lax.rem(p, 2)) + ey,
        (2 * (2 * (inside // OWN) + lax.rem(q + 1, 2)) + ez) * n + y,
    )
    pick = jnp.where(pick_source == row_home * OWN + inside % OWN, 1.0, 0.0).astype(BF16)
    residual[...] = jnp.dot(pick, tokens[...], preferred_element_type=F32)

    per = n // 4
    strip = n * fd

    def merge(b, first, count, start):
        total = jnp.zeros((count * SENT, lanes), F32)
        for i in range(4):
            rows = jnp.concatenate(
                [incoming[b, i, first + j, g].astype(F32) for j in range(count) for g in range(SENT // 4)],
                axis=0,
            )
            total = total + jnp.dot(rows.astype(BF16), placing[i], preferred_element_type=F32)
        for j in range(count):
            for w in range(3):
                there = pl.ds(start + j * 128, 128)
                cut = total[j * SENT : (j + 1) * SENT, w * 128 : (w + 1) * 128]
                weights_8[b, t, w, :, there] = cut[0:8].astype(BF16)
                weights_4[b, t, w, :, there] = cut[8:12].astype(BF16)

    def send_piece(s, slot, send, recv, device, columns=pl.ds(0, d)):
        for held in (weights_8, weights_4):
            source = held.at[s, slot, :, :, columns]
            remote(source, source, send, recv, device).start()

    def taken(sem, columns=d):
        drain(weights_4.at[pl.ds(0, 3), 0, :, :, pl.ds(0, columns)], sem)

    def taken_sets(sem, count):
        drain(weights_4.at[pl.ds(0, 3), pl.ds(0, count)], sem)

    near_first = [0] + far_first(n)[::-1]

    def columns_of(u):
        return pl.multiple_of(lax.rem(z + near_first[u], n) * strip, strip)

    def stream(u):
        home = lax.rem(z + near_first[u], n)
        drain(incoming.at[0, 0, pl.ds(0, n)], w_recv.at[home])
        merge(0, home * per, per, columns_of(u))
        columns = pl.ds(columns_of(u), strip)
        for h, step in enumerate(around):
            send_piece(0, t, x_send.at[0], near_recv.at[u, h], along(step), columns)
        send_piece(0, t, x_send.at[0], die_recv.at[0], partner, columns)

    def stream_relay(u):
        columns = pl.ds(columns_of(u), strip)
        for h, step in enumerate(around):
            slot = slot_of(-step, c)
            taken(near_recv.at[u, h], strip)
            if nx == 4 and h == u % 2:
                send_piece(0, slot, x_send.at[0], half_recv.at[u], along(step), columns)
            send_piece(0, slot, x_send.at[0], die_recv.at[0], partner, columns)

    def stream_finish(u):
        if nx == 4:
            taken(half_recv.at[u], strip)
            send_piece(
                0, slot_of(2, c), x_send.at[0], die_recv.at[0], partner, pl.ds(columns_of(u), strip)
            )

    def spread(s):
        for h, step in enumerate(around):
            send_piece(s, t, x_send.at[s], near_recv.at[n + s - 1, h], along(step))
        send_piece(s, t, x_send.at[s], die_recv.at[s], partner)

    def relay(s):
        for h, step in enumerate(around):
            slot = slot_of(-step, c)
            taken(near_recv.at[n + s - 1, h])
            if nx == 4:
                send_piece(
                    s, slot, x_send.at[s], half_recv.at[n + 2 * (s - 1) + h], along(step),
                    pl.ds(h * (d // 2), d // 2),
                )
            send_piece(s, slot, x_send.at[s], die_recv.at[s], partner)

    def finish(s):
        if nx == 4:
            for h in range(2):
                taken(half_recv.at[n + 2 * (s - 1) + h], d // 2)
                send_piece(
                    s, slot_of(2, c), x_send.at[s], die_recv.at[s], partner, pl.ds(h * (d // 2), d // 2)
                )

    def collected(s):
        taken_sets(die_recv.at[s], nx)

    def units(s, w):
        tail = jnp.concatenate([weights_4[s, j, w].astype(F32) for j in range(n_tp)], axis=0)
        return jnp.concatenate([weights_8[s, :, w].reshape(n_tp * 8, d), tail.astype(BF16)], axis=0)

    def publish(b):
        width = hu * n_tp
        spot = lax.broadcasted_iota(jnp.int32, (width, n_tp * 12), 0)
        source = lax.broadcasted_iota(jnp.int32, (width, n_tp * 12), 1)
        owner_of, unit = spot % n_tp, spot // n_tp
        from_spot = jnp.where(unit < 8, owner_of * 8 + unit, n_tp * 8 + owner_of * 4 + unit - 8)
        swap = jnp.where(source == from_spot, 1.0, 0.0).astype(BF16)
        for w in range(3):
            rows = jnp.dot(swap, units(b, w), preferred_element_type=F32)
            for r in range(hu):
                staged[3 * b + w, r] = rows[r * n_tp : (r + 1) * n_tp].astype(BF16)
            pltpu.make_async_copy(staged.at[3 * b + w], served[3 * b + w], out_sem.at[b]).start()

    contract = (((1,), (1,)), ((), ()))

    def hidden_of(rows, gate, up):
        gate_act = lax.dot_general(rows, gate, contract, preferred_element_type=F32)
        up_act = lax.dot_general(rows, up, contract, preferred_element_type=F32)
        return (gate_act / (1.0 + jnp.exp(-gate_act)) * up_act).astype(BF16)

    def branch_of(hidden, down):
        return jnp.dot(hidden, down, preferred_element_type=F32).astype(BF16)

    def send_blocks(source, target, me, count, send, recv, device):
        for k in far_first(count):
            peer = lax.rem(me + k, count)
            remote(source.at[peer], target.at[me], send, recv, device(peer)).start()

        pltpu.make_async_copy(source.at[me], target.at[me], recv).start()

    def reduced(target, count, recv):
        drain(target, recv)
        total = target[0].astype(F32)
        for k in range(1, count):
            total = total + target[k].astype(F32)
        return total

    def hand_groups(total, held, targets, me, own, send, recv, device):
        for k, peer in enumerate(targets):
            held[k] = total[k * OWN : (k + 1) * OWN].astype(BF16)

            @pl.when(peer != me)
            def _():
                remote(held.at[k], own.at[me], send, recv, device(peer)).start()

            @pl.when(peer == me)
            def _():
                pltpu.make_async_copy(held.at[k], own.at[me], recv).start()

    def added(own, count):
        total = own[0].astype(F32)
        for k in range(1, count):
            total = total + own[k].astype(F32)
        return total

    for u in range(n + 6):
        if u < n:
            stream(u)
        if 3 <= u < n + 3:
            stream_relay(u - 3)
        if 6 <= u:
            if u == n + 4:
                break
            stream_finish(u - 6)
    drain(incoming.at[1], w_recv.at[n])
    merge(1, 0, fs // 4, 0)
    quad = [((z + 1 - 2 * ez) * n + y, t), (z * n + y + 1 - 2 * ey, t)]
    quad.append(((z + 1 - 2 * ez) * n + y + 1 - 2 * ey, t))
    for k, device in enumerate(quad):
        for held in (weights_8, weights_4):
            remote(held.at[1, t], held.at[2 + k, t], quad_send.at[k], quad_recv.at[k], device).start()
    spread(1)
    stream_finish(n - 2)
    stream_finish(n - 1)
    collected(0)
    hidden = hidden_of(normed[...], units(0, 0), units(0, 1))
    down_one = units(0, 2)
    wide = d // 2
    for cut in range(2):
        columns = slice(cut * wide, (cut + 1) * wide)
        for side in range(2):
            branch = branch_of(hidden[side * half : (side + 1) * half], down_one[:, columns])
            part[side, :, :, columns] = branch.reshape(n, block, wide)
            me = z if side == 0 else y
            for k in far_first(n):
                peer = lax.rem(me + k, n)
                remote(
                    part.at[side, peer, :, columns], landed.at[side, me, :, columns],
                    r_send.at[side], r_recv.at[side, cut], at(peer, y) if side == 0 else at(z, peer),
                ).start()
            pltpu.make_async_copy(
                part.at[side, me, :, columns], landed.at[side, me, :, columns], r_recv.at[side, cut]
            ).start()

    def sum_cut(cut):
        columns = slice(cut * wide, (cut + 1) * wide)
        for side in range(2):
            drain(landed.at[side, :, :, columns], r_recv.at[side, cut])
            total = landed[side, 0, :, columns].astype(F32)
            for k in range(1, n):
                total = total + landed[side, k, :, columns].astype(F32)
            for k in range(2):
                group[side, k, :, columns] = total[k * share : (k + 1) * share].astype(BF16)
            me = y if side == 0 else z
            for k in far_first(n):
                peer = lax.rem(me + k, n)
                remote(
                    group.at[side, lax.rem(peer, 2), :, columns], line.at[side, me, :, columns],
                    l_send.at[side], l_recv.at[side], at(z, peer) if side == 0 else at(peer, y),
                ).start()
            pltpu.make_async_copy(
                group.at[side, lax.rem(me, 2), :, columns], line.at[side, me, :, columns], l_recv.at[side]
            ).start()

    def prepare(s):
        collected(s)
        for w in range(3):
            ready[w, (s - 1) * SENT * n_tp : s * SENT * n_tp, :] = units(s, w)

    taken(quad_recv.at[0])
    spread(2)
    relay(1)
    for k in range(1, 3):
        taken(quad_recv.at[k])
        spread(2 + k)
    publish(0)
    sum_cut(0)
    relay(2)
    sum_cut(1)
    finish(1)
    relay(3)
    prepare(1)
    own_slot = jnp.where(even, q // 2, m // 2 + p // 2)
    for side in range(2):
        drain(line.at[side], l_recv.at[side])
        total = line[side, 0].astype(F32)
        for k in range(1, n):
            total = total + line[side, k].astype(F32)
        total = residual[side * share : (side + 1) * share] + 0.5 * total
        for k in range(m // 2):
            middle[side * (m // 2) + k] = total[k * OWN : (k + 1) * OWN].astype(BF16)
        me = p if side == 0 else q
        gathered[side, me] = rsqrt_norm(total.astype(BF16).astype(F32))
        for k in far_first(m):
            peer = lax.rem(me + k, m)
            remote(
                gathered.at[side, me], gathered.at[side, me], g_send.at[side], g_recv.at[side],
                at_two(peer, q) if side == 0 else at_two(p, peer),
            ).start()
    finish(2)
    relay(4)
    prepare(2)
    finish(3)
    prepare(3)
    finish(4)
    prepare(4)
    quarter = OWN * m * m // 2
    for side in range(2):
        drain(gathered.at[side, pl.ds(0, m - 1)], g_recv.at[side])
    hidden = hidden_of(gathered[...].reshape(2 * quarter, d), ready[0], ready[1])
    branch = branch_of(hidden, ready[2])
    part_two[...] = branch.reshape(part_two.shape)
    for side in range(2):
        send_blocks(
            part_two.at[side], landed_two.at[side], p if side == 0 else q, m, two_send.at[side],
            two_recv.at[side],
            (lambda peer: at_two(peer, q)) if side == 0 else (lambda peer: at_two(p, peer)),
        )
    publish(1)
    total = reduced(landed_two.at[0], m, two_recv.at[0])
    hand_groups(
        total, group_two.at[0], [2 * k + lax.rem(p, 2) for k in range(m // 2)], q,
        owner_two, q_send, q_recv, lambda peer: at_two(p, peer),
    )
    total = reduced(landed_two.at[1], m, two_recv.at[1])
    hand_groups(
        total, group_two.at[1], [2 * k + lax.rem(q + 1, 2) for k in range(m // 2)], p,
        owner_two, q_send, q_recv, lambda peer: at_two(peer, q),
    )
    for k in range(3):
        taken(quad_send.at[k])
    for s in range(5):
        taken_sets(x_send.at[s], 2 * nx - 1)
    for b in range(2):
        drain(outgoing.at[b, pl.ds(0, fs - 1)], w_send.at[b])
        drain(staged.at[pl.ds(3 * b, 3)], out_sem.at[b])
        drain(part.at[b, pl.ds(0, n - 1)], r_send.at[b])
        drain(line.at[b, pl.ds(0, n - 1)], l_send.at[b])
        drain(gathered.at[b, pl.ds(0, m - 1)], g_send.at[b])
        drain(gathered.at[b, pl.ds(0, m - 1)], two_send.at[b])
    drain(owner_two.at[pl.ds(0, m - 1)], q_send)
    drain(owner_two, q_recv)
    mixed[...] = (middle[own_slot].astype(F32) + 0.5 * added(owner_two, m)).astype(BF16)


def deliver(count, *refs):
    sources, targets, held = refs[:count], refs[count : 2 * count], refs[2 * count : 3 * count]
    in_sem, out_sem = refs[3 * count :]
    taken = [pltpu.make_async_copy(sources[k], held[k], in_sem.at[k]) for k in range(count)]
    given = [pltpu.make_async_copy(held[k], targets[k], out_sem.at[k]) for k in range(count)]
    for copy in taken:
        copy.start()
    for k in range(count):
        taken[k].wait()
        given[k].start()
    for copy in given:
        copy.wait()


def shards(
    tokens, gain_first, gate_first, up_first, down_first, gain_second, gate_second, up_second, down_second
):
    fs, n_tp = lax.axis_size("fs"), lax.axis_size("tp")
    n = int(round(fs**0.5))
    fd, local = gate_first.shape
    hu = local // fs
    d = fs * fd
    rows = tokens.shape[1]
    block = rows // 2 // n
    wide = -(-(local + 16) // 128) * 128
    vmem = pl.BlockSpec(memory_space=pltpu.VMEM)
    hbm = pl.BlockSpec(memory_space=pltpu.HBM)
    dma = pltpu.SemaphoreType.DMA
    m = n // 2
    two = (2, m, OWN * m // 2, d)
    results = pl.pallas_call(
        functools.partial(kernel, n, n_tp, hu, fd),
        out_shape=(
            jax.ShapeDtypeStruct((OWN, d), BF16),
        )
        + (jax.ShapeDtypeStruct((hu, n_tp, d), BF16),) * 6,
        in_specs=[hbm] * 9,
        out_specs=(vmem,) + (hbm,) * 6,
        scratch_shapes=[
            pltpu.VMEM((rows, d), BF16),
            pltpu.VMEM((2, 1, fd), F32),
            pltpu.VMEM((2, 3, fd, local), F32),
            pltpu.VMEM((4 * fd, wide), F32),
            pltpu.VMEM((wide, 4 * fd), F32),
            pltpu.VMEM((2, fs, SENT // 4, 4, 128), BF16),
            pltpu.VMEM((2, 4, fs // 4, SENT // 4, 4, 128), BF16),
            pltpu.VMEM((4, 128, 3 * 128), BF16),
            pltpu.VMEM((5, n_tp, 3, 8, d), BF16),
            pltpu.VMEM((5, n_tp, 3, 4, d), BF16),
            pltpu.VMEM((3, 4 * 12 * n_tp, d), BF16),
            pltpu.VMEM((rows, d), BF16),
            pltpu.VMEM((2, n, block, d), BF16),
            pltpu.VMEM((2, n, block, d), BF16),
            pltpu.VMEM((2, 2, OWN * m // 2, d), BF16),
            pltpu.VMEM((2, n, OWN * m // 2, d), BF16),
            pltpu.VMEM(two, BF16),
            pltpu.VMEM(two, BF16),
            pltpu.VMEM(two, BF16),
            pltpu.VMEM((2, m // 2, OWN, d), BF16),
            pltpu.VMEM((m, OWN, d), BF16),
            pltpu.VMEM((m, OWN, d), BF16),
            pltpu.VMEM((OWN * m, d), F32),
            pltpu.VMEM((6, hu, n_tp, d), BF16),
            dma((2,)), dma((n + 1,)), dma((5,)), dma((n + 4, 2)), dma((n + 8,)), dma((5,)), dma((3,)), dma((3,)),
            dma((2,)), dma((2, 2)), dma((2,)), dma((2,)), dma((2,)), dma((2,)), dma(()), dma(()),
            dma((2,)), dma((2,)), dma((4,)), dma((2,)),
        ],
        compiler_params=pltpu.CompilerParams(
            collective_id=0, has_side_effects=True, vmem_limit_bytes=67043328
        ),
    )(
        tokens[0],
        gain_first[None], gate_first, up_first, down_first,
        gain_second[None], gate_second, up_second, down_second,
    )
    mixed, *served = pl.pallas_call(
        functools.partial(deliver, 7),
        out_shape=tuple(jax.ShapeDtypeStruct(r.shape, r.dtype) for r in results),
        in_specs=[hbm] * 7,
        out_specs=(hbm,) * 7,
        scratch_shapes=[pltpu.VMEM(r.shape, r.dtype) for r in results] + [dma((7,)), dma((7,))],
    )(*results)
    return (mixed[None],) + tuple(jnp.swapaxes(r, 0, 1) for r in served)


def solution(mesh):
    weight = P("fs", "tp")
    cut = P(None, "fs", None)
    return jax.shard_map(
        shards,
        mesh=mesh,
        in_specs=(P("tp", None, None), P("fs"), weight, weight, weight, P("fs"), weight, weight, weight),
        out_specs=(P("tp", "fs", None),) + (cut,) * 6,
        check_vma=False,
    )
```

```python
import functools

import jax
import jax.numpy as jnp
from jax import lax
from jax.experimental import pallas as pl
from jax.experimental.pallas import tpu as pltpu
from jax.sharding import PartitionSpec as P

MESH = pl.DeviceIdType.MESH
F32, BF16 = jnp.float32, jnp.bfloat16
SENT = 12
OWN = 4


def far_first(count):
    return sorted(range(1, count), key=lambda k: (-min(k, count - k), k))


def rsqrt_norm(wide):
    scale = lax.rsqrt(jnp.mean(wide * wide, axis=-1, keepdims=True) + 1e-06)
    return (wide * scale).astype(BF16)


def kernel(
    n, n_tp, hu, fd,
    tokens_hbm, gain_one, gate_one, up_one, down_one, gain_two, gate_two, up_two, down_two,
    mixed, out_0, out_1, out_2, out_3, out_4, out_5,
    tokens, gains, trained, stack, turned, outgoing, incoming, placing, weights_8, weights_4, ready, normed,
    part, landed, group, line, gathered, part_two, landed_two, group_two, owner_two, middle, residual,
    w_send, w_recv, x_send, near_recv, half_recv, die_recv, quad_send, quad_recv, r_send, r_recv,
    l_send, l_recv, two_send, two_recv, q_send, q_recv, g_send, g_recv, in_sem,
):
    staged = (out_0, out_1, out_2, out_3, out_4, out_5)
    fs = n * n
    d = fs * fd
    half = OWN * fs // 2
    block = half // n
    m = n // 2
    share = OWN * m // 2
    f, t = lax.axis_index("fs"), lax.axis_index("tp")
    z, y = f // n, lax.rem(f, n)
    ez, ey, p, q = lax.rem(z, 2), lax.rem(y, 2), z // 2, y // 2
    x, c = t // 2, lax.rem(t, 2)
    nx = n_tp // 2
    even = lax.rem(p + q, 2) == 0
    partner = (f, x * 2 + 1 - c)

    def at(zz, yy):
        return (zz * n + yy, t)

    def at_two(pp, qq):
        return ((2 * pp + ez) * n + 2 * qq + ey, t)

    def along(step):
        return (f, lax.rem(x + nx + step, nx) * 2 + c)

    def slot_of(step, core):
        return lax.rem(x + nx + step, nx) * 2 + core

    def remote(src, dst, send, recv, device):
        return pltpu.make_async_remote_copy(
            src_ref=src, dst_ref=dst, send_sem=send, recv_sem=recv, device_id=device, device_id_type=MESH
        )

    def drain(ref, sem):
        pltpu.make_async_copy(ref, ref, sem).wait()

    given = ((gain_one, gate_one, up_one, down_one), (gain_two, gate_two, up_two, down_two))
    for b, (gain, *each) in enumerate(given):
        pltpu.make_async_copy(gain, gains.at[b], in_sem.at[3]).start()
        for w in range(3):
            pltpu.make_async_copy(each[w], trained.at[b, w], in_sem.at[b]).start()
    pltpu.make_async_copy(tokens_hbm, tokens, in_sem.at[2]).start()

    barrier = pltpu.get_barrier_semaphore()

    @pl.loop(1, fs)
    def _(k):
        pl.semaphore_signal(barrier, inc=1, device_id=(lax.rem(f + k, fs), t), device_id_type=MESH)

    around = {1: (), 2: (1,), 4: (1, -1)}[nx]
    for step in around:
        pl.semaphore_signal(barrier, inc=1, device_id=along(step), device_id_type=MESH)
    pl.semaphore_signal(barrier, inc=1, device_id=partner, device_id_type=MESH)

    hidden_units = gate_one.shape[1]
    stack[...] = jnp.zeros_like(stack)
    drain(gains, in_sem.at[3])
    for b in range(2):
        drain(trained.at[b], in_sem.at[b])
        for w in range(3):
            stack[w * fd : (w + 1) * fd, 0:hidden_units] = trained[b, w]
        ones = jnp.ones((1, fd), F32)
        scale = jnp.concatenate([gains[b], gains[b], ones, ones], axis=1)
        turned[...] = stack[...].T * scale
        live = lax.broadcasted_iota(jnp.int32, (SENT, 128), 0) < hu
        for k in range(fs):
            rows = jnp.where(live, turned[k * hu : k * hu + SENT, :], 0.0)
            for g in range(SENT // 4):
                outgoing[b, k, g] = rows[4 * g : 4 * g + 4].astype(BF16)

    lanes = 3 * 128
    lane_in = lax.broadcasted_iota(jnp.int32, (128, lanes), 0)
    lane_out = lax.broadcasted_iota(jnp.int32, (128, lanes), 1)
    inner = lane_out % 128
    for i in range(4):
        chosen = (inner // 32 == i) & (lane_in == lane_out // 128 * 32 + inner % 32)
        placing[i] = jnp.where(chosen, 1.0, 0.0).astype(BF16)

    pl.semaphore_wait(barrier, fs - 1 + len(around) + 1)

    offsets = [(dz, dy) for dz in range(n) for dy in range(n) if dz or dy]
    offsets.sort(key=lambda o: (min(o[0], n - o[0]), -min(o[1], n - o[1])))
    for b in range(2):
        for dz, dy in offsets:
            peer = lax.rem(z + dz, n) * n + lax.rem(y + dy, n)
            remote(
                outgoing.at[b, peer],
                incoming.at[b, lax.rem(f, 4), f // 4],
                w_send.at[b],
                w_recv.at[z if b == 0 else n],
                (peer, t),
            ).start()

        pltpu.make_async_copy(
            outgoing.at[b, f], incoming.at[b, lax.rem(f, 4), f // 4], w_recv.at[z if b == 0 else n]
        ).start()

    drain(tokens, in_sem.at[2])
    wide = tokens[...].astype(F32)
    normed_rows = rsqrt_norm(wide)
    spot = lax.broadcasted_iota(jnp.int32, (2 * half, 2 * half), 0)
    source = lax.broadcasted_iota(jnp.int32, (2 * half, 2 * half), 1)
    in_first = spot < half
    inside = jnp.where(in_first, spot, spot - half)
    major = inside // block
    side_e = inside % block // share
    minor = inside % share // OWN
    row = inside % OWN
    first_home = major * n + 2 * (2 * minor + major // 2 % 2) + side_e
    second_home = (2 * (2 * minor + (major // 2 + 1) % 2) + side_e) * n + major
    home = jnp.where(in_first, first_home, second_home) * OWN + row
    shuffle = jnp.where(home == source, 1.0, 0.0).astype(BF16)
    normed[...] = jnp.dot(shuffle, normed_rows, preferred_element_type=F32).astype(BF16)
    pick_row = lax.broadcasted_iota(jnp.int32, (2 * share, 2 * half), 0)
    pick_source = lax.broadcasted_iota(jnp.int32, (2 * share, 2 * half), 1)
    inside = pick_row % share
    row_home = jnp.where(
        pick_row < share,
        z * n + 2 * (2 * (inside // OWN) + lax.rem(p, 2)) + ey,
        (2 * (2 * (inside // OWN) + lax.rem(q + 1, 2)) + ez) * n + y,
    )
    pick = jnp.where(pick_source == row_home * OWN + inside % OWN, 1.0, 0.0).astype(BF16)
    residual[...] = jnp.dot(pick, tokens[...], preferred_element_type=F32)

    per = n // 4
    strip = n * fd

    def merge(b, first, count, start):
        total = jnp.zeros((count * SENT, lanes), F32)
        for i in range(4):
            rows = jnp.concatenate(
                [incoming[b, i, first + j, g].astype(F32) for j in range(count) for g in range(SENT // 4)],
                axis=0,
            )
            total = total + jnp.dot(rows.astype(BF16), placing[i], preferred_element_type=F32)
        for j in range(count):
            for w in range(3):
                there = pl.ds(start + j * 128, 128)
                cut = total[j * SENT : (j + 1) * SENT, w * 128 : (w + 1) * 128]
                weights_8[b, t, w, :, there] = cut[0:8].astype(BF16)
                weights_4[b, t, w, :, there] = cut[8:12].astype(BF16)

    def send_piece(s, slot, send, recv, device, columns=pl.ds(0, d)):
        for held in (weights_8, weights_4):
            source = held.at[s, slot, :, :, columns]
            remote(source, source, send, recv, device).start()

    def taken(sem, columns=d):
        drain(weights_4.at[pl.ds(0, 3), 0, :, :, pl.ds(0, columns)], sem)

    def taken_sets(sem, count):
        drain(weights_4.at[pl.ds(0, 3), pl.ds(0, count)], sem)

    near_first = [0] + far_first(n)[::-1]

    def columns_of(u):
        return pl.multiple_of(lax.rem(z + near_first[u], n) * strip, strip)

    def stream(u):
        home = lax.rem(z + near_first[u], n)
        drain(incoming.at[0, 0, pl.ds(0, n)], w_recv.at[home])
        merge(0, home * per, per, columns_of(u))
        columns = pl.ds(columns_of(u), strip)
        for h, step in enumerate(around):
            send_piece(0, t, x_send.at[0], near_recv.at[u, h], along(step), columns)
        send_piece(0, t, x_send.at[0], die_recv.at[0], partner, columns)

    def stream_relay(u):
        columns = pl.ds(columns_of(u), strip)
        for h, step in enumerate(around):
            slot = slot_of(-step, c)
            taken(near_recv.at[u, h], strip)
            if nx == 4 and h == u % 2:
                send_piece(0, slot, x_send.at[0], half_recv.at[u], along(step), columns)
            send_piece(0, slot, x_send.at[0], die_recv.at[0], partner, columns)

    def stream_finish(u):
        if nx == 4:
            taken(half_recv.at[u], strip)
            send_piece(
                0, slot_of(2, c), x_send.at[0], die_recv.at[0], partner, pl.ds(columns_of(u), strip)
            )

    def spread(s):
        for h, step in enumerate(around):
            send_piece(s, t, x_send.at[s], near_recv.at[n + s - 1, h], along(step))
        send_piece(s, t, x_send.at[s], die_recv.at[s], partner)

    def relay(s):
        for h, step in enumerate(around):
            slot = slot_of(-step, c)
            taken(near_recv.at[n + s - 1, h])
            if nx == 4:
                send_piece(
                    s, slot, x_send.at[s], half_recv.at[n + 2 * (s - 1) + h], along(step),
                    pl.ds(h * (d // 2), d // 2),
                )
            send_piece(s, slot, x_send.at[s], die_recv.at[s], partner)

    def finish(s):
        if nx == 4:
            for h in range(2):
                taken(half_recv.at[n + 2 * (s - 1) + h], d // 2)
                send_piece(
                    s, slot_of(2, c), x_send.at[s], die_recv.at[s], partner, pl.ds(h * (d // 2), d // 2)
                )

    def collected(s):
        taken_sets(die_recv.at[s], nx)

    def units(s, w):
        tail = jnp.concatenate([weights_4[s, j, w].astype(F32) for j in range(n_tp)], axis=0)
        return jnp.concatenate([weights_8[s, :, w].reshape(n_tp * 8, d), tail.astype(BF16)], axis=0)

    def publish(b):
        width = hu * n_tp
        spot = lax.broadcasted_iota(jnp.int32, (width, n_tp * 12), 0)
        source = lax.broadcasted_iota(jnp.int32, (width, n_tp * 12), 1)
        owner_of, unit = spot % n_tp, spot // n_tp
        from_spot = jnp.where(unit < 8, owner_of * 8 + unit, n_tp * 8 + owner_of * 4 + unit - 8)
        swap = jnp.where(source == from_spot, 1.0, 0.0).astype(BF16)
        for w in range(3):
            rows = jnp.dot(swap, units(b, w), preferred_element_type=F32)
            for r in range(hu):
                staged[3 * b + w][r] = rows[r * n_tp : (r + 1) * n_tp].astype(BF16)

    contract = (((1,), (1,)), ((), ()))

    def hidden_of(rows, gate, up):
        gate_act = lax.dot_general(rows, gate, contract, preferred_element_type=F32)
        up_act = lax.dot_general(rows, up, contract, preferred_element_type=F32)
        return (gate_act / (1.0 + jnp.exp(-gate_act)) * up_act).astype(BF16)

    def branch_of(hidden, down):
        return jnp.dot(hidden, down, preferred_element_type=F32).astype(BF16)

    def send_blocks(source, target, me, count, send, recv, device):
        for k in far_first(count):
            peer = lax.rem(me + k, count)
            remote(source.at[peer], target.at[me], send, recv, device(peer)).start()

        pltpu.make_async_copy(source.at[me], target.at[me], recv).start()

    def reduced(target, count, recv):
        drain(target, recv)
        total = target[0].astype(F32)
        for k in range(1, count):
            total = total + target[k].astype(F32)
        return total

    def hand_groups(total, held, targets, me, own, send, recv, device):
        for k, peer in enumerate(targets):
            held[k] = total[k * OWN : (k + 1) * OWN].astype(BF16)

            @pl.when(peer != me)
            def _():
                remote(held.at[k], own.at[me], send, recv, device(peer)).start()

            @pl.when(peer == me)
            def _():
                pltpu.make_async_copy(held.at[k], own.at[me], recv).start()

    def added(own, count):
        total = own[0].astype(F32)
        for k in range(1, count):
            total = total + own[k].astype(F32)
        return total

    for u in range(n + 6):
        if u < n:
            stream(u)
        if 3 <= u < n + 3:
            stream_relay(u - 3)
        if 6 <= u:
            if u == n + 4:
                break
            stream_finish(u - 6)
    drain(incoming.at[1], w_recv.at[n])
    merge(1, 0, fs // 4, 0)
    quad = [((z + 1 - 2 * ez) * n + y, t), (z * n + y + 1 - 2 * ey, t)]
    quad.append(((z + 1 - 2 * ez) * n + y + 1 - 2 * ey, t))
    for k, device in enumerate(quad):
        for held in (weights_8, weights_4):
            remote(held.at[1, t], held.at[2 + k, t], quad_send.at[k], quad_recv.at[k], device).start()
    spread(1)
    stream_finish(n - 2)
    stream_finish(n - 1)
    collected(0)
    hidden = hidden_of(normed[...], units(0, 0), units(0, 1))
    down_one = units(0, 2)
    wide = d // 2
    for cut in range(2):
        columns = slice(cut * wide, (cut + 1) * wide)
        for side in range(2):
            branch = branch_of(hidden[side * half : (side + 1) * half], down_one[:, columns])
            part[side, :, :, columns] = branch.reshape(n, block, wide)
            me = z if side == 0 else y
            for k in far_first(n):
                peer = lax.rem(me + k, n)
                remote(
                    part.at[side, peer, :, columns], landed.at[side, me, :, columns],
                    r_send.at[side], r_recv.at[side, cut], at(peer, y) if side == 0 else at(z, peer),
                ).start()
            pltpu.make_async_copy(
                part.at[side, me, :, columns], landed.at[side, me, :, columns], r_recv.at[side, cut]
            ).start()

    def sum_cut(cut):
        columns = slice(cut * wide, (cut + 1) * wide)
        for side in range(2):
            drain(landed.at[side, :, :, columns], r_recv.at[side, cut])
            total = landed[side, 0, :, columns].astype(F32)
            for k in range(1, n):
                total = total + landed[side, k, :, columns].astype(F32)
            for k in range(2):
                group[side, k, :, columns] = total[k * share : (k + 1) * share].astype(BF16)
            me = y if side == 0 else z
            for k in far_first(n):
                peer = lax.rem(me + k, n)
                remote(
                    group.at[side, lax.rem(peer, 2), :, columns], line.at[side, me, :, columns],
                    l_send.at[side], l_recv.at[side], at(z, peer) if side == 0 else at(peer, y),
                ).start()
            pltpu.make_async_copy(
                group.at[side, lax.rem(me, 2), :, columns], line.at[side, me, :, columns], l_recv.at[side]
            ).start()

    def prepare(s):
        collected(s)
        for w in range(3):
            ready[w, (s - 1) * SENT * n_tp : s * SENT * n_tp, :] = units(s, w)

    taken(quad_recv.at[0])
    spread(2)
    relay(1)
    for k in range(1, 3):
        taken(quad_recv.at[k])
        spread(2 + k)
    publish(0)
    sum_cut(0)
    relay(2)
    sum_cut(1)
    finish(1)
    relay(3)
    prepare(1)
    own_slot = jnp.where(even, q // 2, m // 2 + p // 2)
    for side in range(2):
        drain(line.at[side], l_recv.at[side])
        total = line[side, 0].astype(F32)
        for k in range(1, n):
            total = total + line[side, k].astype(F32)
        total = residual[side * share : (side + 1) * share] + 0.5 * total
        for k in range(m // 2):
            middle[side * (m // 2) + k] = total[k * OWN : (k + 1) * OWN].astype(BF16)
        me = p if side == 0 else q
        gathered[side, me] = rsqrt_norm(total.astype(BF16).astype(F32))
        for k in far_first(m):
            peer = lax.rem(me + k, m)
            remote(
                gathered.at[side, me], gathered.at[side, me], g_send.at[side], g_recv.at[side],
                at_two(peer, q) if side == 0 else at_two(p, peer),
            ).start()
    finish(2)
    relay(4)
    prepare(2)
    finish(3)
    prepare(3)
    finish(4)
    prepare(4)
    quarter = OWN * m * m // 2
    for side in range(2):
        drain(gathered.at[side, pl.ds(0, m - 1)], g_recv.at[side])
    hidden = hidden_of(gathered[...].reshape(2 * quarter, d), ready[0], ready[1])
    branch = branch_of(hidden, ready[2])
    part_two[...] = branch.reshape(part_two.shape)
    for side in range(2):
        send_blocks(
            part_two.at[side], landed_two.at[side], p if side == 0 else q, m, two_send.at[side],
            two_recv.at[side],
            (lambda peer: at_two(peer, q)) if side == 0 else (lambda peer: at_two(p, peer)),
        )
    publish(1)
    total = reduced(landed_two.at[0], m, two_recv.at[0])
    hand_groups(
        total, group_two.at[0], [2 * k + lax.rem(p, 2) for k in range(m // 2)], q,
        owner_two, q_send, q_recv, lambda peer: at_two(p, peer),
    )
    total = reduced(landed_two.at[1], m, two_recv.at[1])
    hand_groups(
        total, group_two.at[1], [2 * k + lax.rem(q + 1, 2) for k in range(m // 2)], p,
        owner_two, q_send, q_recv, lambda peer: at_two(peer, q),
    )
    for k in range(3):
        taken(quad_send.at[k])
    for s in range(5):
        taken_sets(x_send.at[s], 2 * nx - 1)
    for b in range(2):
        drain(outgoing.at[b, pl.ds(0, fs - 1)], w_send.at[b])
        drain(part.at[b, pl.ds(0, n - 1)], r_send.at[b])
        drain(line.at[b, pl.ds(0, n - 1)], l_send.at[b])
        drain(gathered.at[b, pl.ds(0, m - 1)], g_send.at[b])
        drain(gathered.at[b, pl.ds(0, m - 1)], two_send.at[b])
    drain(owner_two.at[pl.ds(0, m - 1)], q_send)
    drain(owner_two, q_recv)
    mixed[...] = (middle[own_slot].astype(F32) + 0.5 * added(owner_two, m)).astype(BF16)


def deliver(count, *refs):
    copies = [pltpu.make_async_copy(refs[k], refs[count + k], refs[-1].at[k]) for k in range(count)]
    for copy in copies:
        copy.start()
    for copy in copies:
        copy.wait()


def shards(
    tokens, gain_first, gate_first, up_first, down_first, gain_second, gate_second, up_second, down_second
):
    fs, n_tp = lax.axis_size("fs"), lax.axis_size("tp")
    n = int(round(fs**0.5))
    fd, local = gate_first.shape
    hu = local // fs
    d = fs * fd
    rows = tokens.shape[1]
    block = rows // 2 // n
    wide = -(-(local + 16) // 128) * 128
    vmem = pl.BlockSpec(memory_space=pltpu.VMEM)
    hbm = pl.BlockSpec(memory_space=pltpu.HBM)
    dma = pltpu.SemaphoreType.DMA
    m = n // 2
    two = (2, m, OWN * m // 2, d)
    results = pl.pallas_call(
        functools.partial(kernel, n, n_tp, hu, fd),
        out_shape=(
            jax.ShapeDtypeStruct((OWN, d), BF16),
        )
        + (jax.ShapeDtypeStruct((hu, n_tp, d), BF16),) * 6,
        in_specs=[hbm] * 9,
        out_specs=(vmem,) * 7,
        scratch_shapes=[
            pltpu.VMEM((rows, d), BF16),
            pltpu.VMEM((2, 1, fd), F32),
            pltpu.VMEM((2, 3, fd, local), F32),
            pltpu.VMEM((4 * fd, wide), F32),
            pltpu.VMEM((wide, 4 * fd), F32),
            pltpu.VMEM((2, fs, SENT // 4, 4, 128), BF16),
            pltpu.VMEM((2, 4, fs // 4, SENT // 4, 4, 128), BF16),
            pltpu.VMEM((4, 128, 3 * 128), BF16),
            pltpu.VMEM((5, n_tp, 3, 8, d), BF16),
            pltpu.VMEM((5, n_tp, 3, 4, d), BF16),
            pltpu.VMEM((3, 4 * 12 * n_tp, d), BF16),
            pltpu.VMEM((rows, d), BF16),
            pltpu.VMEM((2, n, block, d), BF16),
            pltpu.VMEM((2, n, block, d), BF16),
            pltpu.VMEM((2, 2, OWN * m // 2, d), BF16),
            pltpu.VMEM((2, n, OWN * m // 2, d), BF16),
            pltpu.VMEM(two, BF16),
            pltpu.VMEM(two, BF16),
            pltpu.VMEM(two, BF16),
            pltpu.VMEM((2, m // 2, OWN, d), BF16),
            pltpu.VMEM((m, OWN, d), BF16),
            pltpu.VMEM((m, OWN, d), BF16),
            pltpu.VMEM((OWN * m, d), F32),
            dma((2,)), dma((n + 1,)), dma((5,)), dma((n + 4, 2)), dma((n + 8,)), dma((5,)), dma((3,)), dma((3,)),
            dma((2,)), dma((2, 2)), dma((2,)), dma((2,)), dma((2,)), dma((2,)), dma(()), dma(()),
            dma((2,)), dma((2,)), dma((4,)),
        ],
        compiler_params=pltpu.CompilerParams(
            collective_id=0, has_side_effects=True, vmem_limit_bytes=46 * 1024 * 1024
        ),
    )(*[
        pltpu.with_memory_space_constraint(a, pltpu.HBM)
        for a in (
            tokens[0],
            gain_first[None], gate_first, up_first, down_first,
            gain_second[None], gate_second, up_second, down_second,
        )
    ]    )
    mixed, *served = pl.pallas_call(
        functools.partial(deliver, 7),
        out_shape=tuple(jax.ShapeDtypeStruct(r.shape, r.dtype) for r in results),
        in_specs=[vmem] * 7,
        out_specs=(hbm,) * 7,
        scratch_shapes=[dma((7,))],
        compiler_params=pltpu.CompilerParams(vmem_limit_bytes=1024 * 1024),
    )(*results)
    return (mixed[None],) + tuple(jnp.swapaxes(r, 0, 1) for r in served)


def solution(mesh):
    weight = P("fs", "tp")
    cut = P(None, "fs", None)
    return jax.shard_map(
        shards,
        mesh=mesh,
        in_specs=(P("tp", None, None), P("fs"), weight, weight, weight, P("fs"), weight, weight, weight),
        out_specs=(P("tp", "fs", None),) + (cut,) * 6,
        check_vma=False,
    )
```

```python
import functools

import jax
import jax.numpy as jnp
from jax import lax
from jax.experimental import pallas as pl
from jax.experimental.pallas import tpu as pltpu
from jax.sharding import PartitionSpec as P

MESH = pl.DeviceIdType.MESH
F32, BF16 = jnp.float32, jnp.bfloat16
SENT = 12
EARLY = 2
OWN = 4


def far_first(count):
    return sorted(range(1, count), key=lambda k: (-min(k, count - k), k))


def rsqrt_norm(wide):
    scale = lax.rsqrt(jnp.mean(wide * wide, axis=-1, keepdims=True) + 1e-06)
    return (wide * scale).astype(BF16)


def kernel(
    n, n_tp, hu, fd,
    tokens_hbm, gain_one, gate_one, up_one, down_one, gain_two, gate_two, up_two, down_two,
    mixed, out_0, out_1, out_2, out_3, out_4, out_5,
    tokens, gains, trained, stack, turned, outgoing, incoming, placing, weights_8, weights_4, ready, normed,
    part, landed, group, line, gathered, part_two, landed_two, middle, residual,
    w_send, w_recv, x_send, near_recv, half_recv, die_recv, quad_send, quad_recv, r_send, r_recv,
    l_send, l_recv, two_send, two_recv, g_send, g_recv, in_sem,
):
    staged = (out_0, out_1, out_2, out_3, out_4, out_5)
    fs = n * n
    d = fs * fd
    half = OWN * fs // 2
    block = half // n
    m = n // 2
    share = OWN * m // 2
    f, t = lax.axis_index("fs"), lax.axis_index("tp")
    z, y = f // n, lax.rem(f, n)
    ez, ey, p, q = lax.rem(z, 2), lax.rem(y, 2), z // 2, y // 2
    x, c = t // 2, lax.rem(t, 2)
    nx = n_tp // 2
    even = lax.rem(p + q, 2) == 0
    partner = (f, x * 2 + 1 - c)

    def at(zz, yy):
        return (zz * n + yy, t)

    def at_two(pp, qq):
        return ((2 * pp + ez) * n + 2 * qq + ey, t)

    def along(step):
        return (f, lax.rem(x + nx + step, nx) * 2 + c)

    def slot_of(step, core):
        return lax.rem(x + nx + step, nx) * 2 + core

    def remote(src, dst, send, recv, device):
        return pltpu.make_async_remote_copy(
            src_ref=src, dst_ref=dst, send_sem=send, recv_sem=recv, device_id=device, device_id_type=MESH
        )

    def drain(ref, sem):
        pltpu.make_async_copy(ref, ref, sem).wait()

    given = ((gain_one, gate_one, up_one, down_one), (gain_two, gate_two, up_two, down_two))
    for b, (gain, *each) in enumerate(given):
        pltpu.make_async_copy(gain, gains.at[b], in_sem.at[3]).start()
        for w in range(3):
            pltpu.make_async_copy(each[w], trained.at[b, w], in_sem.at[b]).start()
    pltpu.make_async_copy(tokens_hbm, tokens, in_sem.at[2]).start()

    barrier = pltpu.get_barrier_semaphore()

    @pl.loop(1, fs)
    def _(k):
        pl.semaphore_signal(barrier, inc=1, device_id=(lax.rem(f + k, fs), t), device_id_type=MESH)

    around = {1: (), 2: (1,), 4: (1, -1)}[nx]
    across = (2,) if nx == 4 else ()
    for step in around + across:
        pl.semaphore_signal(barrier, inc=1, device_id=along(step), device_id_type=MESH)
    pl.semaphore_signal(barrier, inc=1, device_id=partner, device_id_type=MESH)

    hidden_units = gate_one.shape[1]
    stack[...] = jnp.zeros_like(stack)
    drain(gains, in_sem.at[3])
    for b in range(2):
        drain(trained.at[b], in_sem.at[b])
        for w in range(3):
            stack[w * fd : (w + 1) * fd, 0:hidden_units] = trained[b, w]
        ones = jnp.ones((1, fd), F32)
        scale = jnp.concatenate([gains[b], gains[b], ones, ones], axis=1)
        turned[...] = stack[...].T * scale
        live = lax.broadcasted_iota(jnp.int32, (SENT, 128), 0) < hu
        for k in range(fs):
            rows = jnp.where(live, turned[k * hu : k * hu + SENT, :], 0.0)
            for g in range(SENT // 4):
                outgoing[b, k, g] = rows[4 * g : 4 * g + 4].astype(BF16)

    lanes = 3 * 128
    lane_in = lax.broadcasted_iota(jnp.int32, (128, lanes), 0)
    lane_out = lax.broadcasted_iota(jnp.int32, (128, lanes), 1)
    inner = lane_out % 128
    for i in range(4):
        chosen = (inner // 32 == i) & (lane_in == lane_out // 128 * 32 + inner % 32)
        placing[i] = jnp.where(chosen, 1.0, 0.0).astype(BF16)

    pl.semaphore_wait(barrier, fs - 1 + len(around + across) + 1)

    offsets = [(dz, dy) for dz in range(n) for dy in range(n) if dz or dy]
    offsets.sort(key=lambda o: (min(o[0], n - o[0]), -min(o[1], n - o[1])))
    for b in range(2):
        for dz, dy in offsets:
            peer = lax.rem(z + dz, n) * n + lax.rem(y + dy, n)
            remote(
                outgoing.at[b, peer],
                incoming.at[b, lax.rem(f, 4), f // 4],
                w_send.at[b],
                w_recv.at[z if b == 0 else n],
                (peer, t),
            ).start()

        pltpu.make_async_copy(
            outgoing.at[b, f], incoming.at[b, lax.rem(f, 4), f // 4], w_recv.at[z if b == 0 else n]
        ).start()

    drain(tokens, in_sem.at[2])
    wide = tokens[...].astype(F32)
    normed_rows = rsqrt_norm(wide)
    spot = lax.broadcasted_iota(jnp.int32, (2 * half, 2 * half), 0)
    source = lax.broadcasted_iota(jnp.int32, (2 * half, 2 * half), 1)
    in_first = spot < half
    inside = jnp.where(in_first, spot, spot - half)
    major = inside // block
    side_e = inside % block // share
    minor = inside % share // OWN
    row = inside % OWN
    first_home = major * n + 2 * (2 * minor + major // 2 % 2) + side_e
    second_home = (2 * (2 * minor + (major // 2 + 1) % 2) + side_e) * n + major
    home = jnp.where(in_first, first_home, second_home) * OWN + row
    shuffle = jnp.where(home == source, 1.0, 0.0).astype(BF16)
    normed[...] = jnp.dot(shuffle, normed_rows, preferred_element_type=F32).astype(BF16)
    pick_row = lax.broadcasted_iota(jnp.int32, (2 * share, 2 * half), 0)
    pick_source = lax.broadcasted_iota(jnp.int32, (2 * share, 2 * half), 1)
    inside = pick_row % share
    row_home = jnp.where(
        pick_row < share,
        z * n + 2 * (2 * (inside // OWN) + lax.rem(p, 2)) + ey,
        (2 * (2 * (inside // OWN) + lax.rem(q + 1, 2)) + ez) * n + y,
    )
    pick = jnp.where(pick_source == row_home * OWN + inside % OWN, 1.0, 0.0).astype(BF16)
    residual[...] = jnp.dot(pick, tokens[...], preferred_element_type=F32)

    per = n // 4
    strip = n * fd

    def merge(b, first, count, start):
        total = jnp.zeros((count * SENT, lanes), F32)
        for i in range(4):
            rows = jnp.concatenate(
                [incoming[b, i, first + j, g].astype(F32) for j in range(count) for g in range(SENT // 4)],
                axis=0,
            )
            total = total + jnp.dot(rows.astype(BF16), placing[i], preferred_element_type=F32)
        for j in range(count):
            for w in range(3):
                there = pl.ds(start + j * 128, 128)
                cut = total[j * SENT : (j + 1) * SENT, w * 128 : (w + 1) * 128]
                weights_8[b, t, w, :, there] = cut[0:8].astype(BF16)
                weights_4[b, t, w, :, there] = cut[8:12].astype(BF16)

    def send_piece(s, slot, send, recv, device, columns=pl.ds(0, d)):
        for held in (weights_8, weights_4):
            source = held.at[s, slot, :, :, columns]
            remote(source, source, send, recv, device).start()

    def taken(sem, columns=d):
        drain(weights_4.at[pl.ds(0, 3), 0, :, :, pl.ds(0, columns)], sem)

    def taken_sets(sem, count):
        drain(weights_4.at[pl.ds(0, 3), pl.ds(0, count)], sem)

    near_first = [0] + far_first(n)[::-1]

    def columns_of(u):
        return pl.multiple_of(lax.rem(z + near_first[u], n) * strip, strip)

    def stream(u):
        home = lax.rem(z + near_first[u], n)
        drain(incoming.at[0, 0, pl.ds(0, n)], w_recv.at[home])
        merge(0, home * per, per, columns_of(u))
        columns = pl.ds(columns_of(u), strip)
        for h, step in enumerate(around):
            send_piece(0, t, x_send.at[0], near_recv.at[u, h], along(step), columns)
        for step in across if u >= n // 2 else ():
            send_piece(0, t, x_send.at[0], half_recv.at[u], along(step), columns)
        send_piece(0, t, x_send.at[0], die_recv.at[0], partner, columns)

    def stream_relay(u):
        columns = pl.ds(columns_of(u), strip)
        for h, step in enumerate(around):
            slot = slot_of(-step, c)
            taken(near_recv.at[u, h], strip)
            if nx == 4 and h == u % 2 and u < n // 2:
                send_piece(0, slot, x_send.at[0], half_recv.at[u], along(step), columns)
            send_piece(0, slot, x_send.at[0], die_recv.at[0], partner, columns)

    def stream_finish(u):
        if nx == 4:
            taken(half_recv.at[u], strip)
            send_piece(
                0, slot_of(2, c), x_send.at[0], die_recv.at[0], partner, pl.ds(columns_of(u), strip)
            )

    def spread(s):
        for h, step in enumerate(around):
            send_piece(s, t, x_send.at[s], near_recv.at[n + s - 1, h], along(step))
        send_piece(s, t, x_send.at[s], die_recv.at[s], partner)

    def relay(s):
        for h, step in enumerate(around):
            slot = slot_of(-step, c)
            taken(near_recv.at[n + s - 1, h])
            if nx == 4:
                send_piece(
                    s, slot, x_send.at[s], half_recv.at[n + 2 * (s - 1) + h], along(step),
                    pl.ds(h * (d // 2), d // 2),
                )
            send_piece(s, slot, x_send.at[s], die_recv.at[s], partner)

    def finish(s):
        if nx == 4:
            for h in range(2):
                taken(half_recv.at[n + 2 * (s - 1) + h], d // 2)
                send_piece(
                    s, slot_of(2, c), x_send.at[s], die_recv.at[s], partner, pl.ds(h * (d // 2), d // 2)
                )

    def collected(s):
        taken_sets(die_recv.at[s], nx)

    def units(s, w):
        tail = jnp.concatenate([weights_4[s, j, w].astype(F32) for j in range(n_tp)], axis=0)
        return jnp.concatenate([weights_8[s, :, w].reshape(n_tp * 8, d), tail.astype(BF16)], axis=0)

    def publish(b):
        width = hu * n_tp
        spot = lax.broadcasted_iota(jnp.int32, (width, n_tp * 12), 0)
        source = lax.broadcasted_iota(jnp.int32, (width, n_tp * 12), 1)
        owner_of, unit = spot % n_tp, spot // n_tp
        from_spot = jnp.where(unit < 8, owner_of * 8 + unit, n_tp * 8 + owner_of * 4 + unit - 8)
        swap = jnp.where(source == from_spot, 1.0, 0.0).astype(BF16)
        for w in range(3):
            rows = jnp.dot(swap, units(b, w), preferred_element_type=F32)
            for r in range(hu):
                staged[3 * b + w][r] = rows[r * n_tp : (r + 1) * n_tp].astype(BF16)

    contract = (((1,), (1,)), ((), ()))

    def hidden_of(rows, gate, up):
        gate_act = lax.dot_general(rows, gate, contract, preferred_element_type=F32)
        up_act = lax.dot_general(rows, up, contract, preferred_element_type=F32)
        return (gate_act / (1.0 + jnp.exp(-gate_act)) * up_act).astype(BF16)

    def branch_of(hidden, down):
        return jnp.dot(hidden, down, preferred_element_type=F32).astype(BF16)

    def added(own, count):
        total = own[0].astype(F32)
        for k in range(1, count):
            total = total + own[k].astype(F32)
        return total

    quad = [((z + 1 - 2 * ez) * n + y, t), (z * n + y + 1 - 2 * ey, t)]
    quad.append(((z + 1 - 2 * ez) * n + y + 1 - 2 * ey, t))
    for u in range(n + 4):
        if u == n + EARLY:
            drain(incoming.at[1], w_recv.at[n])
            merge(1, 0, fs // 4, 0)
            for k, device in enumerate(quad):
                for held in (weights_8, weights_4):
                    remote(
                        held.at[1, t], held.at[2 + k, t], quad_send.at[k], quad_recv.at[k], device
                    ).start()
        if u < n:
            stream(u)
        if 3 <= u < n + 3:
            stream_relay(u - 3)
        if 6 <= u:
            stream_finish(u - 6)
    spread(1)
    stream_finish(n - 2)
    stream_finish(n - 1)
    collected(0)
    hidden = hidden_of(normed[...], units(0, 0), units(0, 1))
    down_one = units(0, 2)
    wide = d // 2
    for cut in range(2):
        columns = slice(cut * wide, (cut + 1) * wide)
        for side in range(2):
            branch = branch_of(hidden[side * half : (side + 1) * half], down_one[:, columns])
            part[side, :, :, columns] = branch.reshape(n, block, wide)
            me = z if side == 0 else y
            for k in far_first(n):
                peer = lax.rem(me + k, n)
                remote(
                    part.at[side, peer, :, columns], landed.at[side, me, :, columns],
                    r_send.at[side], r_recv.at[side, cut], at(peer, y) if side == 0 else at(z, peer),
                ).start()
            pltpu.make_async_copy(
                part.at[side, me, :, columns], landed.at[side, me, :, columns], r_recv.at[side, cut]
            ).start()

    def sum_cut(cut):
        columns = slice(cut * wide, (cut + 1) * wide)
        for side in range(2):
            drain(landed.at[side, :, :, columns], r_recv.at[side, cut])
            total = landed[side, 0, :, columns].astype(F32)
            for k in range(1, n):
                total = total + landed[side, k, :, columns].astype(F32)
            for k in range(2):
                group[side, k, :, columns] = total[k * share : (k + 1) * share].astype(BF16)
            me = y if side == 0 else z
            for k in far_first(n):
                peer = lax.rem(me + k, n)
                remote(
                    group.at[side, lax.rem(peer, 2), :, columns], line.at[side, me, :, columns],
                    l_send.at[side], l_recv.at[side], at(z, peer) if side == 0 else at(peer, y),
                ).start()
            pltpu.make_async_copy(
                group.at[side, lax.rem(me, 2), :, columns], line.at[side, me, :, columns], l_recv.at[side]
            ).start()

    def prepare(s):
        collected(s)
        for w in range(3):
            ready[w, (s - 1) * SENT * n_tp : s * SENT * n_tp, :] = units(s, w)

    taken(quad_recv.at[0])
    spread(2)
    relay(1)
    for k in range(1, 3):
        taken(quad_recv.at[k])
        spread(2 + k)
    publish(0)
    sum_cut(0)
    relay(2)
    sum_cut(1)
    relay(3)
    relay(4)
    finish(1)
    prepare(1)
    finish(2)
    prepare(2)
    own_slot = jnp.where(even, q // 2, m // 2 + p // 2)
    for side in range(2):
        drain(line.at[side], l_recv.at[side])
        total = line[side, 0].astype(F32)
        for k in range(1, n):
            total = total + line[side, k].astype(F32)
        total = residual[side * share : (side + 1) * share] + 0.5 * total
        for k in range(m // 2):
            middle[side * (m // 2) + k] = total[k * OWN : (k + 1) * OWN].astype(BF16)
        me = p if side == 0 else q
        gathered[side, me] = rsqrt_norm(total.astype(BF16).astype(F32))
        for k in far_first(m):
            peer = lax.rem(me + k, m)
            remote(
                gathered.at[side, me], gathered.at[side, me], g_send.at[side], g_recv.at[side],
                at_two(peer, q) if side == 0 else at_two(p, peer),
            ).start()
    finish(3)
    prepare(3)
    finish(4)
    prepare(4)
    quarter = OWN * m * m // 2
    for side in range(2):
        drain(gathered.at[side, pl.ds(0, m - 1)], g_recv.at[side])
    hidden = hidden_of(gathered[...].reshape(2 * quarter, d), ready[0], ready[1])
    branch = jnp.dot(hidden, ready[2], preferred_element_type=F32)
    for k in range(m * m):
        part_two[k] = branch[k * OWN : (k + 1) * OWN].astype(BF16)

    def place_of(pp, qq):
        return jnp.where(
            lax.rem(pp + qq, 2) == 0, pp * (m // 2) + qq // 2, m * m // 2 + qq * (m // 2) + pp // 2
        )

    hops = [(dp, dq) for dp in range(m) for dq in range(m) if dp or dq]
    hops.sort(key=lambda o: -(min(o[0], m - o[0]) + min(o[1], m - o[1])))
    for dp, dq in hops:
        pp, qq = lax.rem(p + dp, m), lax.rem(q + dq, m)
        remote(
            part_two.at[place_of(pp, qq)], landed_two.at[p * m + q], two_send, two_recv, at_two(pp, qq)
        ).start()
    pltpu.make_async_copy(part_two.at[place_of(p, q)], landed_two.at[p * m + q], two_recv).start()
    publish(1)
    for k in range(3):
        taken(quad_send.at[k])
    for s in range(5):
        taken_sets(x_send.at[s], 2 * nx - 1)
    for b in range(2):
        drain(outgoing.at[b, pl.ds(0, fs - 1)], w_send.at[b])
        drain(part.at[b, pl.ds(0, n - 1)], r_send.at[b])
        drain(line.at[b, pl.ds(0, n - 1)], l_send.at[b])
        drain(gathered.at[b, pl.ds(0, m - 1)], g_send.at[b])
    drain(part_two.at[pl.ds(0, m * m - 1)], two_send)
    drain(landed_two, two_recv)
    mixed[...] = (middle[own_slot].astype(F32) + 0.5 * added(landed_two, m * m)).astype(BF16)


def deliver(count, *refs):
    copies = [pltpu.make_async_copy(refs[k], refs[count + k], refs[-1].at[k]) for k in range(count)]
    for copy in copies:
        copy.start()
    for copy in copies:
        copy.wait()


def shards(
    tokens, gain_first, gate_first, up_first, down_first, gain_second, gate_second, up_second, down_second
):
    fs, n_tp = lax.axis_size("fs"), lax.axis_size("tp")
    n = int(round(fs**0.5))
    fd, local = gate_first.shape
    hu = local // fs
    d = fs * fd
    rows = tokens.shape[1]
    block = rows // 2 // n
    wide = -(-(local + 16) // 128) * 128
    vmem = pl.BlockSpec(memory_space=pltpu.VMEM)
    hbm = pl.BlockSpec(memory_space=pltpu.HBM)
    dma = pltpu.SemaphoreType.DMA
    m = n // 2
    two = (2, m, OWN * m // 2, d)
    results = pl.pallas_call(
        functools.partial(kernel, n, n_tp, hu, fd),
        out_shape=(
            jax.ShapeDtypeStruct((OWN, d), BF16),
        )
        + (jax.ShapeDtypeStruct((hu, n_tp, d), BF16),) * 6,
        in_specs=[hbm] * 9,
        out_specs=(vmem,) * 7,
        scratch_shapes=[
            pltpu.VMEM((rows, d), BF16),
            pltpu.VMEM((2, 1, fd), F32),
            pltpu.VMEM((2, 3, fd, local), F32),
            pltpu.VMEM((4 * fd, wide), F32),
            pltpu.VMEM((wide, 4 * fd), F32),
            pltpu.VMEM((2, fs, SENT // 4, 4, 128), BF16),
            pltpu.VMEM((2, 4, fs // 4, SENT // 4, 4, 128), BF16),
            pltpu.VMEM((4, 128, 3 * 128), BF16),
            pltpu.VMEM((5, n_tp, 3, 8, d), BF16),
            pltpu.VMEM((5, n_tp, 3, 4, d), BF16),
            pltpu.VMEM((3, 4 * 12 * n_tp, d), BF16),
            pltpu.VMEM((rows, d), BF16),
            pltpu.VMEM((2, n, block, d), BF16),
            pltpu.VMEM((2, n, block, d), BF16),
            pltpu.VMEM((2, 2, OWN * m // 2, d), BF16),
            pltpu.VMEM((2, n, OWN * m // 2, d), BF16),
            pltpu.VMEM(two, BF16),
            pltpu.VMEM((m * m, OWN, d), BF16),
            pltpu.VMEM((m * m, OWN, d), BF16),
            pltpu.VMEM((m, OWN, d), BF16),
            pltpu.VMEM((OWN * m, d), F32),
            dma((2,)), dma((n + 1,)), dma((5,)), dma((n + 4, 2)), dma((n + 8,)), dma((5,)), dma((3,)), dma((3,)),
            dma((2,)), dma((2, 2)), dma((2,)), dma((2,)), dma(()), dma(()),
            dma((2,)), dma((2,)), dma((4,)),
        ],
        compiler_params=pltpu.CompilerParams(
            collective_id=0, has_side_effects=True, vmem_limit_bytes=46 * 1024 * 1024
        ),
    )(*[
        pltpu.with_memory_space_constraint(a, pltpu.HBM)
        for a in (
            tokens[0],
            gain_first[None], gate_first, up_first, down_first,
            gain_second[None], gate_second, up_second, down_second,
        )
    ]    )
    mixed, *served = pl.pallas_call(
        functools.partial(deliver, 7),
        out_shape=tuple(jax.ShapeDtypeStruct(r.shape, r.dtype) for r in results),
        in_specs=[vmem] * 7,
        out_specs=(hbm,) * 7,
        scratch_shapes=[dma((7,))],
        compiler_params=pltpu.CompilerParams(vmem_limit_bytes=1024 * 1024),
    )(*results)
    return (mixed[None],) + tuple(jnp.swapaxes(r, 0, 1) for r in served)


def solution(mesh):
    weight = P("fs", "tp")
    cut = P(None, "fs", None)
    return jax.shard_map(
        shards,
        mesh=mesh,
        in_specs=(P("tp", None, None), P("fs"), weight, weight, weight, P("fs"), weight, weight, weight),
        out_specs=(P("tp", "fs", None),) + (cut,) * 6,
        check_vma=False,
    )
```

```python
import functools

import jax
import jax.numpy as jnp
from jax import lax
from jax.experimental import pallas as pl
from jax.experimental.pallas import tpu as pltpu
from jax.sharding import PartitionSpec as P

MESH = pl.DeviceIdType.MESH
F32, BF16 = jnp.float32, jnp.bfloat16
SENT = 12
EARLY = 4
RELAY = 6
FINISH = 7
DIRECT = 0
OWN = 4


def far_first(count):
    return sorted(range(1, count), key=lambda k: (-min(k, count - k), k))


def rsqrt_norm(wide):
    scale = lax.rsqrt(jnp.mean(wide * wide, axis=-1, keepdims=True) + 1e-06)
    return (wide * scale).astype(BF16)


def kernel(
    n, n_tp, hu, fd,
    tokens_hbm, gain_one, gate_one, up_one, down_one, gain_two, gate_two, up_two, down_two,
    mixed, out_0, out_1, out_2, out_3, out_4, out_5,
    tokens, gains, trained, stack, turned, outgoing, incoming, placing, weights_8, weights_4, ready, normed,
    part, landed, group, line, gathered, part_two, landed_two, middle, residual,
    w_send, w_recv, x_send, near_recv, half_recv, die_recv, quad_send, quad_recv, r_send, r_recv,
    l_send, l_recv, two_send, two_recv, g_send, g_recv, in_sem,
):
    staged = (out_0, out_1, out_2, out_3, out_4, out_5)
    fs = n * n
    d = fs * fd
    half = OWN * fs // 2
    block = half // n
    m = n // 2
    share = OWN * m // 2
    f, t = lax.axis_index("fs"), lax.axis_index("tp")
    z, y = f // n, lax.rem(f, n)
    ez, ey, p, q = lax.rem(z, 2), lax.rem(y, 2), z // 2, y // 2
    x, c = t // 2, lax.rem(t, 2)
    nx = n_tp // 2
    even = lax.rem(p + q, 2) == 0
    partner = (f, x * 2 + 1 - c)

    def at(zz, yy):
        return (zz * n + yy, t)

    def at_two(pp, qq):
        return ((2 * pp + ez) * n + 2 * qq + ey, t)

    def along(step):
        return (f, lax.rem(x + nx + step, nx) * 2 + c)

    def slot_of(step, core):
        return lax.rem(x + nx + step, nx) * 2 + core

    def remote(src, dst, send, recv, device):
        return pltpu.make_async_remote_copy(
            src_ref=src, dst_ref=dst, send_sem=send, recv_sem=recv, device_id=device, device_id_type=MESH
        )

    def drain(ref, sem):
        pltpu.make_async_copy(ref, ref, sem).wait()

    given = ((gain_one, gate_one, up_one, down_one), (gain_two, gate_two, up_two, down_two))
    for b, (gain, *each) in enumerate(given):
        pltpu.make_async_copy(gain, gains.at[b], in_sem.at[3]).start()
        for w in range(3):
            pltpu.make_async_copy(each[w], trained.at[b, w], in_sem.at[b]).start()
    pltpu.make_async_copy(tokens_hbm, tokens, in_sem.at[2]).start()

    barrier = pltpu.get_barrier_semaphore()

    offsets = [(dz, dy) for dz in range(n) for dy in range(n) if dz or dy]
    offsets.sort(key=lambda o: -(min(o[0], n - o[0]) + min(o[1], n - o[1])))
    for dz, dy in offsets:
        pl.semaphore_signal(
            barrier, inc=1, device_id=at(lax.rem(z + dz, n), lax.rem(y + dy, n)), device_id_type=MESH
        )

    around = {1: (), 2: (1,), 4: (1, -1)}[nx]
    across = (2,) if nx == 4 else ()
    for step in around + across:
        pl.semaphore_signal(barrier, inc=1, device_id=along(step), device_id_type=MESH)
    pl.semaphore_signal(barrier, inc=1, device_id=partner, device_id_type=MESH)

    hidden_units = gate_one.shape[1]
    stack[...] = jnp.zeros_like(stack)
    drain(gains, in_sem.at[3])
    ones = jnp.ones((1, fd), F32)
    live = lax.broadcasted_iota(jnp.int32, (SENT, 128), 0) < hu
    by_strip = sorted(offsets, key=lambda o: (min(o[0], n - o[0]), -min(o[1], n - o[1])))
    for b in range(2):
        drain(trained.at[b], in_sem.at[b])
        for w in range(3):
            stack[w * fd : (w + 1) * fd, 0:hidden_units] = trained[b, w]
        scale = jnp.concatenate([gains[b], gains[b], ones, ones], axis=1)
        turned[...] = stack[...].T * scale
        for k in range(fs):
            rows = jnp.where(live, turned[k * hu : k * hu + SENT, :], 0.0)
            for g in range(SENT // 4):
                outgoing[b, k, g] = rows[4 * g : 4 * g + 4].astype(BF16)
        if b == 0:
            pl.semaphore_wait(barrier, fs - 1 + len(around + across) + 1)
        for dz, dy in by_strip if b == 0 else offsets:
            peer = lax.rem(z + dz, n) * n + lax.rem(y + dy, n)
            remote(
                outgoing.at[b, peer],
                incoming.at[b, lax.rem(f, 4), f // 4],
                w_send.at[b],
                w_recv.at[z if b == 0 else n],
                (peer, t),
            ).start()

        pltpu.make_async_copy(
            outgoing.at[b, f], incoming.at[b, lax.rem(f, 4), f // 4], w_recv.at[z if b == 0 else n]
        ).start()

    lanes = 3 * 128
    lane_in = lax.broadcasted_iota(jnp.int32, (128, lanes), 0)
    lane_out = lax.broadcasted_iota(jnp.int32, (128, lanes), 1)
    inner = lane_out % 128
    for i in range(4):
        chosen = (inner // 32 == i) & (lane_in == lane_out // 128 * 32 + inner % 32)
        placing[i] = jnp.where(chosen, 1.0, 0.0).astype(BF16)

    drain(tokens, in_sem.at[2])
    wide = tokens[...].astype(F32)
    normed_rows = rsqrt_norm(wide)
    spot = lax.broadcasted_iota(jnp.int32, (2 * half, 2 * half), 0)
    source = lax.broadcasted_iota(jnp.int32, (2 * half, 2 * half), 1)
    in_first = spot < half
    inside = jnp.where(in_first, spot, spot - half)
    major = inside // block
    side_e = inside % block // share
    minor = inside % share // OWN
    row = inside % OWN
    first_home = major * n + 2 * (2 * minor + major // 2 % 2) + side_e
    second_home = (2 * (2 * minor + (major // 2 + 1) % 2) + side_e) * n + major
    home = jnp.where(in_first, first_home, second_home) * OWN + row
    shuffle = jnp.where(home == source, 1.0, 0.0).astype(BF16)
    normed[...] = jnp.dot(shuffle, normed_rows, preferred_element_type=F32).astype(BF16)
    pick_row = lax.broadcasted_iota(jnp.int32, (2 * share, 2 * half), 0)
    pick_source = lax.broadcasted_iota(jnp.int32, (2 * share, 2 * half), 1)
    inside = pick_row % share
    row_home = jnp.where(
        pick_row < share,
        z * n + 2 * (2 * (inside // OWN) + lax.rem(p, 2)) + ey,
        (2 * (2 * (inside // OWN) + lax.rem(q + 1, 2)) + ez) * n + y,
    )
    pick = jnp.where(pick_source == row_home * OWN + inside % OWN, 1.0, 0.0).astype(BF16)
    residual[...] = jnp.dot(pick, tokens[...], preferred_element_type=F32)

    per = n // 4
    strip = n * fd

    def merge(b, first, count, start):
        total = jnp.zeros((count * SENT, lanes), F32)
        for i in range(4):
            rows = jnp.concatenate(
                [incoming[b, i, first + j, g].astype(F32) for j in range(count) for g in range(SENT // 4)],
                axis=0,
            )
            total = total + jnp.dot(rows.astype(BF16), placing[i], preferred_element_type=F32)
        for j in range(count):
            for w in range(3):
                there = pl.ds(start + j * 128, 128)
                cut = total[j * SENT : (j + 1) * SENT, w * 128 : (w + 1) * 128]
                weights_8[b, t, w, :, there] = cut[0:8].astype(BF16)
                weights_4[b, t, w, :, there] = cut[8:12].astype(BF16)

    def send_piece(s, slot, send, recv, device, columns=pl.ds(0, d)):
        for held in (weights_8, weights_4):
            source = held.at[s, slot, :, :, columns]
            remote(source, source, send, recv, device).start()

    def taken(sem, columns=d):
        drain(weights_4.at[pl.ds(0, 3), 0, :, :, pl.ds(0, columns)], sem)

    def taken_sets(sem, count):
        drain(weights_4.at[pl.ds(0, 3), pl.ds(0, count)], sem)

    near_first = [0] + far_first(n)[::-1]

    def columns_of(u):
        return pl.multiple_of(lax.rem(z + near_first[u], n) * strip, strip)

    def stream(u):
        home = lax.rem(z + near_first[u], n)
        drain(incoming.at[0, 0, pl.ds(0, n)], w_recv.at[home])
        merge(0, home * per, per, columns_of(u))
        columns = pl.ds(columns_of(u), strip)
        for h, step in enumerate(around):
            send_piece(0, t, x_send.at[0], near_recv.at[u, h], along(step), columns)
        for step in across if u >= DIRECT else ():
            send_piece(0, t, x_send.at[0], half_recv.at[u], along(step), columns)
        send_piece(0, t, x_send.at[0], die_recv.at[0], partner, columns)

    def stream_relay(u):
        columns = pl.ds(columns_of(u), strip)
        for h, step in enumerate(around):
            slot = slot_of(-step, c)
            taken(near_recv.at[u, h], strip)
            if nx == 4 and h == u % 2 and u < DIRECT:
                send_piece(0, slot, x_send.at[0], half_recv.at[u], along(step), columns)
            send_piece(0, slot, x_send.at[0], die_recv.at[0], partner, columns)

    def stream_finish(u):
        if nx == 4:
            taken(half_recv.at[u], strip)
            send_piece(
                0, slot_of(2, c), x_send.at[0], die_recv.at[0], partner, pl.ds(columns_of(u), strip)
            )

    def spread(s):
        for h, step in enumerate(around):
            send_piece(s, t, x_send.at[s], near_recv.at[n + s - 1, h], along(step))
        send_piece(s, t, x_send.at[s], die_recv.at[s], partner)

    def relay(s):
        for h, step in enumerate(around):
            slot = slot_of(-step, c)
            taken(near_recv.at[n + s - 1, h])
            if nx == 4:
                send_piece(
                    s, slot, x_send.at[s], half_recv.at[n + 2 * (s - 1) + h], along(step),
                    pl.ds(h * (d // 2), d // 2),
                )
            send_piece(s, slot, x_send.at[s], die_recv.at[s], partner)

    def finish(s):
        if nx == 4:
            for h in range(2):
                taken(half_recv.at[n + 2 * (s - 1) + h], d // 2)
                send_piece(
                    s, slot_of(2, c), x_send.at[s], die_recv.at[s], partner, pl.ds(h * (d // 2), d // 2)
                )

    def collected(s):
        taken_sets(die_recv.at[s], nx)

    def units(s, w):
        tail = jnp.concatenate([weights_4[s, j, w].astype(F32) for j in range(n_tp)], axis=0)
        return jnp.concatenate([weights_8[s, :, w].reshape(n_tp * 8, d), tail.astype(BF16)], axis=0)

    def publish(b):
        width = hu * n_tp
        spot = lax.broadcasted_iota(jnp.int32, (width, n_tp * 12), 0)
        source = lax.broadcasted_iota(jnp.int32, (width, n_tp * 12), 1)
        owner_of, unit = spot % n_tp, spot // n_tp
        from_spot = jnp.where(unit < 8, owner_of * 8 + unit, n_tp * 8 + owner_of * 4 + unit - 8)
        swap = jnp.where(source == from_spot, 1.0, 0.0).astype(BF16)
        for w in range(3):
            rows = jnp.dot(swap, units(b, w), preferred_element_type=F32)
            for r in range(hu):
                staged[3 * b + w][r] = rows[r * n_tp : (r + 1) * n_tp].astype(BF16)

    contract = (((1,), (1,)), ((), ()))

    def hidden_of(rows, gate, up):
        gate_act = lax.dot_general(rows, gate, contract, preferred_element_type=F32)
        up_act = lax.dot_general(rows, up, contract, preferred_element_type=F32)
        return (gate_act / (1.0 + jnp.exp(-gate_act)) * up_act).astype(BF16)

    def branch_of(hidden, down):
        return jnp.dot(hidden, down, preferred_element_type=F32).astype(BF16)

    def added(own, count):
        total = own[0].astype(F32)
        for k in range(1, count):
            total = total + own[k].astype(F32)
        return total

    quad = [((z + 1 - 2 * ez) * n + y, t), (z * n + y + 1 - 2 * ey, t)]
    quad.append(((z + 1 - 2 * ez) * n + y + 1 - 2 * ey, t))
    for u in range(n + FINISH):
        if u == n + EARLY:
            drain(incoming.at[1], w_recv.at[n])
            merge(1, 0, fs // 4, 0)
            for k, device in enumerate(quad):
                for held in (weights_8, weights_4):
                    remote(
                        held.at[1, t], held.at[2 + k, t], quad_send.at[k], quad_recv.at[k], device
                    ).start()
            spread(1)
        if u < n:
            stream(u)
        if RELAY <= u < n + RELAY:
            stream_relay(u - RELAY)
        if FINISH <= u:
            stream_finish(u - FINISH)
    collected(0)
    hidden = hidden_of(normed[...], units(0, 0), units(0, 1))
    down_one = units(0, 2)
    wide = d // 2
    for cut in range(2):
        columns = slice(cut * wide, (cut + 1) * wide)
        for side in range(2):
            branch = branch_of(hidden[side * half : (side + 1) * half], down_one[:, columns])
            part[side, :, :, columns] = branch.reshape(n, block, wide)
            me = z if side == 0 else y
            for k in far_first(n):
                peer = lax.rem(me + k, n)
                remote(
                    part.at[side, peer, :, columns], landed.at[side, me, :, columns],
                    r_send.at[side], r_recv.at[side, cut], at(peer, y) if side == 0 else at(z, peer),
                ).start()
            pltpu.make_async_copy(
                part.at[side, me, :, columns], landed.at[side, me, :, columns], r_recv.at[side, cut]
            ).start()

    def sum_cut(cut):
        columns = slice(cut * wide, (cut + 1) * wide)
        for side in range(2):
            drain(landed.at[side, :, :, columns], r_recv.at[side, cut])
            total = landed[side, 0, :, columns].astype(F32)
            for k in range(1, n):
                total = total + landed[side, k, :, columns].astype(F32)
            for k in range(2):
                group[side, k, :, columns] = total[k * share : (k + 1) * share].astype(BF16)
            me = y if side == 0 else z
            for k in far_first(n):
                peer = lax.rem(me + k, n)
                remote(
                    group.at[side, lax.rem(peer, 2), :, columns], line.at[side, me, :, columns],
                    l_send.at[side], l_recv.at[side], at(z, peer) if side == 0 else at(peer, y),
                ).start()
            pltpu.make_async_copy(
                group.at[side, lax.rem(me, 2), :, columns], line.at[side, me, :, columns], l_recv.at[side]
            ).start()

    def prepare(s):
        collected(s)
        for w in range(3):
            ready[w, (s - 1) * SENT * n_tp : s * SENT * n_tp, :] = units(s, w)

    taken(quad_recv.at[0])
    spread(2)
    relay(1)
    for k in range(1, 3):
        taken(quad_recv.at[k])
        spread(2 + k)
    publish(0)
    sum_cut(0)
    relay(2)
    sum_cut(1)
    relay(3)
    relay(4)
    finish(1)
    prepare(1)
    finish(2)
    prepare(2)
    own_slot = jnp.where(even, q // 2, m // 2 + p // 2)
    for side in range(2):
        drain(line.at[side], l_recv.at[side])
        total = line[side, 0].astype(F32)
        for k in range(1, n):
            total = total + line[side, k].astype(F32)
        total = residual[side * share : (side + 1) * share] + 0.5 * total
        for k in range(m // 2):
            middle[side * (m // 2) + k] = total[k * OWN : (k + 1) * OWN].astype(BF16)
        me = p if side == 0 else q
        gathered[side, me] = rsqrt_norm(total.astype(BF16).astype(F32))
        for k in far_first(m):
            peer = lax.rem(me + k, m)
            remote(
                gathered.at[side, me], gathered.at[side, me], g_send.at[side], g_recv.at[side],
                at_two(peer, q) if side == 0 else at_two(p, peer),
            ).start()
    finish(3)
    prepare(3)
    finish(4)
    prepare(4)
    quarter = OWN * m * m // 2
    for side in range(2):
        drain(gathered.at[side, pl.ds(0, m - 1)], g_recv.at[side])
    hidden = hidden_of(gathered[...].reshape(2 * quarter, d), ready[0], ready[1])
    branch = jnp.dot(hidden, ready[2], preferred_element_type=F32)
    for k in range(m * m):
        part_two[k] = branch[k * OWN : (k + 1) * OWN].astype(BF16)

    def place_of(pp, qq):
        return jnp.where(
            lax.rem(pp + qq, 2) == 0, pp * (m // 2) + qq // 2, m * m // 2 + qq * (m // 2) + pp // 2
        )

    hops = [(dp, dq) for dp in range(m) for dq in range(m) if dp or dq]
    hops.sort(key=lambda o: -(min(o[0], m - o[0]) + min(o[1], m - o[1])))
    for dp, dq in hops:
        pp, qq = lax.rem(p + dp, m), lax.rem(q + dq, m)
        remote(
            part_two.at[place_of(pp, qq)], landed_two.at[p * m + q], two_send, two_recv, at_two(pp, qq)
        ).start()
    pltpu.make_async_copy(part_two.at[place_of(p, q)], landed_two.at[p * m + q], two_recv).start()
    publish(1)
    for k in range(3):
        taken(quad_send.at[k])
    for s in range(5):
        taken_sets(x_send.at[s], 2 * nx - 1)
    for b in range(2):
        drain(outgoing.at[b, pl.ds(0, fs - 1)], w_send.at[b])
        drain(part.at[b, pl.ds(0, n - 1)], r_send.at[b])
        drain(line.at[b, pl.ds(0, n - 1)], l_send.at[b])
        drain(gathered.at[b, pl.ds(0, m - 1)], g_send.at[b])
    drain(part_two.at[pl.ds(0, m * m - 1)], two_send)
    drain(landed_two, two_recv)
    mixed[...] = (middle[own_slot].astype(F32) + 0.5 * added(landed_two, m * m)).astype(BF16)


def deliver(count, *refs):
    copies = [pltpu.make_async_copy(refs[k], refs[count + k], refs[-1].at[k]) for k in range(count)]
    for copy in copies:
        copy.start()
    for copy in copies:
        copy.wait()


def shards(
    tokens, gain_first, gate_first, up_first, down_first, gain_second, gate_second, up_second, down_second
):
    fs, n_tp = lax.axis_size("fs"), lax.axis_size("tp")
    n = int(round(fs**0.5))
    fd, local = gate_first.shape
    hu = local // fs
    d = fs * fd
    rows = tokens.shape[1]
    block = rows // 2 // n
    wide = -(-(local + 16) // 128) * 128
    vmem = pl.BlockSpec(memory_space=pltpu.VMEM)
    hbm = pl.BlockSpec(memory_space=pltpu.HBM)
    dma = pltpu.SemaphoreType.DMA
    m = n // 2
    two = (2, m, OWN * m // 2, d)
    results = pl.pallas_call(
        functools.partial(kernel, n, n_tp, hu, fd),
        out_shape=(
            jax.ShapeDtypeStruct((OWN, d), BF16),
        )
        + (jax.ShapeDtypeStruct((hu, n_tp, d), BF16),) * 6,
        in_specs=[hbm] * 9,
        out_specs=(vmem,) * 7,
        scratch_shapes=[
            pltpu.VMEM((rows, d), BF16),
            pltpu.VMEM((2, 1, fd), F32),
            pltpu.VMEM((2, 3, fd, local), F32),
            pltpu.VMEM((4 * fd, wide), F32),
            pltpu.VMEM((wide, 4 * fd), F32),
            pltpu.VMEM((2, fs, SENT // 4, 4, 128), BF16),
            pltpu.VMEM((2, 4, fs // 4, SENT // 4, 4, 128), BF16),
            pltpu.VMEM((4, 128, 3 * 128), BF16),
            pltpu.VMEM((5, n_tp, 3, 8, d), BF16),
            pltpu.VMEM((5, n_tp, 3, 4, d), BF16),
            pltpu.VMEM((3, 4 * 12 * n_tp, d), BF16),
            pltpu.VMEM((rows, d), BF16),
            pltpu.VMEM((2, n, block, d), BF16),
            pltpu.VMEM((2, n, block, d), BF16),
            pltpu.VMEM((2, 2, OWN * m // 2, d), BF16),
            pltpu.VMEM((2, n, OWN * m // 2, d), BF16),
            pltpu.VMEM(two, BF16),
            pltpu.VMEM((m * m, OWN, d), BF16),
            pltpu.VMEM((m * m, OWN, d), BF16),
            pltpu.VMEM((m, OWN, d), BF16),
            pltpu.VMEM((OWN * m, d), F32),
            dma((2,)), dma((n + 1,)), dma((5,)), dma((n + 4, 2)), dma((n + 8,)), dma((5,)), dma((3,)), dma((3,)),
            dma((2,)), dma((2, 2)), dma((2,)), dma((2,)), dma(()), dma(()),
            dma((2,)), dma((2,)), dma((4,)),
        ],
        compiler_params=pltpu.CompilerParams(
            collective_id=0, has_side_effects=True, vmem_limit_bytes=46 * 1024 * 1024
        ),
    )(*[
        pltpu.with_memory_space_constraint(a, pltpu.HBM)
        for a in (
            tokens[0],
            gain_first[None], gate_first, up_first, down_first,
            gain_second[None], gate_second, up_second, down_second,
        )
    ]    )
    mixed, *served = pl.pallas_call(
        functools.partial(deliver, 7),
        out_shape=tuple(jax.ShapeDtypeStruct(r.shape, r.dtype) for r in results),
        in_specs=[vmem] * 7,
        out_specs=(hbm,) * 7,
        scratch_shapes=[dma((7,))],
        compiler_params=pltpu.CompilerParams(vmem_limit_bytes=1024 * 1024),
    )(*results)
    return (mixed[None],) + tuple(jnp.swapaxes(r, 0, 1) for r in served)


def solution(mesh):
    weight = P("fs", "tp")
    cut = P(None, "fs", None)
    return jax.shard_map(
        shards,
        mesh=mesh,
        in_specs=(P("tp", None, None), P("fs"), weight, weight, weight, P("fs"), weight, weight, weight),
        out_specs=(P("tp", "fs", None),) + (cut,) * 6,
        check_vma=False,
    )
```

```python
import functools

import jax
import jax.numpy as jnp
from jax import lax
from jax.experimental import pallas as pl
from jax.experimental.pallas import tpu as pltpu
from jax.sharding import PartitionSpec as P

MESH = pl.DeviceIdType.MESH
F32, BF16 = jnp.float32, jnp.bfloat16
SENT = 12
EARLY = 3
RELAY = 6
FINISH = 7
DIRECT = 0
OWN = 4


def far_first(count):
    return sorted(range(1, count), key=lambda k: (-min(k, count - k), k))


def rsqrt_norm(wide):
    scale = lax.rsqrt(jnp.mean(wide * wide, axis=-1, keepdims=True) + 1e-06)
    return (wide * scale).astype(BF16)


def kernel(
    n, n_tp, hu, fd,
    tokens_hbm, gain_one, gate_one, up_one, down_one, gain_two, gate_two, up_two, down_two,
    mixed, out_0, out_1, out_2, out_3, out_4, out_5,
    tokens, gains, trained, stack, turned, outgoing, incoming, placing, weights_8, weights_4, ready, normed,
    part, landed, group, line, gathered, part_two, landed_two, middle, residual,
    w_send, w_recv, x_send, near_recv, half_recv, die_recv, quad_send, quad_recv, r_send, r_recv,
    l_send, l_recv, two_send, two_recv, g_send, g_recv, in_sem,
):
    staged = (out_0, out_1, out_2, out_3, out_4, out_5)
    fs = n * n
    d = fs * fd
    half = OWN * fs // 2
    block = half // n
    m = n // 2
    share = OWN * m // 2
    f, t = lax.axis_index("fs"), lax.axis_index("tp")
    z, y = f // n, lax.rem(f, n)
    ez, ey, p, q = lax.rem(z, 2), lax.rem(y, 2), z // 2, y // 2
    x, c = t // 2, lax.rem(t, 2)
    nx = n_tp // 2
    even = lax.rem(p + q, 2) == 0
    partner = (f, x * 2 + 1 - c)

    def at(zz, yy):
        return (zz * n + yy, t)

    def at_two(pp, qq):
        return ((2 * pp + ez) * n + 2 * qq + ey, t)

    def along(step):
        return (f, lax.rem(x + nx + step, nx) * 2 + c)

    def slot_of(step, core):
        return lax.rem(x + nx + step, nx) * 2 + core

    def remote(src, dst, send, recv, device):
        return pltpu.make_async_remote_copy(
            src_ref=src, dst_ref=dst, send_sem=send, recv_sem=recv, device_id=device, device_id_type=MESH
        )

    def drain(ref, sem):
        pltpu.make_async_copy(ref, ref, sem).wait()

    given = ((gain_one, gate_one, up_one, down_one), (gain_two, gate_two, up_two, down_two))
    for b, (gain, *each) in enumerate(given):
        pltpu.make_async_copy(gain, gains.at[b], in_sem.at[3]).start()
        for w in range(3):
            pltpu.make_async_copy(each[w], trained.at[b, w], in_sem.at[b]).start()
    pltpu.make_async_copy(tokens_hbm, tokens, in_sem.at[2]).start()

    barrier = pltpu.get_barrier_semaphore()

    offsets = [(dz, dy) for dz in range(n) for dy in range(n) if dz or dy]
    offsets.sort(key=lambda o: -(min(o[0], n - o[0]) + min(o[1], n - o[1])))
    for dz, dy in offsets:
        pl.semaphore_signal(
            barrier, inc=1, device_id=at(lax.rem(z + dz, n), lax.rem(y + dy, n)), device_id_type=MESH
        )

    around = {1: (), 2: (1,), 4: (1, -1)}[nx]
    across = (2,) if nx == 4 else ()
    for step in around + across:
        pl.semaphore_signal(barrier, inc=1, device_id=along(step), device_id_type=MESH)
    pl.semaphore_signal(barrier, inc=1, device_id=partner, device_id_type=MESH)

    hidden_units = gate_one.shape[1]
    stack[...] = jnp.zeros_like(stack)
    drain(gains, in_sem.at[3])
    ones = jnp.ones((1, fd), F32)
    live = lax.broadcasted_iota(jnp.int32, (SENT, 128), 0) < hu
    by_strip = sorted(offsets, key=lambda o: (min(o[0], n - o[0]), -min(o[1], n - o[1])))
    for b in range(2):
        drain(trained.at[b], in_sem.at[b])
        for w in range(3):
            stack[w * fd : (w + 1) * fd, 0:hidden_units] = trained[b, w]
        scale = jnp.concatenate([gains[b], gains[b], ones, ones], axis=1)
        turned[...] = stack[...].T * scale
        for k in range(fs):
            rows = jnp.where(live, turned[k * hu : k * hu + SENT, :], 0.0)
            for g in range(SENT // 4):
                outgoing[b, k, g] = rows[4 * g : 4 * g + 4].astype(BF16)
        if b == 0:
            pl.semaphore_wait(barrier, fs - 1 + len(around + across) + 1)
        for dz, dy in by_strip if b == 0 else offsets:
            peer = lax.rem(z + dz, n) * n + lax.rem(y + dy, n)
            remote(
                outgoing.at[b, peer],
                incoming.at[b, lax.rem(f, 4), f // 4],
                w_send.at[b],
                w_recv.at[z if b == 0 else n],
                (peer, t),
            ).start()

        pltpu.make_async_copy(
            outgoing.at[b, f], incoming.at[b, lax.rem(f, 4), f // 4], w_recv.at[z if b == 0 else n]
        ).start()

    lanes = 3 * 128
    lane_in = lax.broadcasted_iota(jnp.int32, (128, lanes), 0)
    lane_out = lax.broadcasted_iota(jnp.int32, (128, lanes), 1)
    inner = lane_out % 128
    for i in range(4):
        chosen = (inner // 32 == i) & (lane_in == lane_out // 128 * 32 + inner % 32)
        placing[i] = jnp.where(chosen, 1.0, 0.0).astype(BF16)

    drain(tokens, in_sem.at[2])
    wide = tokens[...].astype(F32)
    normed_rows = rsqrt_norm(wide)
    spot = lax.broadcasted_iota(jnp.int32, (2 * half, 2 * half), 0)
    source = lax.broadcasted_iota(jnp.int32, (2 * half, 2 * half), 1)
    in_first = spot < half
    inside = jnp.where(in_first, spot, spot - half)
    major = inside // block
    side_e = inside % block // share
    minor = inside % share // OWN
    row = inside % OWN
    first_home = major * n + 2 * (2 * minor + major // 2 % 2) + side_e
    second_home = (2 * (2 * minor + (major // 2 + 1) % 2) + side_e) * n + major
    home = jnp.where(in_first, first_home, second_home) * OWN + row
    shuffle = jnp.where(home == source, 1.0, 0.0).astype(BF16)
    normed[...] = jnp.dot(shuffle, normed_rows, preferred_element_type=F32).astype(BF16)
    pick_row = lax.broadcasted_iota(jnp.int32, (2 * share, 2 * half), 0)
    pick_source = lax.broadcasted_iota(jnp.int32, (2 * share, 2 * half), 1)
    inside = pick_row % share
    row_home = jnp.where(
        pick_row < share,
        z * n + 2 * (2 * (inside // OWN) + lax.rem(p, 2)) + ey,
        (2 * (2 * (inside // OWN) + lax.rem(q + 1, 2)) + ez) * n + y,
    )
    pick = jnp.where(pick_source == row_home * OWN + inside % OWN, 1.0, 0.0).astype(BF16)
    residual[...] = jnp.dot(pick, tokens[...], preferred_element_type=F32)

    per = n // 4
    strip = n * fd

    def merge(b, first, count, start):
        total = jnp.zeros((count * SENT, lanes), F32)
        for i in range(4):
            rows = jnp.concatenate(
                [incoming[b, i, first + j, g].astype(F32) for j in range(count) for g in range(SENT // 4)],
                axis=0,
            )
            total = total + jnp.dot(rows.astype(BF16), placing[i], preferred_element_type=F32)
        for j in range(count):
            for w in range(3):
                there = pl.ds(start + j * 128, 128)
                cut = total[j * SENT : (j + 1) * SENT, w * 128 : (w + 1) * 128]
                weights_8[b, t, w, :, there] = cut[0:8].astype(BF16)
                weights_4[b, t, w, :, there] = cut[8:12].astype(BF16)

    def send_piece(s, slot, send, recv, device, columns=pl.ds(0, d)):
        for held in (weights_8, weights_4):
            source = held.at[s, slot, :, :, columns]
            remote(source, source, send, recv, device).start()

    def taken(sem, columns=d):
        drain(weights_4.at[pl.ds(0, 3), 0, :, :, pl.ds(0, columns)], sem)

    def taken_sets(sem, count):
        drain(weights_4.at[pl.ds(0, 3), pl.ds(0, count)], sem)

    near_first = [0] + far_first(n)[::-1]

    def columns_of(u):
        return pl.multiple_of(lax.rem(z + near_first[u], n) * strip, strip)

    def stream(u):
        home = lax.rem(z + near_first[u], n)
        drain(incoming.at[0, 0, pl.ds(0, n)], w_recv.at[home])
        merge(0, home * per, per, columns_of(u))
        columns = pl.ds(columns_of(u), strip)
        for h, step in enumerate(around):
            send_piece(0, t, x_send.at[0], near_recv.at[u, h], along(step), columns)
        for step in across if u >= DIRECT else ():
            send_piece(0, t, x_send.at[0], half_recv.at[u], along(step), columns)
        send_piece(0, t, x_send.at[0], die_recv.at[0], partner, columns)

    def stream_relay(u):
        columns = pl.ds(columns_of(u), strip)
        for h, step in enumerate(around):
            slot = slot_of(-step, c)
            taken(near_recv.at[u, h], strip)
            if nx == 4 and h == u % 2 and u < DIRECT:
                send_piece(0, slot, x_send.at[0], half_recv.at[u], along(step), columns)
            send_piece(0, slot, x_send.at[0], die_recv.at[0], partner, columns)

    def stream_finish(u):
        if nx == 4:
            taken(half_recv.at[u], strip)
            send_piece(
                0, slot_of(2, c), x_send.at[0], die_recv.at[0], partner, pl.ds(columns_of(u), strip)
            )

    def spread(s):
        for h, step in enumerate(around):
            send_piece(s, t, x_send.at[s], near_recv.at[n + s - 1, h], along(step))
        send_piece(s, t, x_send.at[s], die_recv.at[s], partner)

    def relay(s):
        for h, step in enumerate(around):
            slot = slot_of(-step, c)
            taken(near_recv.at[n + s - 1, h])
            if nx == 4:
                send_piece(
                    s, slot, x_send.at[s], half_recv.at[n + 2 * (s - 1) + h], along(step),
                    pl.ds(h * (d // 2), d // 2),
                )
            send_piece(s, slot, x_send.at[s], die_recv.at[s], partner)

    def finish(s):
        if nx == 4:
            for h in range(2):
                taken(half_recv.at[n + 2 * (s - 1) + h], d // 2)
                send_piece(
                    s, slot_of(2, c), x_send.at[s], die_recv.at[s], partner, pl.ds(h * (d // 2), d // 2)
                )

    def collected(s):
        taken_sets(die_recv.at[s], nx)

    def units(s, w):
        tail = jnp.concatenate([weights_4[s, j, w].astype(F32) for j in range(n_tp)], axis=0)
        return jnp.concatenate([weights_8[s, :, w].reshape(n_tp * 8, d), tail.astype(BF16)], axis=0)

    def publish(b):
        width = hu * n_tp
        spot = lax.broadcasted_iota(jnp.int32, (width, n_tp * 12), 0)
        source = lax.broadcasted_iota(jnp.int32, (width, n_tp * 12), 1)
        owner_of, unit = spot % n_tp, spot // n_tp
        from_spot = jnp.where(unit < 8, owner_of * 8 + unit, n_tp * 8 + owner_of * 4 + unit - 8)
        swap = jnp.where(source == from_spot, 1.0, 0.0).astype(BF16)
        for w in range(3):
            rows = jnp.dot(swap, units(b, w), preferred_element_type=F32)
            for r in range(hu):
                staged[3 * b + w][r] = rows[r * n_tp : (r + 1) * n_tp].astype(BF16)

    contract = (((1,), (1,)), ((), ()))

    def hidden_of(rows, gate, up):
        gate_act = lax.dot_general(rows, gate, contract, preferred_element_type=F32)
        up_act = lax.dot_general(rows, up, contract, preferred_element_type=F32)
        return (gate_act / (1.0 + jnp.exp(-gate_act)) * up_act).astype(BF16)

    def branch_of(hidden, down):
        return jnp.dot(hidden, down, preferred_element_type=F32).astype(BF16)

    def added(own, count):
        total = own[0].astype(F32)
        for k in range(1, count):
            total = total + own[k].astype(F32)
        return total

    quad = [((z + 1 - 2 * ez) * n + y, t), (z * n + y + 1 - 2 * ey, t)]
    quad.append(((z + 1 - 2 * ez) * n + y + 1 - 2 * ey, t))
    for u in range(n + FINISH):
        if u == n + EARLY:
            drain(incoming.at[1], w_recv.at[n])
            merge(1, 0, fs // 4, 0)
            for k, device in enumerate(quad):
                for held in (weights_8, weights_4):
                    remote(
                        held.at[1, t], held.at[2 + k, t], quad_send.at[k], quad_recv.at[k], device
                    ).start()
            spread(1)
        if u < n:
            stream(u)
        if RELAY <= u < n + RELAY:
            stream_relay(u - RELAY)
        if FINISH <= u:
            stream_finish(u - FINISH)
    collected(0)
    gate_one_units, up_one_units, down_one = units(0, 0), units(0, 1), units(0, 2)
    hidden = [None, None]
    wide = d // 2
    for cut in range(2):
        columns = slice(cut * wide, (cut + 1) * wide)
        for side in range(2):
            if cut == 0:
                rows = normed[side * half : (side + 1) * half, :]
                hidden[side] = hidden_of(rows, gate_one_units, up_one_units)
            branch = branch_of(hidden[side], down_one[:, columns])
            part[side, :, :, columns] = branch.reshape(n, block, wide)
            me = z if side == 0 else y
            for k in far_first(n):
                peer = lax.rem(me + k, n)
                remote(
                    part.at[side, peer, :, columns], landed.at[side, me, :, columns],
                    r_send.at[side], r_recv.at[side, cut], at(peer, y) if side == 0 else at(z, peer),
                ).start()
            pltpu.make_async_copy(
                part.at[side, me, :, columns], landed.at[side, me, :, columns], r_recv.at[side, cut]
            ).start()

    def sum_cut(cut):
        columns = slice(cut * wide, (cut + 1) * wide)
        for side in range(2):
            drain(landed.at[side, :, :, columns], r_recv.at[side, cut])
            total = landed[side, 0, :, columns].astype(F32)
            for k in range(1, n):
                total = total + landed[side, k, :, columns].astype(F32)
            for k in range(2):
                group[side, k, :, columns] = total[k * share : (k + 1) * share].astype(BF16)
            me = y if side == 0 else z
            for k in far_first(n):
                peer = lax.rem(me + k, n)
                remote(
                    group.at[side, lax.rem(peer, 2), :, columns], line.at[side, me, :, columns],
                    l_send.at[side], l_recv.at[side], at(z, peer) if side == 0 else at(peer, y),
                ).start()
            pltpu.make_async_copy(
                group.at[side, lax.rem(me, 2), :, columns], line.at[side, me, :, columns], l_recv.at[side]
            ).start()

    def prepare(s):
        collected(s)
        for w in range(3):
            ready[w, (s - 1) * SENT * n_tp : s * SENT * n_tp, :] = units(s, w)

    taken(quad_recv.at[0])
    spread(2)
    relay(1)
    for k in range(1, 3):
        taken(quad_recv.at[k])
        spread(2 + k)
    publish(0)
    sum_cut(0)
    relay(2)
    sum_cut(1)
    relay(3)
    relay(4)
    finish(1)
    prepare(1)
    finish(2)
    prepare(2)
    own_slot = jnp.where(even, q // 2, m // 2 + p // 2)
    for side in range(2):
        drain(line.at[side], l_recv.at[side])
        total = line[side, 0].astype(F32)
        for k in range(1, n):
            total = total + line[side, k].astype(F32)
        total = residual[side * share : (side + 1) * share] + 0.5 * total
        for k in range(m // 2):
            middle[side * (m // 2) + k] = total[k * OWN : (k + 1) * OWN].astype(BF16)
        me = p if side == 0 else q
        gathered[side, me] = rsqrt_norm(total.astype(BF16).astype(F32))
        for k in far_first(m):
            peer = lax.rem(me + k, m)
            remote(
                gathered.at[side, me], gathered.at[side, me], g_send.at[side], g_recv.at[side],
                at_two(peer, q) if side == 0 else at_two(p, peer),
            ).start()
    finish(3)
    prepare(3)
    finish(4)
    prepare(4)
    quarter = OWN * m * m // 2
    for side in range(2):
        drain(gathered.at[side, pl.ds(0, m - 1)], g_recv.at[side])
    hidden = hidden_of(gathered[...].reshape(2 * quarter, d), ready[0], ready[1])
    branch = jnp.dot(hidden, ready[2], preferred_element_type=F32)
    for k in range(m * m):
        part_two[k] = branch[k * OWN : (k + 1) * OWN].astype(BF16)

    def place_of(pp, qq):
        return jnp.where(
            lax.rem(pp + qq, 2) == 0, pp * (m // 2) + qq // 2, m * m // 2 + qq * (m // 2) + pp // 2
        )

    hops = [(dp, dq) for dp in range(m) for dq in range(m) if dp or dq]
    hops.sort(key=lambda o: -(min(o[0], m - o[0]) + min(o[1], m - o[1])))
    for dp, dq in hops:
        pp, qq = lax.rem(p + dp, m), lax.rem(q + dq, m)
        remote(
            part_two.at[place_of(pp, qq)], landed_two.at[p * m + q], two_send, two_recv, at_two(pp, qq)
        ).start()
    pltpu.make_async_copy(part_two.at[place_of(p, q)], landed_two.at[p * m + q], two_recv).start()
    publish(1)
    for k in range(3):
        taken(quad_send.at[k])
    for s in range(5):
        taken_sets(x_send.at[s], 2 * nx - 1)
    for b in range(2):
        drain(outgoing.at[b, pl.ds(0, fs - 1)], w_send.at[b])
        drain(part.at[b, pl.ds(0, n - 1)], r_send.at[b])
        drain(line.at[b, pl.ds(0, n - 1)], l_send.at[b])
        drain(gathered.at[b, pl.ds(0, m - 1)], g_send.at[b])
    drain(part_two.at[pl.ds(0, m * m - 1)], two_send)
    drain(landed_two, two_recv)
    mixed[...] = (middle[own_slot].astype(F32) + 0.5 * added(landed_two, m * m)).astype(BF16)


def deliver(count, *refs):
    copies = [pltpu.make_async_copy(refs[k], refs[count + k], refs[-1].at[k]) for k in range(count)]
    for copy in copies:
        copy.start()
    for copy in copies:
        copy.wait()


def shards(
    tokens, gain_first, gate_first, up_first, down_first, gain_second, gate_second, up_second, down_second
):
    fs, n_tp = lax.axis_size("fs"), lax.axis_size("tp")
    n = int(round(fs**0.5))
    fd, local = gate_first.shape
    hu = local // fs
    d = fs * fd
    rows = tokens.shape[1]
    block = rows // 2 // n
    wide = -(-(local + 16) // 128) * 128
    vmem = pl.BlockSpec(memory_space=pltpu.VMEM)
    hbm = pl.BlockSpec(memory_space=pltpu.HBM)
    dma = pltpu.SemaphoreType.DMA
    m = n // 2
    two = (2, m, OWN * m // 2, d)
    results = pl.pallas_call(
        functools.partial(kernel, n, n_tp, hu, fd),
        out_shape=(
            jax.ShapeDtypeStruct((OWN, d), BF16),
        )
        + (jax.ShapeDtypeStruct((hu, n_tp, d), BF16),) * 6,
        in_specs=[hbm] * 9,
        out_specs=(vmem,) * 7,
        scratch_shapes=[
            pltpu.VMEM((rows, d), BF16),
            pltpu.VMEM((2, 1, fd), F32),
            pltpu.VMEM((2, 3, fd, local), F32),
            pltpu.VMEM((4 * fd, wide), F32),
            pltpu.VMEM((wide, 4 * fd), F32),
            pltpu.VMEM((2, fs, SENT // 4, 4, 128), BF16),
            pltpu.VMEM((2, 4, fs // 4, SENT // 4, 4, 128), BF16),
            pltpu.VMEM((4, 128, 3 * 128), BF16),
            pltpu.VMEM((5, n_tp, 3, 8, d), BF16),
            pltpu.VMEM((5, n_tp, 3, 4, d), BF16),
            pltpu.VMEM((3, 4 * 12 * n_tp, d), BF16),
            pltpu.VMEM((rows, d), BF16),
            pltpu.VMEM((2, n, block, d), BF16),
            pltpu.VMEM((2, n, block, d), BF16),
            pltpu.VMEM((2, 2, OWN * m // 2, d), BF16),
            pltpu.VMEM((2, n, OWN * m // 2, d), BF16),
            pltpu.VMEM(two, BF16),
            pltpu.VMEM((m * m, OWN, d), BF16),
            pltpu.VMEM((m * m, OWN, d), BF16),
            pltpu.VMEM((m, OWN, d), BF16),
            pltpu.VMEM((OWN * m, d), F32),
            dma((2,)), dma((n + 1,)), dma((5,)), dma((n + 4, 2)), dma((n + 8,)), dma((5,)), dma((3,)), dma((3,)),
            dma((2,)), dma((2, 2)), dma((2,)), dma((2,)), dma(()), dma(()),
            dma((2,)), dma((2,)), dma((4,)),
        ],
        compiler_params=pltpu.CompilerParams(
            collective_id=0, has_side_effects=True, vmem_limit_bytes=46 * 1024 * 1024
        ),
    )(*[
        pltpu.with_memory_space_constraint(a, pltpu.HBM)
        for a in (
            tokens[0],
            gain_first[None], gate_first, up_first, down_first,
            gain_second[None], gate_second, up_second, down_second,
        )
    ]    )
    mixed, *served = pl.pallas_call(
        functools.partial(deliver, 7),
        out_shape=tuple(jax.ShapeDtypeStruct(r.shape, r.dtype) for r in results),
        in_specs=[vmem] * 7,
        out_specs=(hbm,) * 7,
        scratch_shapes=[dma((7,))],
        compiler_params=pltpu.CompilerParams(vmem_limit_bytes=1024 * 1024),
    )(*results)
    return (mixed[None],) + tuple(jnp.swapaxes(r, 0, 1) for r in served)


def solution(mesh):
    weight = P("fs", "tp")
    cut = P(None, "fs", None)
    return jax.shard_map(
        shards,
        mesh=mesh,
        in_specs=(P("tp", None, None), P("fs"), weight, weight, weight, P("fs"), weight, weight, weight),
        out_specs=(P("tp", "fs", None),) + (cut,) * 6,
        check_vma=False,
    )
```
